512 devices in a mesh: ep: 32 (over z, x), tp: 16 (over y, core).
Axes of the slice: x: 4, y: 8, z: 8, core: 2. Of those that a mesh axis runs over, the one named last changes fastest.
Arguments:
- tokens: bfloat16 [256, 2048], P('ep', 'tp'), may hold values from -10 to 10, as said below
- norm_gain: float32 [2048], P('tp'), may hold values from 0.5 to 1.5
- norm_bias: float32 [2048], P('tp'), may hold values from -0.3 to 0.3
- group_pick: int32 [256, 1], P('ep'), may hold values from 0 to 7; in each aligned block of 8 rows (0 to 7, 8 to 15, ...) at most 2 rows name the same one
- member_pick: int32 [256, 4], P('ep'), may hold values from 0 to 7, all different within a row
- picked_probs: float32 [256, 4], P('ep'), may hold values from 0.05 to 1
- gate_weight: bfloat16 [64, 2048, 1024], P('ep', 'tp'), may hold values from -0.125 to 0.125
- up_weight: bfloat16 [64, 2048, 1024], P('ep', 'tp'), may hold values from -0.125 to 0.125
- down_weight: bfloat16 [64, 1024, 2048], P('ep', None, 'tp'), may hold values from -0.375 to 0.375
Outputs:
- mixed: bfloat16 [256, 2048], P('ep', 'tp')
The draws below stay inside these ranges and needn't reach their ends.
Inputs may be any that keep to these rules, and one draw needn't show every extreme that they name: `group_pick`: each entry is a group number from 0 to 7; within each aligned block of 8 tokens no group is named by more than 2 tokens, a bound that some block reaches. `member_pick`: each token's 4 entries are different member numbers from 0 to 7. `tokens`: each token is its own offset between -2 and 2 plus its own scale between 0.25 and 2 times entries of at most 4 in size.
All inputs are finite; a program needn't handle non-finite values.
Results may differ from the reference program's by a relative error of at most 0.01.
Values may be sent and summed in bfloat16 or wider, within the bound.
A program may use at most 64 MiB of HBM per device.

```python
import math
import jax
import jax.numpy as jnp
import numpy as np
from jax import lax

D = 2048
FF = 1024
EPG = 8
TOP_K = 4
TOK_DEV = 8
TOKENS = 256
EXPERTS = 64
GROUPS = 8
GCAP = 2


def draw_tokens(key, part):
    offset_key, scale_key, noise_key = jax.random.split(key, 3)
    offsets = jax.random.uniform(offset_key, (TOKENS, 1), jnp.float32, -2.0, 2.0)
    logs = jax.random.uniform(scale_key, (TOKENS, 1), jnp.float32, math.log(0.5), math.log(2.0))
    noise = jnp.clip(jax.random.normal(noise_key, (TOKENS, D), jnp.float32), -4.0, 4.0)
    return (offsets + jnp.exp(logs) * noise).astype(jnp.bfloat16)


def level_of(key, extent, cuts, smallest, largest):
    def one(dim, parts):
        heights = jax.random.uniform(jax.random.fold_in(jax.random.fold_in(key, 6), dim), (parts,), jnp.float32, smallest / len(cuts), largest / len(cuts))
        return jnp.repeat(jnp.exp(heights), extent[dim] // parts).reshape((-1,) + (1,) * (len(extent) - dim - 1))

    factor_of = one(*cuts[0])
    for cut in cuts[1:]:
        factor_of = factor_of * one(*cut)
    return factor_of


def picks_of(stream_key, rows, count, top, lift):
    sequence = jax.random.permutation(jax.random.fold_in(stream_key, 1), count)
    favour = sequence
    for power in range(3):
        favour = favour * favour // count
    favour = favour * lift // count
    tickets = jax.random.randint(jax.random.fold_in(stream_key, 2), (rows, count), 0, 4096) + favour
    fixed_rows = jax.random.permutation(jax.random.fold_in(stream_key, 3), rows)[jnp.arange(count) % rows]
    tickets = jnp.where(jnp.arange(rows)[:, None] == fixed_rows[None, :], 1 << 14, tickets)
    score = tickets * count + jnp.arange(count)
    return lax.top_k(score.astype(jnp.int32), top)[1].astype(jnp.int32)


def routed_block(stream_key, own, number, rows, number_of, top, most, lean):
    ranking = jax.random.permutation(stream_key, number_of)
    heavy_load, usual = portions_of(number_of, rows * top, most, lean, True), portions_of(number_of, rows * top, most, lean, False)
    places = jnp.arange(number_of)

    def named(tallies, turn):
        used = int((tallies > 0).sum())
        fixed = max(1, used // 4)
        moved = fixed + (places - fixed + turn * (used - fixed)) % max(1, number_of - fixed)
        return jnp.zeros((number_of,), jnp.int32).at[ranking[jnp.where(places < fixed, places, moved)]].set(jnp.asarray(tallies, jnp.int32))

    tallies = jnp.where(number % 4 == 0, named(heavy_load, number // 4), named(usual, number - number // 4 - 1))
    mixed = jax.random.permutation(jax.random.fold_in(own, 3), number_of)
    source_of, sink = mixed[0:number_of // 2 * 2:2], mixed[1:number_of // 2 * 2:2]
    room = jnp.minimum(tallies[source_of] - 1, most - tallies[sink]) // 2
    room = jnp.where((source_of == ranking[0]) | (sink == ranking[0]) | (tallies[sink] == 0), 0, jnp.maximum(room, 0))
    moved = jax.random.randint(jax.random.fold_in(own, 4), (number_of // 2,), 0, 1 << 20) % (room + 1)
    tallies = tallies.at[source_of].add(-moved).at[sink].add(moved)
    items = jnp.searchsorted(jnp.cumsum(tallies), jnp.arange(rows * top), side="right").astype(jnp.int32)
    grid = items.reshape(top, rows).T
    grid = grid[jax.random.permutation(jax.random.fold_in(own, 1), rows)]
    turn = jax.random.randint(jax.random.fold_in(own, 2), (rows, 1), 0, top)
    return jnp.take_along_axis(grid, (jnp.arange(top)[None, :] + turn) % top, axis=1)


def portions_of(amount, total, bound, lean, full):
    portions = [(1 << 20) // math.isqrt(standing ** lean) + 1 for standing in range(1, amount + 1)]
    largest = bound if full else min(bound, max(-(-total // amount), total * portions[0] // sum(portions)))
    least = 1 if total - largest >= amount - 1 else 0
    given, surplus = [largest] + [least] * (amount - 1), total - largest - least * (amount - 1)
    while surplus > 0:
        free = [i for i in range(1, amount) if given[i] < largest] or [i for i in range(1, amount) if given[i] < bound]
        whole, left = sum([portions[i] for i in free]), surplus
        for i in free:
            extra = min(bound - given[i], max(1, left * portions[i] // whole), surplus)
            given[i] = given[i] + extra
            surplus = surplus - extra
    return np.array(given)


def scatter_about(stream_key, dims, scale, limit, cuts=(), held_as=jnp.bfloat16):
    factor_of = level_of(stream_key, dims, cuts, -0.22, 0.18) if cuts else 1.0
    drawn = jax.random.normal(stream_key, dims, jnp.float32) * scale * factor_of
    return jnp.minimum(jnp.maximum(drawn, -limit), limit).astype(held_as)


def setup_inputs(seed: int = 0) -> dict:
    arg_keys = jax.random.split(jax.random.key(seed), 10)
    tokens = draw_tokens(jax.random.fold_in(arg_keys[9], 71), 0)
    norm_gain = jnp.clip(1.0 + 0.1 * jax.random.normal(arg_keys[1], (D,), jnp.float32), 0.5, 1.5)
    norm_bias = scatter_about(arg_keys[2], (D,), 0.1, 0.3, ((0, 16),), jnp.float32)
    group_pick_keys = jax.random.split(jax.random.fold_in(arg_keys[3], 1), TOKENS // TOK_DEV)
    group_pick_turns = jax.random.permutation(jax.random.fold_in(arg_keys[3], 3), TOKENS // TOK_DEV)
    group_pick = jax.vmap(lambda own, number: routed_block(jax.random.fold_in(arg_keys[3], 2), own, number, TOK_DEV, GROUPS, 1, GCAP, 2))(group_pick_keys, group_pick_turns).reshape((TOKENS, 1))
    member_pick = picks_of(arg_keys[4], TOKENS, EPG, TOP_K, 4096)
    picked_probs = jnp.clip(jnp.exp(math.log(1.0) - 2.9957323 * jax.random.uniform(arg_keys[5], (TOKENS, TOP_K), jnp.float32) ** level_of(arg_keys[5], (TOKENS, TOP_K), ((0, 32),), -0.2, 0.2)), 0.05, 1.0)
    gate_weight = scatter_about(arg_keys[6], (EXPERTS, D, FF), D ** -0.5, 0.125, ((0, 32), (1, 16)))
    up_weight = scatter_about(arg_keys[7], (EXPERTS, D, FF), D ** -0.5, 0.125, ((0, 32), (1, 16)))
    down_weight = scatter_about(arg_keys[8], (EXPERTS, FF, D), (FF // 4) ** -0.5, 0.375, ((0, 32), (2, 16)))
    return {"tokens": tokens, "norm_gain": norm_gain, "norm_bias": norm_bias, "group_pick": group_pick, "member_pick": member_pick, "picked_probs": picked_probs, "gate_weight": gate_weight, "up_weight": up_weight, "down_weight": down_weight}


norm_epsilon = 1e-5


def reference(tokens, norm_gain, norm_bias, group_pick, member_pick, picked_probs, gate_weight, up_weight, down_weight):
    values = tokens.astype(jnp.float32)
    center = jnp.mean(values, axis=1, keepdims=True)
    shifted = values - center
    spread = jnp.mean(shifted * shifted, axis=1, keepdims=True)
    scaled = shifted * lax.rsqrt(spread + norm_epsilon)
    normed = (scaled * norm_gain.astype(jnp.float32) + norm_bias.astype(jnp.float32)).astype(jnp.bfloat16)
    chosen = (group_pick * EPG + member_pick).astype(jnp.int32)
    shares = picked_probs / jnp.sum(picked_probs, axis=1, keepdims=True)

    def one_token(packed):
        row, picks, weights = packed
        row_wide = row.astype(jnp.float32)
        gate_rows = jnp.take(gate_weight, picks, axis=0).astype(jnp.float32)
        up_rows = jnp.take(up_weight, picks, axis=0).astype(jnp.float32)
        down_rows = jnp.take(down_weight, picks, axis=0).astype(jnp.float32)
        gate_sum = jnp.einsum("d,kdf->kf", row_wide, gate_rows)
        up_sum = jnp.einsum("d,kdf->kf", row_wide, up_rows)
        hidden = (jax.nn.silu(gate_sum) * up_sum).astype(jnp.bfloat16)
        expert_out = jnp.einsum("kf,kfd->kd", hidden.astype(jnp.float32), down_rows).astype(jnp.bfloat16)
        return jnp.sum(weights[:, None] * expert_out.astype(jnp.float32), axis=0)

    combined = lax.map(one_token, (normed, chosen, shares))
    return combined.astype(jnp.bfloat16)
```

```python
import functools

import jax
import jax.numpy as jnp
from jax import lax
from jax.experimental import pallas as pl
from jax.experimental.pallas import tpu as pltpu
from jax.sharding import PartitionSpec as P

EPG = 8
CAP = 2
norm_epsilon = 1e-05
MESH = pl.DeviceIdType.MESH
F32 = jnp.float32
BF16 = jnp.bfloat16
L = 128


def iota(shape, axis):
    return lax.broadcasted_iota(jnp.int32, shape, axis)


def far_first(n):
    return sorted(range(1, n), key=lambda d: -min(d, n - d))


def kernel(
    nz, nx, ny, features,
    tok_ref, gain_ref, bias_ref, gp_ref, mp_ref, pp_ref, gate_ref, up_ref, down_ref,
    out_ref,
    wg, wu, wd, gb,
    s1, r1, r2t, r2s, ax1s, ax1r, ax2s, ax2r, ps, pr, hb, o5s, r5, s6, r6,
    lsem, xsem_s, xsem_r, s1s, s1r, s2s_s, s2s_r, s2t_s, s2t_r, a1s, a1r, a2s, a2r,
    p_s, p_r, h_s, h_r, o_s, o_r, f_s, f_r,
):
    tokens = tok_ref.shape[0]
    half = wg.shape[2]
    rows = nz * CAP
    per_expert = ny // 2
    ep, tp = lax.axis_index("ep"), lax.axis_index("tp")
    z, x, y, c = ep // nx, ep % nx, tp // 2, tp % 2

    def dev(dz=0, dx=0, dy=0, dc=0):
        return {
            "ep": ((z + dz + nz) % nz) * nx + (x + dx + nx) % nx,
            "tp": ((y + dy + ny) % ny) * 2 + (c + dc) % 2,
        }

    def remote(src, dst, ss, rs, device):
        return pltpu.make_async_remote_copy(
            src_ref=src, dst_ref=dst, send_sem=ss, recv_sem=rs, device_id=device, device_id_type=MESH
        )

    def each(n, body):
        lax.fori_loop(1, n, lambda d, carry: (body(d), carry)[1], 0)

    mine = pl.ds(pl.multiple_of(c * half, half), half)
    other = pl.ds(pl.multiple_of((1 - c) * half, half), half)
    local = [
        pltpu.make_async_copy(gate_ref.at[:, :, mine], wg.at[:, 0:L, :], lsem.at[0]),
        pltpu.make_async_copy(up_ref.at[:, :, mine], wu.at[:, 0:L, :], lsem.at[1]),
        pltpu.make_async_copy(down_ref.at[:, mine, :], wd.at[:, :, 0:L], lsem.at[2]),
    ]
    for copy in local:
        copy.start()

    barrier = pltpu.get_barrier_semaphore()

    def greet(**where):
        pl.semaphore_signal(barrier, inc=1, device_id=dev(**where), device_id_type=MESH)

    each(nz, lambda d: greet(dz=d))
    each(ny, lambda d: greet(dy=d))
    each(2 * nx, lambda k: greet(dx=k // 2, dc=k % 2))

    group = (gp_ref[...] - z + nz) % nz
    lane = iota((tokens, L), 1)
    member = (group == lane // CAP).astype(F32)
    count = jnp.zeros((tokens, L), F32)
    sub = iota((tokens, L), 0)
    for t in range(tokens - 1):
        count = count + jnp.where(sub > t, member[t : t + 1, :], 0.0)
    chosen = member * (count == (lane % CAP).astype(F32)).astype(F32)
    probs = pp_ref[...]
    share = probs / jnp.sum(probs, axis=1, keepdims=True)
    high = share.astype(BF16).astype(F32)
    low = share - high
    picks = mp_ref[...]
    shares = jnp.zeros((tokens, L), F32)
    for k in range(picks.shape[1]):
        pick = picks[:, k : k + 1]
        shares = shares + jnp.where(lane == pick, high[:, k : k + 1], 0.0)
        shares = shares + jnp.where(lane == pick + EPG, low[:, k : k + 1], 0.0)
    rowwise = jnp.transpose(chosen)[0:rows, :]
    both = jnp.concatenate([tok_ref[...].astype(F32), shares], axis=1)
    packed = jnp.zeros((rows, 2 * L), F32)
    for t in range(tokens):
        packed = packed + rowwise[:, t : t + 1] * both[t : t + 1, :]
    for d in range(nz):
        s1[d] = packed[d * CAP : (d + 1) * CAP, :]
    r1[0] = packed[0:CAP, :]

    pl.semaphore_wait(barrier, (nz - 1) + (ny - 1) + (2 * nx - 1))

    def s1_copy(d):
        return remote(s1.at[d], r1.at[d], s1s.at[d], s1r.at[d], dev(dz=d))

    each(nz, lambda d: s1_copy(d).start())

    def swaps():
        to = dev(dc=1)
        return [
            remote(gate_ref.at[:, :, other], wg.at[:, L : 2 * L, :], xsem_s.at[0], xsem_r.at[0], to),
            remote(up_ref.at[:, :, other], wu.at[:, L : 2 * L, :], xsem_s.at[1], xsem_r.at[1], to),
            remote(down_ref.at[:, other, :], wd.at[:, :, L : 2 * L], xsem_s.at[2], xsem_r.at[2], to),
            remote(gain_ref, gb.at[0], xsem_s.at[3], xsem_r.at[3], to),
            remote(bias_ref, gb.at[1], xsem_s.at[4], xsem_r.at[4], to),
        ]

    for copy in swaps():
        copy.start()

    each(nz, lambda d: s1_copy(d).wait_recv())

    block = jnp.concatenate([r1[d] for d in range(nz)], axis=0)
    r2t[0, 0] = block[:, 0:L].astype(BF16)
    r2s[0] = block[:, L : 2 * L].astype(BF16)

    def s2_copy(k):
        dx, dc = k // 2, k % 2
        return remote(r2t.at[0, 0], r2t.at[dx, dc], s2t_s.at[k], s2t_r.at[k], dev(dx=dx, dc=dc))

    def s2_shares(dx):
        return remote(r2s.at[0], r2s.at[dx], s2s_s.at[dx], s2s_r.at[dx], dev(dx=dx))

    each(2 * nx, lambda k: s2_copy(k).start())
    each(nx, lambda k: s2_shares(k).start())

    for copy in local:
        copy.wait()
    for copy in swaps():
        copy.wait()
    gain = jnp.concatenate([gain_ref[...], gb[0]], axis=1)
    bias = jnp.concatenate([bias_ref[...], gb[1]], axis=1)
    gain_high = gain.astype(BF16).astype(F32)
    bias_high = bias.astype(BF16).astype(F32)
    four = iota((16, 2 * L), 0)
    vectors = jnp.where(four == 0, gain_high, 0.0) + jnp.where(four == 1, gain - gain_high, 0.0)
    vectors = vectors + jnp.where(four == 2, bias_high, 0.0) + jnp.where(four == 3, bias - bias_high, 0.0)
    vectors = vectors.astype(BF16)
    for e in range(2):
        for side, weight in enumerate((wg, wu)):
            line = jnp.dot(vectors, weight[e], preferred_element_type=F32)
            for j in range(per_expert):
                part = line[:, j * L : (j + 1) * L]
                ax1s[e * per_expert + j, 0:1, side * L : (side + 1) * L] = part[0:1] + part[1:2]
                ax1s[e * per_expert + j, 1:2, side * L : (side + 1) * L] = part[2:3] + part[3:4]
    ax1r[0] = ax1s[y]

    def a1_copy(d):
        return remote(ax1s.at[(y + d) % ny], ax1r.at[d], a1s.at[d], a1r.at[d], dev(dy=d))

    each(ny, lambda d: a1_copy(d).start())

    each(2 * nx, lambda k: s2_copy(k).wait_recv())

    all_rows = nx * rows
    own = jnp.concatenate([r2t[dx, 0] for dx in range(nx)], axis=0).astype(F32)
    partner = jnp.concatenate([r2t[dx, 1] for dx in range(nx)], axis=0).astype(F32)
    middle = jnp.sum(own + partner, axis=1, keepdims=True) * (1.0 / (2 * L))
    own = own - middle
    partner = partner - middle
    scaled = jnp.concatenate([own * gain[:, 0:L], partner * gain[:, L : 2 * L]], axis=1).astype(BF16)

    def p_copy(d):
        return remote(ps.at[d], pr.at[d], p_s.at[d], p_r.at[d], dev(dy=d))

    def a2_copy(d):
        return remote(ax2s, ax2r.at[d], a2s.at[d], a2r.at[d], dev(dy=d))

    gate_own = up_own = None
    for place, d in enumerate(far_first(ny) + [0]):
        q = (y + d) % ny
        e = q // per_expert
        cols = pl.ds(pl.multiple_of((q % per_expert) * L, L), L)
        gate_part = jnp.dot(scaled, wg[e, :, cols], preferred_element_type=F32)
        up_part = jnp.dot(scaled, wu[e, :, cols], preferred_element_type=F32)
        if d == 0:
            gate_own, up_own = gate_part, up_part
        else:
            ps[d, 0] = gate_part.astype(BF16)
            ps[d, 1] = up_part.astype(BF16)
            p_copy(d).start()
        if place == 2 or (place == 0 and ny == 2):
            squares = jnp.sum(own * own + partner * partner, axis=1, keepdims=True)
            lanes = iota((all_rows, L), 1)
            columns = jnp.where(lanes == 0, middle, 0.0) + jnp.where(lanes == 1, squares, 0.0)
            turned = jnp.transpose(columns)
            ax2s[:, 0:all_rows] = turned[0:2, :]
            ax2r[0, :, 0:all_rows] = turned[0:2, :]
            each(ny, lambda d: a2_copy(d).start())

    each(ny, lambda d: a1_copy(d).wait_recv())
    each(ny, lambda d: a2_copy(d).wait_recv())
    means = [ax2r[d, 0:1, 0:all_rows] for d in range(ny)]
    center = sum(means) * (1.0 / ny)
    shifts = [m - center for m in means]
    spread = sum(ax2r[d, 1:2, 0:all_rows] for d in range(ny)) + (features // ny) * sum(s * s for s in shifts)
    scale = lax.rsqrt(spread * (1.0 / features) + norm_epsilon)
    depth = 16
    stack = iota((depth, all_rows), 0)
    table = jnp.where(stack == ny, scale, 0.0)
    for d in range(ny):
        table = table + jnp.where(stack == d, shifts[d], 0.0)
    table = jnp.transpose(table)
    scale = table[:, ny : ny + 1]
    gate, up = gate_own, up_own
    gate_bias = up_bias = jnp.zeros((1, L), F32)
    for d in range(ny):
        shift = table[:, d : d + 1]
        gate = gate + shift * ax1r[d, 0:1, 0:L]
        up = up + shift * ax1r[d, 0:1, L : 2 * L]
        gate_bias = gate_bias + ax1r[d, 1:2, 0:L]
        up_bias = up_bias + ax1r[d, 1:2, L : 2 * L]
    each(nx, lambda k: s2_shares(k).wait_recv())
    expert = 2 * x + y // per_expert
    lanes = iota((all_rows, L), 1)
    share = jnp.concatenate([r2s[dx] for dx in range(nx)], axis=0).astype(F32)
    share = jnp.sum(
        jnp.where((lanes == expert) | (lanes == expert + EPG), share, 0.0), axis=1, keepdims=True
    )

    for d in sorted(range(1, ny), key=lambda d: min(d, ny - d)):
        p_copy(d).wait_recv()
        gate = gate + pr[d, 0].astype(F32)
        up = up + pr[d, 1].astype(F32)
    gate = gate * scale + gate_bias
    up = up * scale + up_bias
    hidden = (share * (gate / (1.0 + jnp.exp(-gate)) * up)).astype(BF16)
    hb[0] = hidden

    def h_copy(d):
        return remote(hb.at[0], hb.at[d], h_s.at[d], h_r.at[d], dev(dy=d))

    for d in far_first(ny):
        h_copy(d).start()

    def down(d):
        q = (y - d + ny) % ny
        units = pl.ds(pl.multiple_of((q % per_expert) * L, L), L)
        return jnp.dot(hb[d], wd[q // per_expert, units, :], preferred_element_type=F32)

    total = down(0)
    for d in sorted(range(1, ny), key=lambda d: min(d, ny - d)):
        h_copy(d).wait_recv()
        total = total + down(d)

    for dx in range(nx):
        for dc in range(2):
            o5s[dx, dc] = total[dx * rows : (dx + 1) * rows, dc * L : (dc + 1) * L].astype(BF16)

    def o_copy(k):
        dx, dc = k // 2, k % 2
        return remote(o5s.at[dx, dc], r5.at[dx, dc], o_s.at[k], o_r.at[k], dev(dx=-dx, dc=dc))

    each(2 * nx, lambda k: o_copy(k).start())
    summed = total[0:rows, 0:L]
    each(2 * nx, lambda k: o_copy(k).wait_recv())
    for k in range(1, 2 * nx):
        summed = summed + r5[k // 2, k % 2].astype(F32)
    summed = summed.astype(BF16).astype(F32)

    for d in range(nz):
        s6[d] = summed[d * CAP : (d + 1) * CAP, :]
    r6[0] = summed[0:CAP, :]

    def f_copy(d):
        return remote(s6.at[d], r6.at[d], f_s.at[d], f_r.at[d], dev(dz=-d))

    each(nz, lambda d: f_copy(d).start())

    each(nz, lambda d: s1_copy(d).wait_send())
    each(2 * nx, lambda k: s2_copy(k).wait_send())
    each(nx, lambda k: s2_shares(k).wait_send())
    each(ny, lambda d: a1_copy(d).wait_send())
    each(ny, lambda d: a2_copy(d).wait_send())
    each(ny, lambda d: p_copy(d).wait_send())
    each(ny, lambda d: h_copy(d).wait_send())
    each(2 * nx, lambda k: o_copy(k).wait_send())
    each(nz, lambda d: f_copy(d).wait_send())
    each(nz, lambda d: f_copy(d).wait_recv())

    result = jnp.zeros((tokens, L), F32)
    for d in range(nz):
        back = r6[d]
        for s in range(CAP):
            at = d * CAP + s
            result = result + chosen[:, at : at + 1] * back[s : s + 1, :]
    out_ref[...] = result.astype(BF16)


def solution(mesh):
    nx = EPG // 2
    nz = mesh.shape["ep"] // nx
    ny = mesh.shape["tp"] // 2

    def on_device(tokens, gain, bias, group_pick, member_pick, probs, gate, up, down):
        width = tokens.shape[1]
        half = gate.shape[2] // 2
        rows = nz * CAP
        all_rows = nx * rows
        vmem, dma = pltpu.VMEM, pltpu.SemaphoreType.DMA
        whole = pl.BlockSpec(memory_space=pltpu.VMEM)
        away = pl.BlockSpec(memory_space=pl.ANY)
        return pl.pallas_call(
            functools.partial(kernel, nz, nx, ny, width * 2 * ny),
            out_shape=jax.ShapeDtypeStruct(tokens.shape, BF16),
            in_specs=[whole] * 6 + [away] * 3,
            out_specs=whole,
            scratch_shapes=[
                vmem((2, 2 * L, half), BF16),
                vmem((2, 2 * L, half), BF16),
                vmem((2, half, 2 * L), BF16),
                vmem((2, 1, L), F32),
                vmem((nz, CAP, 2 * L), F32),
                vmem((nz, CAP, 2 * L), F32),
                vmem((nx, 2, rows, L), BF16),
                vmem((nx, rows, L), BF16),
                vmem((ny, 2, 2 * L), F32),
                vmem((ny, 2, 2 * L), F32),
                vmem((2, L), F32),
                vmem((ny, 2, L), F32),
                vmem((ny, 2, all_rows, L), BF16),
                vmem((ny, 2, all_rows, L), BF16),
                vmem((ny, all_rows, L), BF16),
                vmem((nx, 2, rows, L), BF16),
                vmem((nx, 2, rows, L), BF16),
                vmem((nz, CAP, L), F32),
                vmem((nz, CAP, L), F32),
                dma((3,)),
                dma((5,)),
                dma((5,)),
                dma((nz,)),
                dma((nz,)),
                dma((nx,)),
                dma((nx,)),
                dma((2 * nx,)),
                dma((2 * nx,)),
                dma((ny,)),
                dma((ny,)),
                dma((ny,)),
                dma((ny,)),
                dma((ny,)),
                dma((ny,)),
                dma((ny,)),
                dma((ny,)),
                dma((2 * nx,)),
                dma((2 * nx,)),
                dma((nz,)),
                dma((nz,)),
            ],
            compiler_params=pltpu.CompilerParams(collective_id=0, has_side_effects=True),
        )(tokens, gain.reshape(1, -1), bias.reshape(1, -1), group_pick, member_pick, probs, gate, up, down)

    return jax.shard_map(
        on_device,
        mesh=mesh,
        in_specs=(
            P("ep", "tp"),
            P("tp"),
            P("tp"),
            P("ep", None),
            P("ep", None),
            P("ep", None),
            P("ep", "tp", None),
            P("ep", "tp", None),
            P("ep", None, "tp"),
        ),
        out_specs=P("ep", "tp"),
        check_vma=False,
    )
```

```python
import functools

import jax
import jax.numpy as jnp
from jax import lax
from jax.experimental import pallas as pl
from jax.experimental.pallas import tpu as pltpu
from jax.sharding import PartitionSpec as P

EPG = 8
CAP = 2
norm_epsilon = 1e-05
MESH = pl.DeviceIdType.MESH
F32 = jnp.float32
BF16 = jnp.bfloat16
L = 128


def iota(shape, axis):
    return lax.broadcasted_iota(jnp.int32, shape, axis)


def far_first(n):
    return sorted(range(1, n), key=lambda d: -min(d, n - d))


def kernel(
    nz, nx, ny, features,
    tok_hbm, gain_hbm, bias_hbm, gp_hbm, mp_hbm, pp_hbm, gate_ref, up_ref, down_ref,
    out_ref,
    tok_ref, gain_ref, bias_ref, gp_ref, mp_ref, pp_ref, isem,
    wg, wu, wd, gb,
    s1, r1, r2t, r2s, ax1s, ax1r, ax2s, ax2r, ps, pr, hb, o5s, r5, s6, r6,
    lsem, xsem_s, xsem_r, s1s, s1r, s2s_s, s2s_r, s2t_s, s2t_r, a1s, a1r, a2s, a2r,
    p_s, p_r, h_s, h_r, o_s, o_r, f_s, f_r,
):
    tokens = tok_ref.shape[0]
    half = wg.shape[2]
    rows = nz * CAP
    per_expert = ny // 2
    ep, tp = lax.axis_index("ep"), lax.axis_index("tp")
    z, x, y, c = ep // nx, ep % nx, tp // 2, tp % 2

    def dev(dz=0, dx=0, dy=0, dc=0):
        return {
            "ep": ((z + dz + nz) % nz) * nx + (x + dx + nx) % nx,
            "tp": ((y + dy + ny) % ny) * 2 + (c + dc) % 2,
        }

    def remote(src, dst, ss, rs, device):
        return pltpu.make_async_remote_copy(
            src_ref=src, dst_ref=dst, send_sem=ss, recv_sem=rs, device_id=device, device_id_type=MESH
        )

    def each(n, body):
        lax.fori_loop(1, n, lambda d, carry: (body(d), carry)[1], 0)

    inputs = [
        pltpu.make_async_copy(src, dst, isem.at[i])
        for i, (src, dst) in enumerate(
            (
                (tok_hbm, tok_ref),
                (gp_hbm, gp_ref),
                (mp_hbm, mp_ref),
                (pp_hbm, pp_ref),
                (gain_hbm, gain_ref),
                (bias_hbm, bias_ref),
            )
        )
    ]
    for copy in inputs:
        copy.start()

    mine = pl.ds(pl.multiple_of(c * half, half), half)
    other = pl.ds(pl.multiple_of((1 - c) * half, half), half)
    local = [
        pltpu.make_async_copy(gate_ref.at[:, :, mine], wg.at[:, 0:L, :], lsem.at[0]),
        pltpu.make_async_copy(up_ref.at[:, :, mine], wu.at[:, 0:L, :], lsem.at[1]),
        pltpu.make_async_copy(down_ref.at[:, mine, :], wd.at[:, :, 0:L], lsem.at[2]),
    ]
    for copy in local:
        copy.start()

    barrier = pltpu.get_barrier_semaphore()

    def greet(**where):
        pl.semaphore_signal(barrier, inc=1, device_id=dev(**where), device_id_type=MESH)

    each(nz, lambda d: greet(dz=d))
    each(ny, lambda d: greet(dy=d))
    each(2 * nx, lambda k: greet(dx=k // 2, dc=k % 2))

    for copy in inputs:
        copy.wait()

    group = (gp_ref[...] - z + nz) % nz
    row = iota((rows, tokens), 0)
    lane = iota((rows, tokens), 1)
    member = (group == row // CAP).astype(F32)
    count = jnp.zeros((rows, tokens), F32)
    for t in range(tokens - 1):
        count = count + jnp.where(lane > t, member[:, t : t + 1], 0.0)
    rowwise = member * (count == (row % CAP).astype(F32)).astype(F32)
    probs = pp_ref[...]
    share = probs / jnp.sum(probs, axis=0, keepdims=True)
    top = probs.shape[0]
    table = [share[k : k + 1] for k in range(top)] + [mp_ref[k : k + 1].astype(F32) for k in range(top)]
    wide = jnp.concatenate([jnp.concatenate(table + [rowwise], axis=0), jnp.zeros((2 * top + rows, L - tokens), F32)], axis=1)
    turned = jnp.transpose(wide)[0:tokens, :]
    chosen = turned[:, 2 * top :]
    lane = iota((tokens, L), 1).astype(F32)
    shares = jnp.zeros((tokens, L), F32)
    for k in range(top):
        high = turned[:, k : k + 1].astype(BF16).astype(F32)
        low = turned[:, k : k + 1] - high
        pick = turned[:, top + k : top + k + 1]
        shares = shares + jnp.where(lane == pick, high, 0.0)
        shares = shares + jnp.where(lane == pick + EPG, low, 0.0)
    both = jnp.concatenate([tok_ref[...].astype(F32), shares], axis=1)
    packed = jnp.zeros((rows, 2 * L), F32)
    for t in range(tokens):
        packed = packed + rowwise[:, t : t + 1] * both[t : t + 1, :]
    for d in range(nz):
        s1[d] = packed[d * CAP : (d + 1) * CAP, :]
    r1[0] = packed[0:CAP, :]

    pl.semaphore_wait(barrier, (nz - 1) + (ny - 1) + (2 * nx - 1))

    def s1_copy(d):
        return remote(s1.at[d], r1.at[d], s1s.at[d], s1r.at[d], dev(dz=d))

    each(nz, lambda d: s1_copy(d).start())

    def swaps():
        to = dev(dc=1)
        return [
            remote(gate_ref.at[:, :, other], wg.at[:, L : 2 * L, :], xsem_s.at[0], xsem_r.at[0], to),
            remote(up_ref.at[:, :, other], wu.at[:, L : 2 * L, :], xsem_s.at[1], xsem_r.at[1], to),
            remote(down_ref.at[:, other, :], wd.at[:, :, L : 2 * L], xsem_s.at[2], xsem_r.at[2], to),
            remote(gain_ref, gb.at[0], xsem_s.at[3], xsem_r.at[3], to),
            remote(bias_ref, gb.at[1], xsem_s.at[4], xsem_r.at[4], to),
        ]

    for copy in swaps():
        copy.start()

    each(nz, lambda d: s1_copy(d).wait_recv())

    block = jnp.concatenate([r1[d] for d in range(nz)], axis=0)
    r2t[0, 0] = block[:, 0:L].astype(BF16)
    r2s[0] = block[:, L : 2 * L].astype(BF16)

    def s2_copy(k):
        dx, dc = k // 2, k % 2
        return remote(r2t.at[0, 0], r2t.at[dx, dc], s2t_s.at[k], s2t_r.at[k], dev(dx=dx, dc=dc))

    def s2_shares(dx):
        return remote(r2s.at[0], r2s.at[dx], s2s_s.at[dx], s2s_r.at[dx], dev(dx=dx))

    each(2 * nx, lambda k: s2_copy(k).start())
    each(nx, lambda k: s2_shares(k).start())

    for copy in local:
        copy.wait()
    for copy in swaps():
        copy.wait()
    gain = jnp.concatenate([gain_ref[...], gb[0]], axis=1)
    bias = jnp.concatenate([bias_ref[...], gb[1]], axis=1)
    gain_high = gain.astype(BF16).astype(F32)
    bias_high = bias.astype(BF16).astype(F32)
    four = iota((16, 2 * L), 0)
    vectors = jnp.where(four == 0, gain_high, 0.0) + jnp.where(four == 1, gain - gain_high, 0.0)
    vectors = vectors + jnp.where(four == 2, bias_high, 0.0) + jnp.where(four == 3, bias - bias_high, 0.0)
    vectors = vectors.astype(BF16)
    for e in range(2):
        for side, weight in enumerate((wg, wu)):
            line = jnp.dot(vectors, weight[e], preferred_element_type=F32)
            for j in range(per_expert):
                part = line[:, j * L : (j + 1) * L]
                ax1s[e * per_expert + j, 0:1, side * L : (side + 1) * L] = part[0:1] + part[1:2]
                ax1s[e * per_expert + j, 1:2, side * L : (side + 1) * L] = part[2:3] + part[3:4]
    ax1r[0] = ax1s[y]

    def a1_copy(d):
        return remote(ax1s.at[(y + d) % ny], ax1r.at[d], a1s.at[d], a1r.at[d], dev(dy=d))

    each(ny, lambda d: a1_copy(d).start())

    each(2 * nx, lambda k: s2_copy(k).wait_recv())

    all_rows = nx * rows
    own = jnp.concatenate([r2t[dx, 0] for dx in range(nx)], axis=0).astype(F32)
    partner = jnp.concatenate([r2t[dx, 1] for dx in range(nx)], axis=0).astype(F32)
    middle = jnp.sum(own + partner, axis=1, keepdims=True) * (1.0 / (2 * L))
    own = own - middle
    partner = partner - middle
    scaled = jnp.concatenate([own * gain[:, 0:L], partner * gain[:, L : 2 * L]], axis=1).astype(BF16)

    def p_copy(d):
        return remote(ps.at[d], pr.at[d], p_s.at[d], p_r.at[d], dev(dy=d))

    def a2_copy(d):
        return remote(ax2s, ax2r.at[d], a2s.at[d], a2r.at[d], dev(dy=d))

    gate_own = up_own = None
    for place, d in enumerate(far_first(ny) + [0]):
        q = (y + d) % ny
        e = q // per_expert
        cols = pl.ds(pl.multiple_of((q % per_expert) * L, L), L)
        gate_part = jnp.dot(scaled, wg[e, :, cols], preferred_element_type=F32)
        up_part = jnp.dot(scaled, wu[e, :, cols], preferred_element_type=F32)
        if d == 0:
            gate_own, up_own = gate_part, up_part
        else:
            ps[d, 0] = gate_part.astype(BF16)
            ps[d, 1] = up_part.astype(BF16)
            p_copy(d).start()
        if place == 2 or (place == 0 and ny == 2):
            squares = jnp.sum(own * own + partner * partner, axis=1, keepdims=True)
            lanes = iota((all_rows, L), 1)
            columns = jnp.where(lanes == 0, middle, 0.0) + jnp.where(lanes == 1, squares, 0.0)
            turned = jnp.transpose(columns)
            ax2s[:, 0:all_rows] = turned[0:2, :]
            ax2r[0, :, 0:all_rows] = turned[0:2, :]
            each(ny, lambda d: a2_copy(d).start())

    each(ny, lambda d: a1_copy(d).wait_recv())
    each(ny, lambda d: a2_copy(d).wait_recv())
    means = [ax2r[d, 0:1, 0:all_rows] for d in range(ny)]
    center = sum(means) * (1.0 / ny)
    shifts = [m - center for m in means]
    spread = sum(ax2r[d, 1:2, 0:all_rows] for d in range(ny)) + (features // ny) * sum(s * s for s in shifts)
    scale = lax.rsqrt(spread * (1.0 / features) + norm_epsilon)
    depth = 16
    stack = iota((depth, all_rows), 0)
    table = jnp.where(stack == ny, scale, 0.0)
    for d in range(ny):
        table = table + jnp.where(stack == d, shifts[d], 0.0)
    table = jnp.transpose(table)
    scale = table[:, ny : ny + 1]
    gate, up = gate_own, up_own
    gate_bias = up_bias = jnp.zeros((1, L), F32)
    for d in range(ny):
        shift = table[:, d : d + 1]
        gate = gate + shift * ax1r[d, 0:1, 0:L]
        up = up + shift * ax1r[d, 0:1, L : 2 * L]
        gate_bias = gate_bias + ax1r[d, 1:2, 0:L]
        up_bias = up_bias + ax1r[d, 1:2, L : 2 * L]
    each(nx, lambda k: s2_shares(k).wait_recv())
    expert = 2 * x + y // per_expert
    lanes = iota((all_rows, L), 1)
    share = jnp.concatenate([r2s[dx] for dx in range(nx)], axis=0).astype(F32)
    share = jnp.sum(
        jnp.where((lanes == expert) | (lanes == expert + EPG), share, 0.0), axis=1, keepdims=True
    )

    for d in sorted(range(1, ny), key=lambda d: min(d, ny - d)):
        p_copy(d).wait_recv()
        gate = gate + pr[d, 0].astype(F32)
        up = up + pr[d, 1].astype(F32)
    gate = gate * scale + gate_bias
    up = up * scale + up_bias
    hidden = (share * (gate / (1.0 + jnp.exp(-gate)) * up)).astype(BF16)
    hb[0] = hidden

    def h_copy(d):
        return remote(hb.at[0], hb.at[d], h_s.at[d], h_r.at[d], dev(dy=d))

    for d in far_first(ny):
        h_copy(d).start()

    def down(d):
        q = (y - d + ny) % ny
        units = pl.ds(pl.multiple_of((q % per_expert) * L, L), L)
        return jnp.dot(hb[d], wd[q // per_expert, units, :], preferred_element_type=F32)

    total = down(0)
    for d in sorted(range(1, ny), key=lambda d: min(d, ny - d)):
        h_copy(d).wait_recv()
        total = total + down(d)

    for dx in range(nx):
        for dc in range(2):
            o5s[dx, dc] = total[dx * rows : (dx + 1) * rows, dc * L : (dc + 1) * L].astype(BF16)

    def o_copy(k):
        dx, dc = k // 2, k % 2
        return remote(o5s.at[dx, dc], r5.at[dx, dc], o_s.at[k], o_r.at[k], dev(dx=-dx, dc=dc))

    each(2 * nx, lambda k: o_copy(k).start())
    summed = total[0:rows, 0:L]
    each(2 * nx, lambda k: o_copy(k).wait_recv())
    for k in range(1, 2 * nx):
        summed = summed + r5[k // 2, k % 2].astype(F32)
    summed = summed.astype(BF16).astype(F32)

    for d in range(nz):
        s6[d] = summed[d * CAP : (d + 1) * CAP, :]
    r6[0] = summed[0:CAP, :]

    def f_copy(d):
        return remote(s6.at[d], r6.at[d], f_s.at[d], f_r.at[d], dev(dz=-d))

    each(nz, lambda d: f_copy(d).start())

    each(nz, lambda d: s1_copy(d).wait_send())
    each(2 * nx, lambda k: s2_copy(k).wait_send())
    each(nx, lambda k: s2_shares(k).wait_send())
    each(ny, lambda d: a1_copy(d).wait_send())
    each(ny, lambda d: a2_copy(d).wait_send())
    each(ny, lambda d: p_copy(d).wait_send())
    each(ny, lambda d: h_copy(d).wait_send())
    each(2 * nx, lambda k: o_copy(k).wait_send())
    each(nz, lambda d: f_copy(d).wait_send())
    each(nz, lambda d: f_copy(d).wait_recv())

    result = jnp.zeros((tokens, L), F32)
    for d in range(nz):
        back = r6[d]
        for s in range(CAP):
            at = d * CAP + s
            result = result + chosen[:, at : at + 1] * back[s : s + 1, :]
    out_ref[...] = result.astype(BF16)


def solution(mesh):
    nx = EPG // 2
    nz = mesh.shape["ep"] // nx
    ny = mesh.shape["tp"] // 2

    def on_device(tokens, gain, bias, group_pick, member_pick, probs, gate, up, down):
        width = tokens.shape[1]
        half = gate.shape[2] // 2
        rows = nz * CAP
        all_rows = nx * rows
        vmem, dma = pltpu.VMEM, pltpu.SemaphoreType.DMA
        whole = pl.BlockSpec(memory_space=pltpu.VMEM)
        away = pl.BlockSpec(memory_space=pl.ANY)
        return pl.pallas_call(
            functools.partial(kernel, nz, nx, ny, width * 2 * ny),
            out_shape=pltpu.VMEM(tokens.shape, BF16),
            in_specs=[away] * 9,
            out_specs=whole,
            scratch_shapes=[
                vmem(tokens.shape, BF16),
                vmem((1, L), F32),
                vmem((1, L), F32),
                vmem((1, tokens.shape[0]), jnp.int32),
                vmem(member_pick.shape[::-1], jnp.int32),
                vmem(probs.shape[::-1], F32),
                dma((6,)),
                vmem((2, 2 * L, half), BF16),
                vmem((2, 2 * L, half), BF16),
                vmem((2, half, 2 * L), BF16),
                vmem((2, 1, L), F32),
                vmem((nz, CAP, 2 * L), F32),
                vmem((nz, CAP, 2 * L), F32),
                vmem((nx, 2, rows, L), BF16),
                vmem((nx, rows, L), BF16),
                vmem((ny, 2, 2 * L), F32),
                vmem((ny, 2, 2 * L), F32),
                vmem((2, L), F32),
                vmem((ny, 2, L), F32),
                vmem((ny, 2, all_rows, L), BF16),
                vmem((ny, 2, all_rows, L), BF16),
                vmem((ny, all_rows, L), BF16),
                vmem((nx, 2, rows, L), BF16),
                vmem((nx, 2, rows, L), BF16),
                vmem((nz, CAP, L), F32),
                vmem((nz, CAP, L), F32),
                dma((3,)),
                dma((5,)),
                dma((5,)),
                dma((nz,)),
                dma((nz,)),
                dma((nx,)),
                dma((nx,)),
                dma((2 * nx,)),
                dma((2 * nx,)),
                dma((ny,)),
                dma((ny,)),
                dma((ny,)),
                dma((ny,)),
                dma((ny,)),
                dma((ny,)),
                dma((ny,)),
                dma((ny,)),
                dma((2 * nx,)),
                dma((2 * nx,)),
                dma((nz,)),
                dma((nz,)),
            ],
            compiler_params=pltpu.CompilerParams(collective_id=0, has_side_effects=True),
        )(tokens, gain.reshape(1, -1), bias.reshape(1, -1), group_pick.T, member_pick.T, probs.T, gate, up, down)

    return jax.shard_map(
        on_device,
        mesh=mesh,
        in_specs=(
            P("ep", "tp"),
            P("tp"),
            P("tp"),
            P("ep", None),
            P("ep", None),
            P("ep", None),
            P("ep", "tp", None),
            P("ep", "tp", None),
            P("ep", None, "tp"),
        ),
        out_specs=P("ep", "tp"),
        check_vma=False,
    )
```

```python
import functools

import jax
import jax.numpy as jnp
from jax import lax
from jax.experimental import pallas as pl
from jax.experimental.pallas import tpu as pltpu
from jax.sharding import PartitionSpec as P

EPG = 8
CAP = 2
norm_epsilon = 1e-05
MESH = pl.DeviceIdType.MESH
F32 = jnp.float32
BF16 = jnp.bfloat16
L = 128


def iota(shape, axis):
    return lax.broadcasted_iota(jnp.int32, shape, axis)


def far_first(n):
    return sorted(range(1, n), key=lambda d: -min(d, n - d))


def kernel(
    nz, nx, ny, features,
    tok_hbm, gain_hbm, bias_hbm, gp_hbm, mp_hbm, pp_hbm, gate_hbm, up_hbm, down_hbm,
    out_ref,
    tok_ref, gain_ref, bias_ref, gp_ref, mp_ref, pp_ref,
    wgu, wd, gb,
    xt, xs, zt, zs, tr, sr, ax1s, ax1r, ax2s, ax2r, ps, pr, hb, os, rr,
    zready, yin, ygo, isem, lsem, wsem, ssem, rsem, psem, hsem,
):
    tokens = tok_ref.shape[0]
    half = wgu.shape[3]
    rows = nz * CAP
    per_plane = nx * CAP
    all_rows = nz * per_plane
    per_expert = ny // 2
    ep, tp = lax.axis_index("ep"), lax.axis_index("tp")
    z, x, y, c = ep // nx, ep % nx, tp // 2, tp % 2

    def dev(dz=0, dx=0, dy=0, dc=0):
        return {
            "ep": lax.rem(z + dz + nz, nz) * nx + lax.rem(x + dx + nx, nx),
            "tp": lax.rem(y + dy + ny, ny) * 2 + lax.rem(c + dc, 2),
        }

    def remote(src, dst, ss, rs, device):
        return pltpu.make_async_remote_copy(
            src_ref=src, dst_ref=dst, send_sem=ss, recv_sem=rs, device_id=device, device_id_type=MESH
        )

    def each(n, body):
        lax.fori_loop(1, n, lambda d, carry: (body(d), carry)[1], 0)

    def done(ref, sem):
        pltpu.make_async_copy(ref, ref, sem).wait()

    def signal(sem, device):
        pl.semaphore_signal(sem, inc=1, device_id=device, device_id_type=MESH)

    barrier = pltpu.get_barrier_semaphore()
    lax.fori_loop(
        z + 1, nz, lambda to, carry: (signal(barrier, {"ep": to * nx + x, "tp": tp}), carry)[1], 0
    )
    each(2 * nx, lambda k: signal(barrier, dev(dx=k // 2, dc=k % 2)))

    @pl.when(y == 0)
    def _():
        each(ny, lambda d: signal(barrier, dev(dy=d)))

    inputs = [
        pltpu.make_async_copy(src, dst, isem.at[i])
        for i, (src, dst) in enumerate(
            (
                (gp_hbm, gp_ref),
                (mp_hbm, mp_ref),
                (pp_hbm, pp_ref),
                (tok_hbm, tok_ref),
                (gain_hbm, gain_ref),
                (bias_hbm, bias_ref),
            )
        )
    ]
    for copy in inputs:
        copy.start()

    mine = pl.ds(pl.multiple_of(c * half, half), half)
    other = pl.ds(pl.multiple_of((1 - c) * half, half), half)
    pltpu.make_async_copy(gate_hbm.at[:, :, mine], wgu.at[0, :, 0:L, :], lsem.at[0]).start()
    pltpu.make_async_copy(up_hbm.at[:, :, mine], wgu.at[1, :, 0:L, :], lsem.at[0]).start()
    pltpu.make_async_copy(down_hbm.at[:, mine, :], wd.at[:, :, 0:L], lsem.at[1]).start()

    for copy in inputs:
        copy.wait()

    group = (gp_ref[...] - z + nz) % nz
    row = iota((rows, tokens), 0)
    lane = iota((rows, tokens), 1)
    member = (group == row // CAP).astype(F32)
    count = jnp.zeros((rows, tokens), F32)
    for t in range(tokens - 1):
        count = count + jnp.where(lane > t, member[:, t : t + 1], 0.0)
    rowwise = member * (count == (row % CAP).astype(F32)).astype(F32)
    probs = pp_ref[...]
    share = probs / jnp.sum(probs, axis=0, keepdims=True)
    top = probs.shape[0]
    table = [share[k : k + 1] for k in range(top)]
    table = table + [mp_ref[k : k + 1].astype(F32) for k in range(top)] + [rowwise]
    table = jnp.concatenate(table, axis=0)
    table = jnp.concatenate([table, jnp.zeros((2 * top + rows, L - tokens), F32)], axis=1)
    turned = jnp.transpose(table)[0:tokens, :]
    chosen = turned[:, 2 * top :]
    lane = iota((tokens, L), 1).astype(F32)
    shares = jnp.zeros((tokens, L), F32)
    for k in range(top):
        high = turned[:, k : k + 1].astype(BF16).astype(F32)
        low = turned[:, k : k + 1] - high
        pick = turned[:, top + k : top + k + 1]
        shares = shares + jnp.where(lane == pick, high, 0.0)
        shares = shares + jnp.where(lane == pick + EPG, low, 0.0)
    both = jnp.concatenate([tok_ref[...].astype(F32), shares], axis=1)
    packed = jnp.zeros((rows, 2 * L), F32)
    for t in range(tokens):
        packed = packed + rowwise[:, t : t + 1] * both[t : t + 1, :]
    xt[0] = packed[:, 0:L].astype(BF16)
    xs[0] = packed[:, L : 2 * L].astype(BF16)

    pl.semaphore_wait(barrier, (2 * nx - 1) + z + jnp.where(y > 0, 1, 0))
    lax.fori_loop(0, z, lambda to, carry: (signal(zready, {"ep": to * nx + x, "tp": tp}), carry)[1], 0)

    def x_copy(k):
        return remote(xt.at[0], xt.at[k], ssem.at[0], rsem.at[0], dev(dx=k // 2, dc=k % 2))

    def x_shares(dx):
        return remote(xs.at[0], xs.at[dx], ssem.at[1], rsem.at[1], dev(dx=dx))

    each(2 * nx, lambda k: x_copy(k).start())
    each(nx, lambda k: x_shares(k).start())

    @pl.when(y > 0)
    def _():
        signal(yin, {"ep": ep, "tp": c})

    to = dev(dc=1)
    remote(gain_ref, gb.at[0], wsem.at[0], wsem.at[1], to).start()
    remote(bias_ref, gb.at[1], wsem.at[0], wsem.at[1], to).start()
    remote(gate_hbm.at[:, :, other], wgu.at[0, :, L : 2 * L, :], wsem.at[2], wsem.at[3], to).start()
    remote(up_hbm.at[:, :, other], wgu.at[1, :, L : 2 * L, :], wsem.at[2], wsem.at[3], to).start()
    remote(down_hbm.at[:, other, :], wd.at[:, :, L : 2 * L], wsem.at[4], wsem.at[5], to).start()

    done(xt.at[pl.ds(1, 2 * nx - 1)], rsem.at[0])

    for dc in range(2):
        parts = [xt[2 * dx + dc].astype(F32) for dx in range(nx)]
        for d in range(nz):
            block = [part[d * CAP : (d + 1) * CAP, :] for part in parts]
            zt[d, :, dc * L : (dc + 1) * L] = jnp.concatenate(block, axis=0).astype(BF16)
    tr[0] = zt[0]

    @pl.when(z < nz - 1)
    def _():
        pl.semaphore_wait(zready, nz - 1 - z)


    def z_copy(d):
        return remote(zt.at[d], tr.at[d], ssem.at[2], rsem.at[2], dev(dz=d))

    def z_shares(d):
        return remote(zs.at[d], sr.at[d], ssem.at[3], rsem.at[3], dev(dz=d))

    for d in far_first(nz):
        z_copy(d).start()
    done(xs.at[pl.ds(1, nx - 1)], rsem.at[1])
    parts = [xs[dx].astype(F32) for dx in range(nx)]
    for d in range(nz):
        block = [part[d * CAP : (d + 1) * CAP, :] for part in parts]
        zs[d] = jnp.concatenate(block, axis=0).astype(BF16)
    sr[0] = zs[0]
    each(nz, lambda d: z_shares(d).start())

    @pl.when(y == 0)
    def _():
        pl.semaphore_wait(yin, ny - 1)
        each(ny, lambda d: signal(ygo, dev(dy=d)))

    done(wgu.at[:, :, 0:L, :], lsem.at[0])
    done(gb, wsem.at[1])
    done(wgu.at[:, :, L : 2 * L, :], wsem.at[3])
    gain = jnp.concatenate([gain_ref[...], gb[0]], axis=1)
    bias = jnp.concatenate([bias_ref[...], gb[1]], axis=1)
    gain_high = gain.astype(BF16).astype(F32)
    bias_high = bias.astype(BF16).astype(F32)
    four = iota((16, 2 * L), 0)
    vectors = jnp.where(four == 0, gain_high, 0.0) + jnp.where(four == 1, gain - gain_high, 0.0)
    vectors = vectors + jnp.where(four == 2, bias_high, 0.0) + jnp.where(four == 3, bias - bias_high, 0.0)
    vectors = vectors.astype(BF16)
    for e in range(2):
        for side in range(2):
            line = jnp.dot(vectors, wgu[side, e], preferred_element_type=F32)
            for j in range(per_expert):
                part = line[:, j * L : (j + 1) * L]
                ax1s[e * per_expert + j, 0:1, side * L : (side + 1) * L] = part[0:1] + part[1:2]
                ax1s[e * per_expert + j, 1:2, side * L : (side + 1) * L] = part[2:3] + part[3:4]
    ax1r[0] = ax1s[y]

    @pl.when(y > 0)
    def _():
        pl.semaphore_wait(ygo, 1)

    def a1_copy(d):
        return remote(ax1s.at[(y + d) % ny], ax1r.at[d], ssem.at[4], rsem.at[4], dev(dy=d))

    each(ny, lambda d: a1_copy(d).start())

    done(tr.at[pl.ds(1, nz - 1)], rsem.at[2])

    values = jnp.concatenate([tr[d].astype(F32) for d in range(nz)], axis=0)
    middle = jnp.sum(values, axis=1, keepdims=True) * (1.0 / (2 * L))
    values = values - middle
    scaled = (values * gain).astype(BF16)

    def p_copy(d):
        return remote(ps.at[d - 1], pr.at[d - 1], ssem.at[6], psem.at[d - 1], dev(dy=d))

    def a2_copy(d):
        return remote(ax2s.at[0], ax2r.at[d], ssem.at[5], rsem.at[5], dev(dy=d))

    gate_own = up_own = None
    for place, d in enumerate(far_first(ny) + [0]):
        q = (y + d) % ny
        e = q // per_expert
        cols = pl.ds(pl.multiple_of((q % per_expert) * L, L), L)
        gate_part = jnp.dot(scaled, wgu[0, e, :, cols], preferred_element_type=F32)
        up_part = jnp.dot(scaled, wgu[1, e, :, cols], preferred_element_type=F32)
        if d == 0:
            gate_own, up_own = gate_part, up_part
        else:
            ps[d - 1, 0] = gate_part.astype(BF16)
            ps[d - 1, 1] = up_part.astype(BF16)
            p_copy(d).start()
        if place == min(2, ny - 2):
            squares = jnp.sum(values * values, axis=1, keepdims=True)
            lanes = iota((all_rows, L), 1)
            columns = jnp.where(lanes == 0, middle, 0.0) + jnp.where(lanes == 1, squares, 0.0)
            columns = jnp.transpose(columns)
            ax2s[0, :, 0:all_rows] = columns[0:2, :]
            ax2r[0, :, 0:all_rows] = columns[0:2, :]
            each(ny, lambda d: a2_copy(d).start())

    done(sr.at[pl.ds(1, nz - 1)], rsem.at[3])
    expert = 2 * x + y // per_expert
    lanes = iota((all_rows, L), 1)
    share = jnp.concatenate([sr[d].astype(F32) for d in range(nz)], axis=0)
    share = jnp.sum(
        jnp.where((lanes == expert) | (lanes == expert + EPG), share, 0.0), axis=1, keepdims=True
    )
    done(ax1r.at[pl.ds(1, ny - 1)], rsem.at[4])
    done(ax2r.at[pl.ds(1, ny - 1)], rsem.at[5])
    means = [ax2r[d, 0:1, 0:all_rows] for d in range(ny)]
    center = sum(means) * (1.0 / ny)
    shifts = [m - center for m in means]
    spread = sum(ax2r[d, 1:2, 0:all_rows] for d in range(ny)) + (features // ny) * sum(s * s for s in shifts)
    scale = lax.rsqrt(spread * (1.0 / features) + norm_epsilon)
    stack = iota((16, all_rows), 0)
    table = jnp.where(stack == ny, scale, 0.0)
    for d in range(ny):
        table = table + jnp.where(stack == d, shifts[d], 0.0)
    table = jnp.transpose(table)
    scale = table[:, ny : ny + 1]
    gate, up = gate_own, up_own
    gate_bias = up_bias = jnp.zeros((1, L), F32)
    for d in range(ny):
        shift = table[:, d : d + 1]
        gate = gate + shift * ax1r[d, 0:1, 0:L]
        up = up + shift * ax1r[d, 0:1, L : 2 * L]
        gate_bias = gate_bias + ax1r[d, 1:2, 0:L]
        up_bias = up_bias + ax1r[d, 1:2, L : 2 * L]

    for d in sorted(range(1, ny), key=lambda d: min(d, ny - d)):
        p_copy(d).wait_recv()
        gate = gate + pr[d - 1, 0].astype(F32)
        up = up + pr[d - 1, 1].astype(F32)
    gate = gate * scale + gate_bias
    up = up * scale + up_bias
    hidden = (share * (gate / (1.0 + jnp.exp(-gate)) * up)).astype(BF16)
    hb[0] = hidden

    def h_copy(d):
        return remote(hb.at[0], hb.at[d], ssem.at[7], hsem.at[d - 1], dev(dy=d))

    for d in far_first(ny):
        h_copy(d).start()

    def down(d):
        q = (y - d + ny) % ny
        units = pl.ds(pl.multiple_of((q % per_expert) * L, L), L)
        return jnp.dot(hb[d], wd[q // per_expert, units, :], preferred_element_type=F32)

    done(wd.at[:, :, 0:L], lsem.at[1])
    done(wd.at[:, :, L : 2 * L], wsem.at[5])
    total = down(0)
    for d in sorted(range(1, ny), key=lambda d: min(d, ny - d)):
        h_copy(d).wait_recv()
        total = total + down(d)

    for d in range(nz):
        for k in range(2 * nx):
            dx, dc = k // 2, k % 2
            at = d * per_plane + dx * CAP
            os[d * 2 * nx + k] = total[at : at + CAP, dc * L : (dc + 1) * L].astype(BF16)
    rr[0] = os[0]

    back_z = [lax.rem(z - d + nz, nz) * nx for d in range(nz)]
    back_x = [lax.rem(x - d + nx, nx) for d in range(nx)]
    back_tp = [tp, tp + 1 - 2 * c]
    ring = lambda d, n: min(d, n - d)
    for i in sorted(
        range(1, 2 * nx * nz), key=lambda i: -ring(i // (2 * nx), nz) - ring(i // 2 % nx, nx)
    ):
        to = {"ep": back_z[i // (2 * nx)] + back_x[i // 2 % nx], "tp": back_tp[i % 2]}
        remote(os.at[i], rr.at[i], ssem.at[8], rsem.at[6], to).start()

    done(xt.at[pl.ds(1, 2 * nx - 1)], ssem.at[0])
    done(xs.at[pl.ds(1, nx - 1)], ssem.at[1])
    done(tr.at[pl.ds(1, nz - 1)], ssem.at[2])
    done(sr.at[pl.ds(1, nz - 1)], ssem.at[3])
    done(ax1r.at[pl.ds(1, ny - 1)], ssem.at[4])
    done(ax2r.at[pl.ds(1, ny - 1)], ssem.at[5])
    done(ps, ssem.at[6])
    done(hb.at[pl.ds(1, ny - 1)], ssem.at[7])
    done(gb, wsem.at[0])
    done(wgu.at[:, :, 0:L, :], wsem.at[2])
    done(wd.at[:, :, 0:L], wsem.at[4])
    done(rr.at[pl.ds(1, 2 * nx * nz - 1)], rsem.at[6])

    result = jnp.zeros((tokens, L), F32)
    for d in range(nz):
        back = rr[d * 2 * nx].astype(F32)
        for k in range(1, 2 * nx):
            back = back + rr[d * 2 * nx + k].astype(F32)
        for s in range(CAP):
            at = d * CAP + s
            result = result + chosen[:, at : at + 1] * back[s : s + 1, :]
    out_ref[...] = result.astype(BF16)
    done(os.at[pl.ds(1, 2 * nx * nz - 1)], ssem.at[8])


def solution(mesh):
    nx = EPG // 2
    nz = mesh.shape["ep"] // nx
    ny = mesh.shape["tp"] // 2

    def on_device(tokens, gain, bias, group_pick, member_pick, probs, gate, up, down):
        width = tokens.shape[1]
        half = gate.shape[2] // 2
        rows = nz * CAP
        all_rows = nx * rows
        vmem, dma = pltpu.VMEM, pltpu.SemaphoreType.DMA
        whole = pl.BlockSpec(memory_space=pltpu.VMEM)
        away = pl.BlockSpec(memory_space=pl.ANY)
        return pl.pallas_call(
            functools.partial(kernel, nz, nx, ny, width * 2 * ny),
            out_shape=pltpu.VMEM(tokens.shape, BF16),
            in_specs=[away] * 9,
            out_specs=whole,
            scratch_shapes=[
                vmem(tokens.shape, BF16),
                vmem((1, L), F32),
                vmem((1, L), F32),
                vmem((1, tokens.shape[0]), jnp.int32),
                vmem(member_pick.shape[::-1], jnp.int32),
                vmem(probs.shape[::-1], F32),
                vmem((2, 2, 2 * L, half), BF16),
                vmem((2, half, 2 * L), BF16),
                vmem((2, 1, L), F32),
                vmem((2 * nx, rows, L), BF16),
                vmem((nx, rows, L), BF16),
                vmem((nz, nx * CAP, 2 * L), BF16),
                vmem((nz, nx * CAP, L), BF16),
                vmem((nz, nx * CAP, 2 * L), BF16),
                vmem((nz, nx * CAP, L), BF16),
                vmem((ny, 2, 2 * L), F32),
                vmem((ny, 2, 2 * L), F32),
                vmem((1, 2, L), F32),
                vmem((ny, 2, L), F32),
                vmem((ny - 1, 2, all_rows, L), BF16),
                vmem((ny - 1, 2, all_rows, L), BF16),
                vmem((ny, all_rows, L), BF16),
                vmem((2 * nx * nz, CAP, L), BF16),
                vmem((2 * nx * nz, CAP, L), BF16),
                pltpu.SemaphoreType.REGULAR,
                pltpu.SemaphoreType.REGULAR,
                pltpu.SemaphoreType.REGULAR,
                dma((6,)),
                dma((2,)),
                dma((6,)),
                dma((9,)),
                dma((7,)),
                dma((ny - 1,)),
                dma((ny - 1,)),
            ],
            compiler_params=pltpu.CompilerParams(collective_id=0, has_side_effects=True),
        )(tokens, gain.reshape(1, -1), bias.reshape(1, -1), group_pick.T, member_pick.T, probs.T, gate, up, down)

    return jax.shard_map(
        on_device,
        mesh=mesh,
        in_specs=(
            P("ep", "tp"),
            P("tp"),
            P("tp"),
            P("ep", None),
            P("ep", None),
            P("ep", None),
            P("ep", "tp", None),
            P("ep", "tp", None),
            P("ep", None, "tp"),
        ),
        out_specs=P("ep", "tp"),
        check_vma=False,
    )
```

```python
import functools

import jax
import jax.numpy as jnp
from jax import lax
from jax.experimental import pallas as pl
from jax.experimental.pallas import tpu as pltpu
from jax.sharding import PartitionSpec as P

EPG = 8
CAP = 2
norm_epsilon = 1e-05
MESH = pl.DeviceIdType.MESH
F32 = jnp.float32
BF16 = jnp.bfloat16
L = 128


def iota(shape, axis):
    return lax.broadcasted_iota(jnp.int32, shape, axis)


def far_first(n):
    return sorted(range(1, n), key=lambda d: -min(d, n - d))


def kernel(
    nz, nx, ny, features,
    tok_hbm, gain_hbm, bias_hbm, gp_hbm, mp_hbm, pp_hbm, gate_hbm, up_hbm, down_hbm,
    out_ref,
    tok_ref, gain_ref, bias_ref, gp_ref, mp_ref, pp_ref,
    wgu, wd, gb,
    xt, xs, zs, tr, sr, ax1s, ax1r, ax2s, ax2r, ps, pr, hb, os, rr,
    zready, yready, isem, lsem, wsem, ssem, rsem, tsem, asem, psem, hsem,
):
    tokens = tok_ref.shape[0]
    half = wgu.shape[3]
    rows = nz * CAP
    per_plane = nx * CAP
    all_rows = nz * per_plane
    per_expert = ny // 2
    ep, tp = lax.axis_index("ep"), lax.axis_index("tp")
    z, x, y, c = ep // nx, ep % nx, tp // 2, tp % 2

    def dev(dz=0, dx=0, dy=0, dc=0):
        return {
            "ep": lax.rem(z + dz + nz, nz) * nx + lax.rem(x + dx + nx, nx),
            "tp": lax.rem(y + dy + ny, ny) * 2 + lax.rem(c + dc, 2),
        }

    def remote(src, dst, ss, rs, device):
        return pltpu.make_async_remote_copy(
            src_ref=src, dst_ref=dst, send_sem=ss, recv_sem=rs, device_id=device, device_id_type=MESH
        )

    def each(n, body):
        lax.fori_loop(1, n, lambda d, carry: (body(d), carry)[1], 0)

    def done(ref, sem):
        pltpu.make_async_copy(ref, ref, sem).wait()

    def signal(sem, device):
        pl.semaphore_signal(sem, inc=1, device_id=device, device_id_type=MESH)

    inputs = [
        pltpu.make_async_copy(src, dst, isem.at[i])
        for i, (src, dst) in enumerate(
            (
                (gp_hbm, gp_ref),
                (mp_hbm, mp_ref),
                (pp_hbm, pp_ref),
                (tok_hbm, tok_ref),
                (gain_hbm, gain_ref),
                (bias_hbm, bias_ref),
            )
        )
    ]
    for copy in inputs:
        copy.start()

    def planes(low, high, body):
        lax.fori_loop(low, high, lambda to, carry: (body(to), carry)[1], 0)

    part = nz // 2
    side = z // part
    first = side * part

    def ranked(r):
        return r + r // per_expert * (3 * per_expert - 1 - 2 * r)

    rank = ranked(y)
    barrier = pltpu.get_barrier_semaphore()

    def greet(to):
        signal(barrier, {"ep": to * nx + x, "tp": tp})

    planes(z + 1, first + part, greet)
    each(2 * nx, lambda k: signal(barrier, dev(dx=k // 2, dc=k % 2)))

    planes(rank + 1, ny, lambda r: signal(barrier, {"ep": ep, "tp": 2 * ranked(r) + c}))

    mine = pl.ds(pl.multiple_of(c * half, half), half)
    other = pl.ds(pl.multiple_of((1 - c) * half, half), half)
    pltpu.make_async_copy(gate_hbm.at[:, :, mine], wgu.at[0, :, 0:L, :], lsem.at[0]).start()
    pltpu.make_async_copy(up_hbm.at[:, :, mine], wgu.at[1, :, 0:L, :], lsem.at[0]).start()
    pltpu.make_async_copy(down_hbm.at[:, mine, :], wd.at[:, :, 0:L], lsem.at[1]).start()

    for copy in inputs:
        copy.wait()

    group = (gp_ref[...] - z + 1 + nz) % nz
    row = iota((rows, tokens), 0)
    lane = iota((rows, tokens), 1)
    member = (group == row // CAP).astype(F32)
    count = jnp.zeros((rows, tokens), F32)
    for t in range(tokens - 1):
        count = count + jnp.where(lane > t, member[:, t : t + 1], 0.0)
    rowwise = member * (count == (row % CAP).astype(F32)).astype(F32)
    def pack(source):
        packed = jnp.zeros((rows, L), F32)
        for t in range(tokens):
            packed = packed + rowwise[:, t : t + 1] * source[t : t + 1, :]
        return packed

    packed = pack(tok_ref[...].astype(F32))
    for d in range(nz):
        xt[0, d] = packed[d * CAP : (d + 1) * CAP, :].astype(BF16)
    tr[1, 0] = packed[CAP : 2 * CAP, :].astype(BF16)

    pl.semaphore_wait(barrier, (2 * nx - 1) + z + rank)
    planes(0, z, lambda to: signal(zready.at[z], {"ep": to * nx + x, "tp": tp}))
    planes(0, rank, lambda r: signal(yready, {"ep": ep, "tp": 2 * ranked(r) + c}))

    @pl.when(side == 0)
    def _():
        planes(part, nz, greet)

    def x_copy(k):
        return remote(xt.at[0], xt.at[k], ssem.at[0], rsem.at[0], dev(dx=k // 2, dc=k % 2))

    def x_shares(dx):
        return remote(xs.at[0], xs.at[dx], ssem.at[1], rsem.at[1], dev(dx=dx))

    each(2 * nx, lambda k: x_copy(k).start())

    go_x = [lax.rem(x + d, nx) for d in range(nx)]
    go_tp = [tp, tp + 1 - 2 * c]

    def straight(to):
        i = lax.rem(to - z + 1 + nz, nz)
        for k in range(2 * nx):
            device = {"ep": to * nx + go_x[k // 2], "tp": go_tp[k % 2]}
            remote(xt.at[0, i], tr.at[i, k], ssem.at[2], tsem.at[i // part], device).start()

    @pl.when(side == 1)
    def _():
        planes(0, part, straight)

    to = dev(dc=1)
    remote(gain_ref, gb.at[0], wsem.at[0], wsem.at[1], to).start()
    remote(bias_ref, gb.at[1], wsem.at[0], wsem.at[1], to).start()
    remote(gate_hbm.at[:, :, other], wgu.at[0, :, L : 2 * L, :], wsem.at[2], wsem.at[3], to).start()
    remote(up_hbm.at[:, :, other], wgu.at[1, :, L : 2 * L, :], wsem.at[2], wsem.at[3], to).start()
    remote(down_hbm.at[:, other, :], wd.at[:, :, L : 2 * L], wsem.at[4], wsem.at[5], to).start()

    probs = pp_ref[...]
    share = probs / jnp.sum(probs, axis=0, keepdims=True)
    top = probs.shape[0]
    table = [share[k : k + 1] for k in range(top)]
    table = table + [mp_ref[k : k + 1].astype(F32) for k in range(top)] + [rowwise]
    table = jnp.concatenate(table, axis=0)
    table = jnp.concatenate([table, jnp.zeros((2 * top + rows, L - tokens), F32)], axis=1)
    turned = jnp.transpose(table)[0:tokens, :]
    chosen = turned[:, 2 * top :]
    lane = iota((tokens, L), 1).astype(F32)
    shares = jnp.zeros((tokens, L), F32)
    for k in range(top):
        high = turned[:, k : k + 1].astype(BF16).astype(F32)
        low = turned[:, k : k + 1] - high
        pick = turned[:, top + k : top + k + 1]
        shares = shares + jnp.where(lane == pick, high, 0.0)
        shares = shares + jnp.where(lane == pick + EPG, low, 0.0)
    xs[0] = pack(shares).astype(BF16)
    each(nx, lambda k: x_shares(k).start())

    done(wgu.at[:, :, 0:L, :], lsem.at[0])
    done(gb, wsem.at[1])
    done(wgu.at[:, :, L : 2 * L, :], wsem.at[3])
    gain = jnp.concatenate([gain_ref[...], gb[0]], axis=1)
    bias = jnp.concatenate([bias_ref[...], gb[1]], axis=1)
    gain_high = gain.astype(BF16).astype(F32)
    bias_high = bias.astype(BF16).astype(F32)
    four = iota((16, 2 * L), 0)
    vectors = jnp.where(four == 0, gain_high, 0.0) + jnp.where(four == 1, gain - gain_high, 0.0)
    vectors = vectors + jnp.where(four == 2, bias_high, 0.0) + jnp.where(four == 3, bias - bias_high, 0.0)
    vectors = vectors.astype(BF16)
    for e in range(2):
        for g in range(2):
            line = jnp.dot(vectors, wgu[g, e], preferred_element_type=F32)
            for j in range(per_expert):
                piece = line[:, j * L : (j + 1) * L]
                ax1s[e * per_expert + j, 0:1, g * L : (g + 1) * L] = piece[0:1] + piece[1:2]
                ax1s[e * per_expert + j, 1:2, g * L : (g + 1) * L] = piece[2:3] + piece[3:4]
    ax1r[0] = ax1s[y]

    done(xt.at[pl.ds(1, 2 * nx - 1)], rsem.at[0])

    for k in range(1, 2 * nx):
        tr[1, k] = xt[k, 1]

    def z_copy(to):
        i = lax.rem(to - z + 1 + nz, nz)
        device = {"ep": to * nx + x, "tp": tp}
        remote(xt.at[:, i], tr.at[i], ssem.at[2], tsem.at[i // part], device).start()

    def z_ready_copy(to):
        pl.semaphore_wait(zready.at[to], 1)
        z_copy(to)

    planes(first, z, z_copy)
    planes(z + 1, first + part, z_ready_copy)

    @pl.when(side == 0)
    def _():
        planes(part, nz, z_ready_copy)

    def z_shares(d):
        i = lax.rem(d + 1, nz)
        return remote(zs.at[i], sr.at[i], ssem.at[3], rsem.at[3], dev(dz=d))

    done(xs.at[pl.ds(1, nx - 1)], rsem.at[1])
    blocks = [xs[dx].astype(F32) for dx in range(nx)]
    for d in range(nz):
        block = [b[d * CAP : (d + 1) * CAP, :] for b in blocks]
        zs[d] = jnp.concatenate(block, axis=0).astype(BF16)
    sr[1] = zs[1]
    each(nz, lambda d: z_shares(d).start())

    @pl.when(rank < ny - 1)
    def _():
        pl.semaphore_wait(yready, ny - 1 - rank)

    def a1_copy(d):
        return remote(ax1s.at[(y + d) % ny], ax1r.at[d], ssem.at[4], rsem.at[4], dev(dy=d))

    each(ny, lambda d: a1_copy(d).start())

    batch_rows = all_rows // 2
    own_batch = 1 // part

    def p_copy(b, d):
        return remote(ps.at[b, d - 1], pr.at[b, d - 1], ssem.at[6], psem.at[b, d - 1], dev(dy=d))

    def a2_copy(b, d):
        return remote(ax2s.at[b], ax2r.at[b, d], ssem.at[5], asem.at[b], dev(dy=d))

    gate_own, up_own = [], []
    for b in range(2):
        here = part - 1 if b == own_batch else part
        if here:
            done(tr.at[pl.ds(b * part, here)], tsem.at[b])

        slots = range(b * part, b * part + part)
        values = [
            jnp.concatenate([tr[i, 2 * dx + dc].astype(F32) for i in slots for dx in range(nx)], axis=0)
            for dc in range(2)
        ]
        values = jnp.concatenate(values, axis=1)
        middle = jnp.sum(values, axis=1, keepdims=True) * (1.0 / (2 * L))
        values = values - middle
        scaled = (values * gain).astype(BF16)
        for place, d in enumerate(far_first(ny) + [0]):
            q = (y + d) % ny
            e = q // per_expert
            cols = pl.ds(pl.multiple_of((q % per_expert) * L, L), L)
            gate_part = jnp.dot(scaled, wgu[0, e, :, cols], preferred_element_type=F32)
            up_part = jnp.dot(scaled, wgu[1, e, :, cols], preferred_element_type=F32)
            if d == 0:
                gate_own.append(gate_part)
                up_own.append(up_part)
            else:
                ps[b, d - 1, 0] = gate_part.astype(BF16)
                ps[b, d - 1, 1] = up_part.astype(BF16)
                p_copy(b, d).start()
            if place == 0:
                squares = jnp.sum(values * values, axis=1, keepdims=True)
                lanes = iota((batch_rows, L), 1)
                columns = jnp.where(lanes == 0, middle, 0.0) + jnp.where(lanes == 1, squares, 0.0)
                columns = jnp.transpose(columns)
                ax2s[b, :, 0:batch_rows] = columns[0:2, :]
                ax2r[b, 0, :, 0:batch_rows] = columns[0:2, :]
                each(ny, lambda d: a2_copy(b, d).start())

    def h_copy(b, d):
        return remote(hb.at[b, 0], hb.at[b, d], ssem.at[7], hsem.at[b, d - 1], dev(dy=d))

    done(sr.at[pl.ds(1, nz - 1)], rsem.at[3])
    done(ax1r.at[pl.ds(1, ny - 1)], rsem.at[4])
    expert = 2 * x + y // per_expert
    lanes = iota((batch_rows, L), 1)
    gate_bias = up_bias = jnp.zeros((1, L), F32)
    for d in range(ny):
        gate_bias = gate_bias + ax1r[d, 1:2, 0:L]
        up_bias = up_bias + ax1r[d, 1:2, L : 2 * L]
    for b in range(2):
        share = jnp.concatenate([sr[i].astype(F32) for i in range(b * part, b * part + part)], axis=0)
        share = jnp.sum(
            jnp.where((lanes == expert) | (lanes == expert + EPG), share, 0.0), axis=1, keepdims=True
        )
        done(ax2r.at[b, pl.ds(1, ny - 1)], asem.at[b])
        means = [ax2r[b, d, 0:1, 0:batch_rows] for d in range(ny)]
        center = sum(means) * (1.0 / ny)
        shifts = [m - center for m in means]
        spread = sum(ax2r[b, d, 1:2, 0:batch_rows] for d in range(ny))
        spread = spread + (features // ny) * sum(s * s for s in shifts)
        scale = lax.rsqrt(spread * (1.0 / features) + norm_epsilon)
        stack = iota((16, batch_rows), 0)
        table = jnp.where(stack == ny, scale, 0.0)
        for d in range(ny):
            table = table + jnp.where(stack == d, shifts[d], 0.0)
        table = jnp.transpose(table)
        scale = table[:, ny : ny + 1]
        gate, up = gate_own[b], up_own[b]
        for d in range(ny):
            shift = table[:, d : d + 1]
            gate = gate + shift * ax1r[d, 0:1, 0:L]
            up = up + shift * ax1r[d, 0:1, L : 2 * L]
        for d in sorted(range(1, ny), key=lambda d: min(d, ny - d)):
            p_copy(b, d).wait_recv()
            gate = gate + pr[b, d - 1, 0].astype(F32)
            up = up + pr[b, d - 1, 1].astype(F32)
        gate = gate * scale + gate_bias
        up = up * scale + up_bias
        hb[b, 0] = (share * (gate / (1.0 + jnp.exp(-gate)) * up)).astype(BF16)
        for d in far_first(ny):
            h_copy(b, d).start()

    def down(b, d):
        q = (y - d + ny) % ny
        units = pl.ds(pl.multiple_of((q % per_expert) * L, L), L)
        return jnp.dot(hb[b, d], wd[q // per_expert, units, :], preferred_element_type=F32)

    done(wd.at[:, :, 0:L], lsem.at[1])
    done(wd.at[:, :, L : 2 * L], wsem.at[5])

    back_z = [lax.rem(z - i + 1 + nz, nz) * nx for i in range(nz)]
    back_x = [lax.rem(x - d + nx, nx) for d in range(nx)]
    back_tp = [tp, tp + 1 - 2 * c]
    mine = 2 * nx

    def ring(d, n):
        return min(d % n, n - d % n)

    for b in range(2):
        total = down(b, 0)
        for d in sorted(range(1, ny), key=lambda d: min(d, ny - d)):
            h_copy(b, d).wait_recv()
            total = total + down(b, d)
        places = range(b * part * 2 * nx, (b + 1) * part * 2 * nx)
        for i in places:
            at = (i // (2 * nx) - b * part) * per_plane + (i // 2 % nx) * CAP
            os[i] = total[at : at + CAP, (i % 2) * L : (i % 2 + 1) * L].astype(BF16)
            if i == mine:
                rr[i] = total[at : at + CAP, 0:L].astype(BF16)
        for i in sorted(places, key=lambda i: -ring(i // (2 * nx) - 1, nz) - ring(i // 2 % nx, nx)):
            if i != mine:
                to = {"ep": back_z[i // (2 * nx)] + back_x[i // 2 % nx], "tp": back_tp[i % 2]}
                remote(os.at[i], rr.at[i], ssem.at[8], rsem.at[6], to).start()

    done(xt.at[pl.ds(1, 2 * nx - 1)], ssem.at[0])
    done(xs.at[pl.ds(1, nx - 1)], ssem.at[1])
    done(tr.at[pl.ds(1, nz - 1)], ssem.at[2])
    done(sr.at[pl.ds(1, nz - 1)], ssem.at[3])
    done(ax1r.at[pl.ds(1, ny - 1)], ssem.at[4])
    done(ax2r.at[:, pl.ds(1, ny - 1)], ssem.at[5])
    done(ps, ssem.at[6])
    done(hb.at[:, pl.ds(1, ny - 1)], ssem.at[7])
    done(gb, wsem.at[0])
    done(wgu.at[:, :, 0:L, :], wsem.at[2])
    done(wd.at[:, :, 0:L], wsem.at[4])
    done(rr.at[pl.ds(1, 2 * nx * nz - 1)], rsem.at[6])

    result = jnp.zeros((tokens, L), F32)
    for d in range(nz):
        back = rr[d * 2 * nx].astype(F32)
        for k in range(1, 2 * nx):
            back = back + rr[d * 2 * nx + k].astype(F32)
        for s in range(CAP):
            at = d * CAP + s
            result = result + chosen[:, at : at + 1] * back[s : s + 1, :]
    out_ref[...] = result.astype(BF16)
    done(os.at[pl.ds(1, 2 * nx * nz - 1)], ssem.at[8])


def solution(mesh):
    nx = EPG // 2
    nz = mesh.shape["ep"] // nx
    ny = mesh.shape["tp"] // 2

    def on_device(tokens, gain, bias, group_pick, member_pick, probs, gate, up, down):
        width = tokens.shape[1]
        half = gate.shape[2] // 2
        rows = nz * CAP
        all_rows = nx * rows
        vmem, dma = pltpu.VMEM, pltpu.SemaphoreType.DMA
        whole = pl.BlockSpec(memory_space=pltpu.VMEM)
        away = pl.BlockSpec(memory_space=pl.ANY)
        return pl.pallas_call(
            functools.partial(kernel, nz, nx, ny, width * 2 * ny),
            out_shape=pltpu.VMEM(tokens.shape, BF16),
            in_specs=[away] * 9,
            out_specs=whole,
            scratch_shapes=[
                vmem(tokens.shape, BF16),
                vmem((1, L), F32),
                vmem((1, L), F32),
                vmem((1, tokens.shape[0]), jnp.int32),
                vmem(member_pick.shape[::-1], jnp.int32),
                vmem(probs.shape[::-1], F32),
                vmem((2, 2, 2 * L, half), BF16),
                vmem((2, half, 2 * L), BF16),
                vmem((2, 1, L), F32),
                vmem((2 * nx, nz, CAP, L), BF16),
                vmem((nx, rows, L), BF16),
                vmem((nz, nx * CAP, L), BF16),
                vmem((nz, 2 * nx, CAP, L), BF16),
                vmem((nz, nx * CAP, L), BF16),
                vmem((ny, 2, 2 * L), F32),
                vmem((ny, 2, 2 * L), F32),
                vmem((2, 2, L), F32),
                vmem((2, ny, 2, L), F32),
                vmem((2, ny - 1, 2, all_rows // 2, L), BF16),
                vmem((2, ny - 1, 2, all_rows // 2, L), BF16),
                vmem((2, ny, all_rows // 2, L), BF16),
                vmem((2 * nx * nz, CAP, L), BF16),
                vmem((2 * nx * nz, CAP, L), BF16),
                pltpu.SemaphoreType.REGULAR((nz,)),
                pltpu.SemaphoreType.REGULAR,
                dma((6,)),
                dma((2,)),
                dma((6,)),
                dma((9,)),
                dma((7,)),
                dma((2,)),
                dma((2,)),
                dma((2, ny - 1)),
                dma((2, ny - 1)),
            ],
            compiler_params=pltpu.CompilerParams(collective_id=0, has_side_effects=True),
        )(tokens, gain.reshape(1, -1), bias.reshape(1, -1), group_pick.T, member_pick.T, probs.T, gate, up, down)

    return jax.shard_map(
        on_device,
        mesh=mesh,
        in_specs=(
            P("ep", "tp"),
            P("tp"),
            P("tp"),
            P("ep", None),
            P("ep", None),
            P("ep", None),
            P("ep", "tp", None),
            P("ep", "tp", None),
            P("ep", None, "tp"),
        ),
        out_specs=P("ep", "tp"),
        check_vma=False,
    )
```

```python
import functools

import jax
import jax.numpy as jnp
from jax import lax
from jax.experimental import pallas as pl
from jax.experimental.pallas import tpu as pltpu
from jax.sharding import PartitionSpec as P

EPG = 8
CAP = 2
norm_epsilon = 1e-05
MESH = pl.DeviceIdType.MESH
F32 = jnp.float32
BF16 = jnp.bfloat16
L = 128


def iota(shape, axis):
    return lax.broadcasted_iota(jnp.int32, shape, axis)


def far_first(n):
    return sorted(range(1, n), key=lambda d: -min(d, n - d))


def kernel(
    nz, nx, ny, features,
    tok_hbm, gain_hbm, bias_hbm, gp_hbm, mp_hbm, pp_hbm, gate_hbm, up_hbm, down_hbm,
    out_ref,
    tok_ref, gain_ref, bias_ref, gp_ref, mp_ref, pp_ref,
    wgu, wd, gb,
    xt, xs, zs, tr, sr, ax1s, ax1r, ax2s, ax2r, ps, pr, hb, os, rr,
    zready, yready, isem, lsem, wsem, ssem, rsem, tsem, asem, psem, hsem,
):
    tokens = tok_ref.shape[0]
    half = wgu.shape[3]
    rows = nz * CAP
    per_plane = nx * CAP
    all_rows = nz * per_plane
    per_expert = ny // 2
    ep, tp = lax.axis_index("ep"), lax.axis_index("tp")
    z, x, y, c = ep // nx, ep % nx, tp // 2, tp % 2

    def dev(dz=0, dx=0, dy=0, dc=0):
        return {
            "ep": lax.rem(z + dz + nz, nz) * nx + lax.rem(x + dx + nx, nx),
            "tp": lax.rem(y + dy + ny, ny) * 2 + lax.rem(c + dc, 2),
        }

    def remote(src, dst, ss, rs, device):
        return pltpu.make_async_remote_copy(
            src_ref=src, dst_ref=dst, send_sem=ss, recv_sem=rs, device_id=device, device_id_type=MESH
        )

    def each(n, body):
        lax.fori_loop(1, n, lambda d, carry: (body(d), carry)[1], 0)

    def done(ref, sem):
        pltpu.make_async_copy(ref, ref, sem).wait()

    def signal(sem, device):
        pl.semaphore_signal(sem, inc=1, device_id=device, device_id_type=MESH)

    inputs = [
        pltpu.make_async_copy(src, dst, isem.at[i])
        for i, (src, dst) in enumerate(
            (
                (gp_hbm, gp_ref),
                (mp_hbm, mp_ref),
                (pp_hbm, pp_ref),
                (tok_hbm, tok_ref),
                (gain_hbm, gain_ref),
                (bias_hbm, bias_ref),
            )
        )
    ]
    for copy in inputs:
        copy.start()

    def planes(low, high, body):
        lax.fori_loop(low, high, lambda to, carry: (body(to), carry)[1], 0)

    part = nz // 2
    side = z // part
    first = side * part

    def ranked(r):
        return r + r // per_expert * (3 * per_expert - 1 - 2 * r)

    rank = ranked(y)
    barrier = pltpu.get_barrier_semaphore()

    def greet(to):
        signal(barrier, {"ep": to * nx + x, "tp": tp})

    planes(z + 1, first + part, greet)
    each(2 * nx, lambda k: signal(barrier, dev(dx=k // 2, dc=k % 2)))

    planes(rank + 1, ny, lambda r: signal(barrier, {"ep": ep, "tp": 2 * ranked(r) + c}))

    mine = pl.ds(pl.multiple_of(c * half, half), half)
    other = pl.ds(pl.multiple_of((1 - c) * half, half), half)
    pltpu.make_async_copy(gate_hbm.at[:, :, mine], wgu.at[0, :, 0:L, :], lsem.at[0]).start()
    pltpu.make_async_copy(up_hbm.at[:, :, mine], wgu.at[1, :, 0:L, :], lsem.at[0]).start()
    pltpu.make_async_copy(down_hbm.at[:, mine, :], wd.at[:, :, 0:L], lsem.at[1]).start()

    for copy in inputs:
        copy.wait()

    group = (gp_ref[...] - z + 1 + nz) % nz
    row = iota((rows, tokens), 0)
    lane = iota((rows, tokens), 1)
    member = (group == row // CAP).astype(F32)
    count = jnp.zeros((rows, tokens), F32)
    for t in range(tokens - 1):
        count = count + jnp.where(lane > t, member[:, t : t + 1], 0.0)
    rowwise = member * (count == (row % CAP).astype(F32)).astype(F32)
    def pack(source):
        packed = jnp.zeros((rows, L), F32)
        for t in range(tokens):
            packed = packed + rowwise[:, t : t + 1] * source[t : t + 1, :]
        return packed

    packed = pack(tok_ref[...].astype(F32))
    for d in range(nz):
        xt[0, d] = packed[d * CAP : (d + 1) * CAP, :].astype(BF16)
    tr[1, 0] = packed[CAP : 2 * CAP, :].astype(BF16)

    pl.semaphore_wait(barrier, (2 * nx - 1) + z + rank)
    planes(0, z, lambda to: signal(zready.at[z], {"ep": to * nx + x, "tp": tp}))
    planes(0, rank, lambda r: signal(yready, {"ep": ep, "tp": 2 * ranked(r) + c}))

    @pl.when(side == 0)
    def _():
        planes(part, nz, greet)

    def x_copy(k):
        return remote(xt.at[0], xt.at[k], ssem.at[0], rsem.at[0], dev(dx=k // 2, dc=k % 2))

    def x_shares(dx):
        return remote(xs.at[0], xs.at[dx], ssem.at[1], rsem.at[1], dev(dx=dx))

    each(2 * nx, lambda k: x_copy(k).start())

    go_x = [lax.rem(x + d, nx) for d in range(nx)]
    go_tp = [tp, tp + 1 - 2 * c]

    def straight(to):
        i = lax.rem(to - z + 1 + nz, nz)
        for k in range(2 * nx):
            device = {"ep": to * nx + go_x[k // 2], "tp": go_tp[k % 2]}
            remote(xt.at[0, i], tr.at[i, k], ssem.at[2], tsem.at[i // part], device).start()

    @pl.when(side == 1)
    def _():
        planes(0, part, straight)

    to = dev(dc=1)
    remote(gain_ref, gb.at[0], wsem.at[0], wsem.at[1], to).start()
    remote(bias_ref, gb.at[1], wsem.at[0], wsem.at[1], to).start()
    remote(gate_hbm.at[:, :, other], wgu.at[0, :, L : 2 * L, :], wsem.at[2], wsem.at[3], to).start()
    remote(up_hbm.at[:, :, other], wgu.at[1, :, L : 2 * L, :], wsem.at[2], wsem.at[3], to).start()
    remote(down_hbm.at[:, other, :], wd.at[:, :, L : 2 * L], wsem.at[4], wsem.at[5], to).start()

    probs = pp_ref[...]
    share = probs / jnp.sum(probs, axis=0, keepdims=True)
    top = probs.shape[0]
    table = [share[k : k + 1] for k in range(top)]
    table = table + [mp_ref[k : k + 1].astype(F32) for k in range(top)] + [rowwise]
    table = jnp.concatenate(table, axis=0)
    table = jnp.concatenate([table, jnp.zeros((2 * top + rows, L - tokens), F32)], axis=1)
    turned = jnp.transpose(table)[0:tokens, :]
    chosen = turned[:, 2 * top :]
    lane = iota((tokens, L), 1).astype(F32)
    shares = jnp.zeros((tokens, L), F32)
    for k in range(top):
        high = turned[:, k : k + 1].astype(BF16).astype(F32)
        low = turned[:, k : k + 1] - high
        pick = turned[:, top + k : top + k + 1]
        shares = shares + jnp.where(lane == pick, high, 0.0)
        shares = shares + jnp.where(lane == pick + EPG, low, 0.0)
    xs[0] = pack(shares).astype(BF16)
    each(nx, lambda k: x_shares(k).start())

    done(wgu.at[:, :, 0:L, :], lsem.at[0])
    done(gb, wsem.at[1])
    done(wgu.at[:, :, L : 2 * L, :], wsem.at[3])
    gain = jnp.concatenate([gain_ref[...], gb[0]], axis=1)
    bias = jnp.concatenate([bias_ref[...], gb[1]], axis=1)
    gain_high = gain.astype(BF16).astype(F32)
    bias_high = bias.astype(BF16).astype(F32)
    four = iota((16, 2 * L), 0)
    vectors = jnp.where(four == 0, gain_high, 0.0) + jnp.where(four == 1, gain - gain_high, 0.0)
    vectors = vectors + jnp.where(four == 2, bias_high, 0.0) + jnp.where(four == 3, bias - bias_high, 0.0)
    vectors = vectors.astype(BF16)
    for e in range(2):
        for g in range(2):
            line = jnp.dot(vectors, wgu[g, e], preferred_element_type=F32)
            for j in range(per_expert):
                piece = line[:, j * L : (j + 1) * L]
                ax1s[e * per_expert + j, 0:1, g * L : (g + 1) * L] = piece[0:1] + piece[1:2]
                ax1s[e * per_expert + j, 1:2, g * L : (g + 1) * L] = piece[2:3] + piece[3:4]
    ax1r[0] = ax1s[y]

    done(xt.at[pl.ds(1, 2 * nx - 1)], rsem.at[0])

    for k in range(1, 2 * nx):
        tr[1, k] = xt[k, 1]

    def z_copy(to):
        i = lax.rem(to - z + 1 + nz, nz)
        device = {"ep": to * nx + x, "tp": tp}
        remote(xt.at[:, i], tr.at[i], ssem.at[2], tsem.at[i // part], device).start()

    def z_ready_copy(to):
        pl.semaphore_wait(zready.at[to], 1)
        z_copy(to)

    planes(first, z, z_copy)
    planes(z + 1, nz, z_ready_copy)

    def z_shares(d):
        i = lax.rem(d + 1, nz)
        return remote(zs.at[i], sr.at[i], ssem.at[3], rsem.at[3], dev(dz=d))

    done(xs.at[pl.ds(1, nx - 1)], rsem.at[1])
    blocks = [xs[dx].astype(F32) for dx in range(nx)]
    for d in range(nz):
        block = [b[d * CAP : (d + 1) * CAP, :] for b in blocks]
        zs[d] = jnp.concatenate(block, axis=0).astype(BF16)
    sr[1] = zs[1]
    each(nz, lambda d: z_shares(d).start())

    @pl.when(rank < ny - 1)
    def _():
        pl.semaphore_wait(yready, ny - 1 - rank)

    def a1_copy(d):
        return remote(ax1s.at[(y + d) % ny], ax1r.at[d], ssem.at[4], rsem.at[4], dev(dy=d))

    each(ny, lambda d: a1_copy(d).start())

    batch_rows = all_rows // 2
    own_batch = 1 // part

    def p_copy(b, d):
        return remote(ps.at[b, d - 1], pr.at[b, d - 1], ssem.at[6], psem.at[b, d - 1], dev(dy=d))

    def a2_copy(b, d):
        return remote(ax2s.at[b], ax2r.at[b, d], ssem.at[5], asem.at[b], dev(dy=d))

    gate_own, up_own = [], []
    far = [d for d in far_first(ny) if min(d, ny - d) > 2]
    held = []
    for b in range(2):
        here = part - 1 if b == own_batch else part
        if here:
            done(tr.at[pl.ds(b * part, here)], tsem.at[b])

        slots = range(b * part, b * part + part)
        values = [
            jnp.concatenate([tr[i, 2 * dx + dc].astype(F32) for i in slots for dx in range(nx)], axis=0)
            for dc in range(2)
        ]
        values = jnp.concatenate(values, axis=1)
        middle = jnp.sum(values, axis=1, keepdims=True) * (1.0 / (2 * L))
        values = values - middle
        scaled = (values * gain).astype(BF16)
        for place, d in enumerate(far_first(ny) + [0]):
            q = (y + d) % ny
            e = q // per_expert
            cols = pl.ds(pl.multiple_of((q % per_expert) * L, L), L)
            gate_part = jnp.dot(scaled, wgu[0, e, :, cols], preferred_element_type=F32)
            up_part = jnp.dot(scaled, wgu[1, e, :, cols], preferred_element_type=F32)
            if d == 0:
                gate_own.append(gate_part)
                up_own.append(up_part)
            else:
                ps[b, d - 1, 0] = gate_part.astype(BF16)
                ps[b, d - 1, 1] = up_part.astype(BF16)
                if b == 1 and d not in far:
                    while held:
                        p_copy(0, held.pop(0)).start()
                if b == 1 or d in far:
                    p_copy(b, d).start()
                else:
                    held.append(d)
            if place == 0:
                squares = jnp.sum(values * values, axis=1, keepdims=True)
                lanes = iota((batch_rows, L), 1)
                columns = jnp.where(lanes == 0, middle, 0.0) + jnp.where(lanes == 1, squares, 0.0)
                columns = jnp.transpose(columns)
                ax2s[b, :, 0:batch_rows] = columns[0:2, :]
                ax2r[b, 0, :, 0:batch_rows] = columns[0:2, :]
                each(ny, lambda d: a2_copy(b, d).start())

    def h_copy(b, d):
        return remote(hb.at[b, 0], hb.at[b, d], ssem.at[7], hsem.at[b, d - 1], dev(dy=d))

    done(sr.at[pl.ds(1, nz - 1)], rsem.at[3])
    done(ax1r.at[pl.ds(1, ny - 1)], rsem.at[4])
    expert = 2 * x + y // per_expert
    lanes = iota((batch_rows, L), 1)
    gate_bias = up_bias = jnp.zeros((1, L), F32)
    for d in range(ny):
        gate_bias = gate_bias + ax1r[d, 1:2, 0:L]
        up_bias = up_bias + ax1r[d, 1:2, L : 2 * L]
    ready = []
    for b in range(2):
        share = jnp.concatenate([sr[i].astype(F32) for i in range(b * part, b * part + part)], axis=0)
        share = jnp.sum(
            jnp.where((lanes == expert) | (lanes == expert + EPG), share, 0.0), axis=1, keepdims=True
        )
        done(ax2r.at[b, pl.ds(1, ny - 1)], asem.at[b])
        means = [ax2r[b, d, 0:1, 0:batch_rows] for d in range(ny)]
        center = sum(means) * (1.0 / ny)
        shifts = [m - center for m in means]
        spread = sum(ax2r[b, d, 1:2, 0:batch_rows] for d in range(ny))
        spread = spread + (features // ny) * sum(s * s for s in shifts)
        scale = lax.rsqrt(spread * (1.0 / features) + norm_epsilon)
        stack = iota((16, batch_rows), 0)
        table = jnp.where(stack == ny, scale, 0.0)
        for d in range(ny):
            table = table + jnp.where(stack == d, shifts[d], 0.0)
        table = jnp.transpose(table)
        scale = table[:, ny : ny + 1]
        gate, up = gate_own[b], up_own[b]
        for d in range(ny):
            shift = table[:, d : d + 1]
            gate = gate + shift * ax1r[d, 0:1, 0:L]
            up = up + shift * ax1r[d, 0:1, L : 2 * L]
        ready.append((gate, up, scale, share))
    for b in range(2):
        gate, up, scale, share = ready[b]
        for d in far_first(ny):
            p_copy(b, d).wait_recv()
            gate = gate + pr[b, d - 1, 0].astype(F32)
            up = up + pr[b, d - 1, 1].astype(F32)
        gate = gate * scale + gate_bias
        up = up * scale + up_bias
        hb[b, 0] = (share * (gate / (1.0 + jnp.exp(-gate)) * up)).astype(BF16)
        for d in far_first(ny):
            h_copy(b, d).start()

    def down(b, d):
        q = (y - d + ny) % ny
        units = pl.ds(pl.multiple_of((q % per_expert) * L, L), L)
        return jnp.dot(hb[b, d], wd[q // per_expert, units, :], preferred_element_type=F32)

    done(wd.at[:, :, 0:L], lsem.at[1])
    done(wd.at[:, :, L : 2 * L], wsem.at[5])

    back_z = [lax.rem(z - i + 1 + nz, nz) * nx for i in range(nz)]
    back_x = [lax.rem(x - d + nx, nx) for d in range(nx)]
    back_tp = [tp, tp + 1 - 2 * c]
    mine = 2 * nx

    def ring(d, n):
        return min(d % n, n - d % n)

    for b in range(2):
        total = down(b, 0)
        for d in sorted(range(1, ny), key=lambda d: min(d, ny - d)):
            h_copy(b, d).wait_recv()
            total = total + down(b, d)
        places = range(b * part * 2 * nx, (b + 1) * part * 2 * nx)
        for i in places:
            at = (i // (2 * nx) - b * part) * per_plane + (i // 2 % nx) * CAP
            os[i] = total[at : at + CAP, (i % 2) * L : (i % 2 + 1) * L].astype(BF16)
            if i == mine:
                rr[i] = total[at : at + CAP, 0:L].astype(BF16)
        for i in sorted(places, key=lambda i: -ring(i // (2 * nx) - 1, nz) - ring(i // 2 % nx, nx)):
            if i != mine:
                to = {"ep": back_z[i // (2 * nx)] + back_x[i // 2 % nx], "tp": back_tp[i % 2]}
                remote(os.at[i], rr.at[i], ssem.at[8], rsem.at[6], to).start()

    done(xt.at[pl.ds(1, 2 * nx - 1)], ssem.at[0])
    done(xs.at[pl.ds(1, nx - 1)], ssem.at[1])
    done(tr.at[pl.ds(1, nz - 1)], ssem.at[2])
    done(sr.at[pl.ds(1, nz - 1)], ssem.at[3])
    done(ax1r.at[pl.ds(1, ny - 1)], ssem.at[4])
    done(ax2r.at[:, pl.ds(1, ny - 1)], ssem.at[5])
    done(ps, ssem.at[6])
    done(hb.at[:, pl.ds(1, ny - 1)], ssem.at[7])
    done(gb, wsem.at[0])
    done(wgu.at[:, :, 0:L, :], wsem.at[2])
    done(wd.at[:, :, 0:L], wsem.at[4])
    done(rr.at[pl.ds(1, 2 * nx * nz - 1)], rsem.at[6])

    result = jnp.zeros((tokens, L), F32)
    for d in range(nz):
        back = rr[d * 2 * nx].astype(F32)
        for k in range(1, 2 * nx):
            back = back + rr[d * 2 * nx + k].astype(F32)
        for s in range(CAP):
            at = d * CAP + s
            result = result + chosen[:, at : at + 1] * back[s : s + 1, :]
    out_ref[...] = result.astype(BF16)
    done(os.at[pl.ds(1, 2 * nx * nz - 1)], ssem.at[8])


def solution(mesh):
    nx = EPG // 2
    nz = mesh.shape["ep"] // nx
    ny = mesh.shape["tp"] // 2

    def on_device(tokens, gain, bias, group_pick, member_pick, probs, gate, up, down):
        width = tokens.shape[1]
        half = gate.shape[2] // 2
        rows = nz * CAP
        all_rows = nx * rows
        vmem, dma = pltpu.VMEM, pltpu.SemaphoreType.DMA
        whole = pl.BlockSpec(memory_space=pltpu.VMEM)
        away = pl.BlockSpec(memory_space=pl.ANY)
        return pl.pallas_call(
            functools.partial(kernel, nz, nx, ny, width * 2 * ny),
            out_shape=pltpu.VMEM(tokens.shape, BF16),
            in_specs=[away] * 9,
            out_specs=whole,
            scratch_shapes=[
                vmem(tokens.shape, BF16),
                vmem((1, L), F32),
                vmem((1, L), F32),
                vmem((1, tokens.shape[0]), jnp.int32),
                vmem(member_pick.shape[::-1], jnp.int32),
                vmem(probs.shape[::-1], F32),
                vmem((2, 2, 2 * L, half), BF16),
                vmem((2, half, 2 * L), BF16),
                vmem((2, 1, L), F32),
                vmem((2 * nx, nz, CAP, L), BF16),
                vmem((nx, rows, L), BF16),
                vmem((nz, nx * CAP, L), BF16),
                vmem((nz, 2 * nx, CAP, L), BF16),
                vmem((nz, nx * CAP, L), BF16),
                vmem((ny, 2, 2 * L), F32),
                vmem((ny, 2, 2 * L), F32),
                vmem((2, 2, L), F32),
                vmem((2, ny, 2, L), F32),
                vmem((2, ny - 1, 2, all_rows // 2, L), BF16),
                vmem((2, ny - 1, 2, all_rows // 2, L), BF16),
                vmem((2, ny, all_rows // 2, L), BF16),
                vmem((2 * nx * nz, CAP, L), BF16),
                vmem((2 * nx * nz, CAP, L), BF16),
                pltpu.SemaphoreType.REGULAR((nz,)),
                pltpu.SemaphoreType.REGULAR,
                dma((6,)),
                dma((2,)),
                dma((6,)),
                dma((9,)),
                dma((7,)),
                dma((2,)),
                dma((2,)),
                dma((2, ny - 1)),
                dma((2, ny - 1)),
            ],
            compiler_params=pltpu.CompilerParams(collective_id=0, has_side_effects=True),
        )(tokens, gain.reshape(1, -1), bias.reshape(1, -1), group_pick.T, member_pick.T, probs.T, gate, up, down)

    return jax.shard_map(
        on_device,
        mesh=mesh,
        in_specs=(
            P("ep", "tp"),
            P("tp"),
            P("tp"),
            P("ep", None),
            P("ep", None),
            P("ep", None),
            P("ep", "tp", None),
            P("ep", "tp", None),
            P("ep", None, "tp"),
        ),
        out_specs=P("ep", "tp"),
        check_vma=False,
    )
```

```python
import functools

import jax
import jax.numpy as jnp
from jax import lax
from jax.experimental import pallas as pl
from jax.experimental.pallas import tpu as pltpu
from jax.sharding import PartitionSpec as P

EPG = 8
CAP = 2
norm_epsilon = 1e-05
MESH = pl.DeviceIdType.MESH
F32 = jnp.float32
BF16 = jnp.bfloat16
L = 128


def iota(shape, axis):
    return lax.broadcasted_iota(jnp.int32, shape, axis)


def far_first(n):
    return sorted(range(1, n), key=lambda d: -min(d, n - d))


def kernel(
    nz, nx, ny, features,
    tok_hbm, gain_hbm, bias_hbm, gp_hbm, mp_hbm, pp_hbm, gate_hbm, up_hbm, down_hbm,
    out_ref,
    tok_ref, gain_ref, bias_ref, gp_ref, mp_ref, pp_ref,
    wgu, wd, gb,
    xt, xs, zs, tr, sr, ax1s, ax1r, ax2s, ax2r, ps, pr, hb, os, rr,
    zready, yready, isem, lsem, wsem, ssem, rsem, tsem, asem, psem, hsem,
):
    tokens = tok_ref.shape[0]
    half = wgu.shape[3]
    rows = nz * CAP
    per_plane = nx * CAP
    all_rows = nz * per_plane
    per_expert = ny // 2
    ep, tp = lax.axis_index("ep"), lax.axis_index("tp")
    z, x, y, c = ep // nx, ep % nx, tp // 2, tp % 2

    def dev(dz=0, dx=0, dy=0, dc=0):
        return {
            "ep": lax.rem(z + dz + nz, nz) * nx + lax.rem(x + dx + nx, nx),
            "tp": lax.rem(y + dy + ny, ny) * 2 + lax.rem(c + dc, 2),
        }

    def remote(src, dst, ss, rs, device):
        return pltpu.make_async_remote_copy(
            src_ref=src, dst_ref=dst, send_sem=ss, recv_sem=rs, device_id=device, device_id_type=MESH
        )

    def each(n, body):
        lax.fori_loop(1, n, lambda d, carry: (body(d), carry)[1], 0)

    def done(ref, sem):
        pltpu.make_async_copy(ref, ref, sem).wait()

    def signal(sem, device):
        pl.semaphore_signal(sem, inc=1, device_id=device, device_id_type=MESH)

    inputs = [
        pltpu.make_async_copy(src, dst, isem.at[i])
        for i, (src, dst) in enumerate(
            (
                (gp_hbm, gp_ref),
                (mp_hbm, mp_ref),
                (pp_hbm, pp_ref),
                (tok_hbm, tok_ref),
                (gain_hbm, gain_ref),
                (bias_hbm, bias_ref),
            )
        )
    ]
    for copy in inputs:
        copy.start()

    def planes(low, high, body):
        lax.fori_loop(low, high, lambda to, carry: (body(to), carry)[1], 0)

    part = nz // 2
    side = z // part
    first = side * part

    def ranked(r):
        return r + r // per_expert * (3 * per_expert - 1 - 2 * r)

    rank = ranked(y)

    def slot(source, to):
        near = lax.rem(to - source + 1 + nz, nz)
        near = (source + nz - 1) // nz * (near + (lax.rem(to + 1, nz) - near + nz - 1) // nz)
        return (1 - to // part) * source + to // part * near

    own_slot = slot(z, z)
    barrier = pltpu.get_barrier_semaphore()

    def greet(to):
        signal(barrier, {"ep": to * nx + x, "tp": tp})

    planes(z + 1, first + part, greet)
    each(2 * nx, lambda k: signal(barrier, dev(dx=k // 2, dc=k % 2)))

    planes(rank + 1, ny, lambda r: signal(barrier, {"ep": ep, "tp": 2 * ranked(r) + c}))

    mine = pl.ds(pl.multiple_of(c * half, half), half)
    other = pl.ds(pl.multiple_of((1 - c) * half, half), half)
    pltpu.make_async_copy(gate_hbm.at[:, :, mine], wgu.at[0, :, 0:L, :], lsem.at[0]).start()
    pltpu.make_async_copy(up_hbm.at[:, :, mine], wgu.at[1, :, 0:L, :], lsem.at[0]).start()
    pltpu.make_async_copy(down_hbm.at[:, mine, :], wd.at[:, :, 0:L], lsem.at[1]).start()

    for copy in inputs:
        copy.wait()

    group = (gp_ref[...] - z + 1 + nz) % nz
    row = iota((rows, tokens), 0)
    lane = iota((rows, tokens), 1)
    member = (group == row // CAP).astype(F32)
    count = jnp.zeros((rows, tokens), F32)
    for t in range(tokens - 1):
        count = count + jnp.where(lane > t, member[:, t : t + 1], 0.0)
    rowwise = member * (count == (row % CAP).astype(F32)).astype(F32)
    def pack(source):
        packed = jnp.zeros((rows, L), F32)
        for t in range(tokens):
            packed = packed + rowwise[:, t : t + 1] * source[t : t + 1, :]
        return packed

    packed = pack(tok_ref[...].astype(F32))
    for d in range(nz):
        xt[0, d] = packed[d * CAP : (d + 1) * CAP, :].astype(BF16)

    pl.semaphore_wait(barrier, (2 * nx - 1) + z + rank)
    planes(0, z, lambda to: signal(zready.at[z], {"ep": to * nx + x, "tp": tp}))
    planes(0, rank, lambda r: signal(yready, {"ep": ep, "tp": 2 * ranked(r) + c}))

    @pl.when(side == 0)
    def _():
        planes(part, nz, greet)

    def x_copy(k):
        return remote(xt.at[0], xt.at[k], ssem.at[0], rsem.at[0], dev(dx=k // 2, dc=k % 2))

    def x_shares(dx):
        return remote(xs.at[0], xs.at[dx], ssem.at[1], rsem.at[1], dev(dx=dx))

    each(2 * nx, lambda k: x_copy(k).start())

    go_x = [lax.rem(x + d, nx) for d in range(nx)]
    go_tp = [tp, tp + 1 - 2 * c]

    def straight(to):
        i = lax.rem(to - z + 1 + nz, nz)
        at = slot(z, to)
        for k in range(2 * nx):
            device = {"ep": to * nx + go_x[k // 2], "tp": go_tp[k % 2]}
            remote(xt.at[0, i], tr.at[at, k], ssem.at[2], tsem.at[at // part], device).start()

    @pl.when(side == 1)
    def _():
        planes(0, part, straight)

    to = dev(dc=1)
    remote(gain_ref, gb.at[0], wsem.at[0], wsem.at[1], to).start()
    remote(bias_ref, gb.at[1], wsem.at[0], wsem.at[1], to).start()
    remote(gate_hbm.at[:, :, other], wgu.at[0, :, L : 2 * L, :], wsem.at[2], wsem.at[3], to).start()
    remote(up_hbm.at[:, :, other], wgu.at[1, :, L : 2 * L, :], wsem.at[2], wsem.at[3], to).start()
    remote(down_hbm.at[:, other, :], wd.at[:, :, L : 2 * L], wsem.at[4], wsem.at[5], to).start()

    probs = pp_ref[...]
    share = probs / jnp.sum(probs, axis=0, keepdims=True)
    top = probs.shape[0]
    table = [share[k : k + 1] for k in range(top)]
    table = table + [mp_ref[k : k + 1].astype(F32) for k in range(top)] + [rowwise]
    table = jnp.concatenate(table, axis=0)
    table = jnp.concatenate([table, jnp.zeros((2 * top + rows, L - tokens), F32)], axis=1)
    turned = jnp.transpose(table)[0:tokens, :]
    chosen = turned[:, 2 * top :]
    lane = iota((tokens, L), 1).astype(F32)
    shares = jnp.zeros((tokens, L), F32)
    for k in range(top):
        high = turned[:, k : k + 1].astype(BF16).astype(F32)
        low = turned[:, k : k + 1] - high
        pick = turned[:, top + k : top + k + 1]
        shares = shares + jnp.where(lane == pick, high, 0.0)
        shares = shares + jnp.where(lane == pick + EPG, low, 0.0)
    xs[0] = pack(shares).astype(BF16)
    each(nx, lambda k: x_shares(k).start())

    done(wgu.at[:, :, 0:L, :], lsem.at[0])
    done(gb, wsem.at[1])
    done(wgu.at[:, :, L : 2 * L, :], wsem.at[3])
    gain = jnp.concatenate([gain_ref[...], gb[0]], axis=1)
    bias = jnp.concatenate([bias_ref[...], gb[1]], axis=1)
    gain_high = gain.astype(BF16).astype(F32)
    bias_high = bias.astype(BF16).astype(F32)
    four = iota((16, 2 * L), 0)
    vectors = jnp.where(four == 0, gain_high, 0.0) + jnp.where(four == 1, gain - gain_high, 0.0)
    vectors = vectors + jnp.where(four == 2, bias_high, 0.0) + jnp.where(four == 3, bias - bias_high, 0.0)
    vectors = vectors.astype(BF16)
    for e in range(2):
        for g in range(2):
            line = jnp.dot(vectors, wgu[g, e], preferred_element_type=F32)
            for j in range(per_expert):
                piece = line[:, j * L : (j + 1) * L]
                ax1s[e * per_expert + j, 0:1, g * L : (g + 1) * L] = piece[0:1] + piece[1:2]
                ax1s[e * per_expert + j, 1:2, g * L : (g + 1) * L] = piece[2:3] + piece[3:4]
    ax1r[0] = ax1s[y]

    done(xt.at[pl.ds(1, 2 * nx - 1)], rsem.at[0])

    for k in range(2 * nx):
        tr[own_slot, k] = xt[k, 1]

    def z_copy(to):
        i = lax.rem(to - z + 1 + nz, nz)
        device = {"ep": to * nx + x, "tp": tp}
        at = slot(z, to)
        remote(xt.at[:, i], tr.at[at], ssem.at[2], tsem.at[at // part], device).start()

    def z_ready_copy(to):
        pl.semaphore_wait(zready.at[to], 1)
        z_copy(to)

    planes(first, z, z_copy)
    planes(z + 1, nz, z_ready_copy)

    def z_shares(d):
        i = lax.rem(d + 1, nz)
        at = slot(z, lax.rem(z + d, nz))
        return remote(zs.at[i], sr.at[at], ssem.at[3], rsem.at[3], dev(dz=d))

    done(xs.at[pl.ds(1, nx - 1)], rsem.at[1])
    blocks = [xs[dx].astype(F32) for dx in range(nx)]
    for d in range(nz):
        block = [b[d * CAP : (d + 1) * CAP, :] for b in blocks]
        zs[d] = jnp.concatenate(block, axis=0).astype(BF16)
    sr[own_slot] = zs[1]
    each(nz, lambda d: z_shares(d).start())

    @pl.when(rank < ny - 1)
    def _():
        pl.semaphore_wait(yready, ny - 1 - rank)

    def a1_copy(d):
        return remote(ax1s.at[(y + d) % ny], ax1r.at[d], ssem.at[4], rsem.at[4], dev(dy=d))

    each(ny, lambda d: a1_copy(d).start())

    batch_rows = all_rows // 2
    own_batch = 0

    def p_copy(b, d):
        return remote(ps.at[b, d - 1], pr.at[b, d - 1], ssem.at[6], psem.at[b, d - 1], dev(dy=d))

    def a2_copy(b, d):
        return remote(ax2s.at[b], ax2r.at[b, d], ssem.at[5], asem.at[b], dev(dy=d))

    gate_own, up_own = [], []
    far = [d for d in far_first(ny) if min(d, ny - d) > 2]
    held = []
    for b in range(2):
        here = part - 1 if b == own_batch else part
        if here:
            done(tr.at[pl.ds(b * part, here)], tsem.at[b])

        slots = range(b * part, b * part + part)
        values = [
            jnp.concatenate([tr[i, 2 * dx + dc].astype(F32) for i in slots for dx in range(nx)], axis=0)
            for dc in range(2)
        ]
        values = jnp.concatenate(values, axis=1)
        middle = jnp.sum(values, axis=1, keepdims=True) * (1.0 / (2 * L))
        values = values - middle
        scaled = (values * gain).astype(BF16)
        for place, d in enumerate(far_first(ny) + [0]):
            q = (y + d) % ny
            e = q // per_expert
            cols = pl.ds(pl.multiple_of((q % per_expert) * L, L), L)
            gate_part = jnp.dot(scaled, wgu[0, e, :, cols], preferred_element_type=F32)
            up_part = jnp.dot(scaled, wgu[1, e, :, cols], preferred_element_type=F32)
            if d == 0:
                gate_own.append(gate_part)
                up_own.append(up_part)
            else:
                ps[b, d - 1, 0] = gate_part.astype(BF16)
                ps[b, d - 1, 1] = up_part.astype(BF16)
                if b == 1 and d not in far:
                    while held:
                        p_copy(0, held.pop(0)).start()
                if b == 1 or d in far:
                    p_copy(b, d).start()
                else:
                    held.append(d)
            if place == 0:
                squares = jnp.sum(values * values, axis=1, keepdims=True)
                lanes = iota((batch_rows, L), 1)
                columns = jnp.where(lanes == 0, middle, 0.0) + jnp.where(lanes == 1, squares, 0.0)
                columns = jnp.transpose(columns)
                ax2s[b, :, 0:batch_rows] = columns[0:2, :]
                ax2r[b, 0, :, 0:batch_rows] = columns[0:2, :]
                each(ny, lambda d: a2_copy(b, d).start())

    def h_copy(b, d):
        return remote(hb.at[b, 0], hb.at[b, d], ssem.at[7], hsem.at[b, d - 1], dev(dy=d))

    done(sr.at[pl.ds(1, nz - 1)], rsem.at[3])
    done(ax1r.at[pl.ds(1, ny - 1)], rsem.at[4])
    expert = 2 * x + y // per_expert
    lanes = iota((batch_rows, L), 1)
    gate_bias = up_bias = jnp.zeros((1, L), F32)
    for d in range(ny):
        gate_bias = gate_bias + ax1r[d, 1:2, 0:L]
        up_bias = up_bias + ax1r[d, 1:2, L : 2 * L]
    ready = []
    for b in range(2):
        share = jnp.concatenate([sr[i].astype(F32) for i in range(b * part, b * part + part)], axis=0)
        share = jnp.sum(
            jnp.where((lanes == expert) | (lanes == expert + EPG), share, 0.0), axis=1, keepdims=True
        )
        done(ax2r.at[b, pl.ds(1, ny - 1)], asem.at[b])
        means = [ax2r[b, d, 0:1, 0:batch_rows] for d in range(ny)]
        center = sum(means) * (1.0 / ny)
        shifts = [m - center for m in means]
        spread = sum(ax2r[b, d, 1:2, 0:batch_rows] for d in range(ny))
        spread = spread + (features // ny) * sum(s * s for s in shifts)
        scale = lax.rsqrt(spread * (1.0 / features) + norm_epsilon)
        stack = iota((16, batch_rows), 0)
        table = jnp.where(stack == ny, scale, 0.0)
        for d in range(ny):
            table = table + jnp.where(stack == d, shifts[d], 0.0)
        table = jnp.transpose(table)
        scale = table[:, ny : ny + 1]
        gate, up = gate_own[b], up_own[b]
        for d in range(ny):
            shift = table[:, d : d + 1]
            gate = gate + shift * ax1r[d, 0:1, 0:L]
            up = up + shift * ax1r[d, 0:1, L : 2 * L]
        ready.append((gate, up, scale, share))
    for b in range(2):
        gate, up, scale, share = ready[b]
        for d in far_first(ny):
            p_copy(b, d).wait_recv()
            gate = gate + pr[b, d - 1, 0].astype(F32)
            up = up + pr[b, d - 1, 1].astype(F32)
        gate = gate * scale + gate_bias
        up = up * scale + up_bias
        hb[b, 0] = (share * (gate / (1.0 + jnp.exp(-gate)) * up)).astype(BF16)
        for d in far_first(ny):
            h_copy(b, d).start()

    def down(b, d):
        q = (y - d + ny) % ny
        units = pl.ds(pl.multiple_of((q % per_expert) * L, L), L)
        return jnp.dot(hb[b, d], wd[q // per_expert, units, :], preferred_element_type=F32)

    done(wd.at[:, :, 0:L], lsem.at[1])
    done(wd.at[:, :, L : 2 * L], wsem.at[5])

    back_z, back_at = [], []
    last = lax.rem(z + 1, nz)
    for h in range(nz):
        source = lax.rem(z + 1 - h + (last - h + nz) // nz + nz, nz) * side if h else 0
        source = source + (1 - side) * h
        back_z.append(source * nx)
        back_at.append(lax.rem(z - source + 1 + nz, nz) * 2 * nx)
    back_x = [lax.rem(x - d + nx, nx) for d in range(nx)]
    back_tp = [tp, tp + 1 - 2 * c]
    order = sorted(range(2 * nx), key=lambda k: -min(k // 2, nx - k // 2))

    def send_back(h, k):
        to = {"ep": back_z[h] + back_x[k // 2], "tp": back_tp[k % 2]}
        remote(os.at[h * 2 * nx + k], rr.at[back_at[h] + k], ssem.at[8], rsem.at[6], to).start()

    for b in range(2):
        total = down(b, 0)
        for d in sorted(range(1, ny), key=lambda d: min(d, ny - d)):
            h_copy(b, d).wait_recv()
            total = total + down(b, d)
        slots = range(b * part, (b + 1) * part)
        for h in slots:
            for k in range(2 * nx):
                at = (h - b * part) * per_plane + k // 2 * CAP
                piece = total[at : at + CAP, (k % 2) * L : (k % 2 + 1) * L]
                os[h * 2 * nx + k] = piece.astype(BF16)
        for h in slots:
            for k in order:
                if k:
                    send_back(h, k)
                elif b == own_batch:
                    pl.when(own_slot != h)(functools.partial(send_back, h, k))
                else:
                    send_back(h, k)
    rr[2 * nx] = os[own_slot * 2 * nx]

    done(xt.at[pl.ds(1, 2 * nx - 1)], ssem.at[0])
    done(xs.at[pl.ds(1, nx - 1)], ssem.at[1])
    done(tr.at[pl.ds(1, nz - 1)], ssem.at[2])
    done(sr.at[pl.ds(1, nz - 1)], ssem.at[3])
    done(ax1r.at[pl.ds(1, ny - 1)], ssem.at[4])
    done(ax2r.at[:, pl.ds(1, ny - 1)], ssem.at[5])
    done(ps, ssem.at[6])
    done(hb.at[:, pl.ds(1, ny - 1)], ssem.at[7])
    done(gb, wsem.at[0])
    done(wgu.at[:, :, 0:L, :], wsem.at[2])
    done(wd.at[:, :, 0:L], wsem.at[4])
    done(rr.at[pl.ds(1, 2 * nx * nz - 1)], rsem.at[6])

    result = jnp.zeros((tokens, L), F32)
    for d in range(nz):
        back = rr[d * 2 * nx].astype(F32)
        for k in range(1, 2 * nx):
            back = back + rr[d * 2 * nx + k].astype(F32)
        for s in range(CAP):
            at = d * CAP + s
            result = result + chosen[:, at : at + 1] * back[s : s + 1, :]
    out_ref[...] = result.astype(BF16)
    done(os.at[pl.ds(1, 2 * nx * nz - 1)], ssem.at[8])


def solution(mesh):
    nx = EPG // 2
    nz = mesh.shape["ep"] // nx
    ny = mesh.shape["tp"] // 2

    def on_device(tokens, gain, bias, group_pick, member_pick, probs, gate, up, down):
        width = tokens.shape[1]
        half = gate.shape[2] // 2
        rows = nz * CAP
        all_rows = nx * rows
        vmem, dma = pltpu.VMEM, pltpu.SemaphoreType.DMA
        whole = pl.BlockSpec(memory_space=pltpu.VMEM)
        away = pl.BlockSpec(memory_space=pl.ANY)
        return pl.pallas_call(
            functools.partial(kernel, nz, nx, ny, width * 2 * ny),
            out_shape=pltpu.VMEM(tokens.shape, BF16),
            in_specs=[away] * 9,
            out_specs=whole,
            scratch_shapes=[
                vmem(tokens.shape, BF16),
                vmem((1, L), F32),
                vmem((1, L), F32),
                vmem((1, tokens.shape[0]), jnp.int32),
                vmem(member_pick.shape[::-1], jnp.int32),
                vmem(probs.shape[::-1], F32),
                vmem((2, 2, 2 * L, half), BF16),
                vmem((2, half, 2 * L), BF16),
                vmem((2, 1, L), F32),
                vmem((2 * nx, nz, CAP, L), BF16),
                vmem((nx, rows, L), BF16),
                vmem((nz, nx * CAP, L), BF16),
                vmem((nz, 2 * nx, CAP, L), BF16),
                vmem((nz, nx * CAP, L), BF16),
                vmem((ny, 2, 2 * L), F32),
                vmem((ny, 2, 2 * L), F32),
                vmem((2, 2, L), F32),
                vmem((2, ny, 2, L), F32),
                vmem((2, ny - 1, 2, all_rows // 2, L), BF16),
                vmem((2, ny - 1, 2, all_rows // 2, L), BF16),
                vmem((2, ny, all_rows // 2, L), BF16),
                vmem((2 * nx * nz, CAP, L), BF16),
                vmem((2 * nx * nz, CAP, L), BF16),
                pltpu.SemaphoreType.REGULAR((nz,)),
                pltpu.SemaphoreType.REGULAR,
                dma((6,)),
                dma((2,)),
                dma((6,)),
                dma((9,)),
                dma((7,)),
                dma((2,)),
                dma((2,)),
                dma((2, ny - 1)),
                dma((2, ny - 1)),
            ],
            compiler_params=pltpu.CompilerParams(collective_id=0, has_side_effects=True),
        )(tokens, gain.reshape(1, -1), bias.reshape(1, -1), group_pick.T, member_pick.T, probs.T, gate, up, down)

    return jax.shard_map(
        on_device,
        mesh=mesh,
        in_specs=(
            P("ep", "tp"),
            P("tp"),
            P("tp"),
            P("ep", None),
            P("ep", None),
            P("ep", None),
            P("ep", "tp", None),
            P("ep", "tp", None),
            P("ep", None, "tp"),
        ),
        out_specs=P("ep", "tp"),
        check_vma=False,
    )
```

```python
import functools

import jax
import jax.numpy as jnp
from jax import lax
from jax.experimental import pallas as pl
from jax.experimental.pallas import tpu as pltpu
from jax.sharding import PartitionSpec as P

EPG = 8
CAP = 2
norm_epsilon = 1e-05
MESH = pl.DeviceIdType.MESH
F32 = jnp.float32
BF16 = jnp.bfloat16
L = 128


def iota(shape, axis):
    return lax.broadcasted_iota(jnp.int32, shape, axis)


def far_first(n):
    return sorted(range(1, n), key=lambda d: -min(d, n - d))


def kernel(
    nz, nx, ny, features,
    tok_hbm, gain_hbm, bias_hbm, gp_hbm, mp_hbm, pp_hbm, gate_hbm, up_hbm, down_hbm,
    out_ref,
    tok_ref, gain_ref, bias_ref, gp_ref, mp_ref, pp_ref,
    wgu, wd, gb,
    xt, xs, zs, tr, sr, ax1s, ax1r, ax2s, ax2r, ps, pr, hb, os, rr,
    zready, yready, isem, lsem, wsem, ssem, rsem, tsem, asem, psem, hsem,
):
    tokens = tok_ref.shape[0]
    half = wgu.shape[3]
    rows = nz * CAP
    per_plane = nx * CAP
    all_rows = nz * per_plane
    per_expert = ny // 2
    ep, tp = lax.axis_index("ep"), lax.axis_index("tp")
    z, x, y, c = ep // nx, ep % nx, tp // 2, tp % 2

    def dev(dz=0, dx=0, dy=0, dc=0):
        return {
            "ep": lax.rem(z + dz + nz, nz) * nx + lax.rem(x + dx + nx, nx),
            "tp": lax.rem(y + dy + ny, ny) * 2 + lax.rem(c + dc, 2),
        }

    def remote(src, dst, ss, rs, device):
        return pltpu.make_async_remote_copy(
            src_ref=src, dst_ref=dst, send_sem=ss, recv_sem=rs, device_id=device, device_id_type=MESH
        )

    def each(n, body):
        lax.fori_loop(1, n, lambda d, carry: (body(d), carry)[1], 0)

    def done(ref, sem):
        pltpu.make_async_copy(ref, ref, sem).wait()

    def signal(sem, device):
        pl.semaphore_signal(sem, inc=1, device_id=device, device_id_type=MESH)

    inputs = [
        pltpu.make_async_copy(src, dst, isem.at[i])
        for i, (src, dst) in enumerate(
            (
                (gp_hbm, gp_ref),
                (mp_hbm, mp_ref),
                (pp_hbm, pp_ref),
                (tok_hbm, tok_ref),
                (gain_hbm, gain_ref),
                (bias_hbm, bias_ref),
            )
        )
    ]
    for copy in inputs:
        copy.start()

    def planes(low, high, body):
        lax.fori_loop(low, high, lambda to, carry: (body(to), carry)[1], 0)

    part = nz // 2
    side = z // part
    first = side * part

    def ranked(r):
        return r + r // per_expert * (3 * per_expert - 1 - 2 * r)

    rank = ranked(y)

    def slot(source, to):
        near = lax.rem(to - source + 1 + nz, nz)
        near = (source + nz - 1) // nz * (near + (lax.rem(to + 1, nz) - near + nz - 1) // nz)
        return (1 - to // part) * source + to // part * near

    own_slot = slot(z, z)
    barrier = pltpu.get_barrier_semaphore()

    def greet(to):
        signal(barrier, {"ep": to * nx + x, "tp": tp})

    planes(z + 1, first + part, greet)
    each(2 * nx, lambda k: signal(barrier, dev(dx=k // 2, dc=k % 2)))

    planes(rank + 1, ny, lambda r: signal(barrier, {"ep": ep, "tp": 2 * ranked(r) + c}))

    mine = pl.ds(pl.multiple_of(c * half, half), half)
    other = pl.ds(pl.multiple_of((1 - c) * half, half), half)
    pltpu.make_async_copy(gate_hbm.at[:, :, mine], wgu.at[0, :, 0:L, :], lsem.at[0]).start()
    pltpu.make_async_copy(up_hbm.at[:, :, mine], wgu.at[1, :, 0:L, :], lsem.at[0]).start()
    pltpu.make_async_copy(down_hbm.at[:, mine, :], wd.at[:, :, 0:L], lsem.at[1]).start()

    for copy in inputs:
        copy.wait()

    group = (gp_ref[...] - z + 1 + nz) % nz
    row = iota((rows, tokens), 0)
    lane = iota((rows, tokens), 1)
    member = (group == row // CAP).astype(F32)
    count = jnp.zeros((rows, tokens), F32)
    for t in range(tokens - 1):
        count = count + jnp.where(lane > t, member[:, t : t + 1], 0.0)
    rowwise = member * (count == (row % CAP).astype(F32)).astype(F32)
    def pack(source):
        packed = jnp.zeros((rows, L), F32)
        for t in range(tokens):
            packed = packed + rowwise[:, t : t + 1] * source[t : t + 1, :]
        return packed

    packed = pack(tok_ref[...].astype(F32))
    for d in range(nz):
        xt[0, d] = packed[d * CAP : (d + 1) * CAP, :].astype(BF16)

    pl.semaphore_wait(barrier, (2 * nx - 1) + z + rank)
    planes(0, z, lambda to: signal(zready.at[z], {"ep": to * nx + x, "tp": tp}))
    planes(0, rank, lambda r: signal(yready, {"ep": ep, "tp": 2 * ranked(r) + c}))

    @pl.when(side == 0)
    def _():
        planes(part, nz, greet)

    def x_copy(k):
        return remote(xt.at[0], xt.at[k], ssem.at[0], rsem.at[0], dev(dx=k // 2, dc=k % 2))

    def x_shares(dx):
        return remote(xs.at[0], xs.at[dx], ssem.at[1], rsem.at[1], dev(dx=dx))

    each(2 * nx, lambda k: x_copy(k).start())

    go_x = [lax.rem(x + d, nx) for d in range(nx)]
    go_tp = [tp, tp + 1 - 2 * c]

    def straight(to):
        i = lax.rem(to - z + 1 + nz, nz)
        at = slot(z, to)
        for k in range(2 * nx):
            device = {"ep": to * nx + go_x[k // 2], "tp": go_tp[k % 2]}
            remote(xt.at[0, i], tr.at[at, k], ssem.at[2], tsem.at[at // part], device).start()

    @pl.when(side == 1)
    def _():
        planes(0, part, straight)

    to = dev(dc=1)
    remote(gain_ref, gb.at[0], wsem.at[0], wsem.at[1], to).start()
    remote(bias_ref, gb.at[1], wsem.at[0], wsem.at[1], to).start()
    remote(gate_hbm.at[:, :, other], wgu.at[0, :, L : 2 * L, :], wsem.at[2], wsem.at[3], to).start()
    remote(up_hbm.at[:, :, other], wgu.at[1, :, L : 2 * L, :], wsem.at[2], wsem.at[3], to).start()
    remote(down_hbm.at[:, other, :], wd.at[:, :, L : 2 * L], wsem.at[4], wsem.at[5], to).start()

    probs = pp_ref[...]
    share = probs / jnp.sum(probs, axis=0, keepdims=True)
    top = probs.shape[0]
    table = [share[k : k + 1] for k in range(top)]
    table = table + [mp_ref[k : k + 1].astype(F32) for k in range(top)] + [rowwise]
    table = jnp.concatenate(table, axis=0)
    table = jnp.concatenate([table, jnp.zeros((2 * top + rows, L - tokens), F32)], axis=1)
    turned = jnp.transpose(table)[0:tokens, :]
    chosen = turned[:, 2 * top :]
    lane = iota((tokens, L), 1).astype(F32)
    shares = jnp.zeros((tokens, L), F32)
    for k in range(top):
        high = turned[:, k : k + 1].astype(BF16).astype(F32)
        low = turned[:, k : k + 1] - high
        pick = turned[:, top + k : top + k + 1]
        shares = shares + jnp.where(lane == pick, high, 0.0)
        shares = shares + jnp.where(lane == pick + EPG, low, 0.0)
    xs[0] = pack(shares).astype(BF16)
    each(nx, lambda k: x_shares(k).start())

    done(wgu.at[:, :, 0:L, :], lsem.at[0])
    done(gb, wsem.at[1])
    done(wgu.at[:, :, L : 2 * L, :], wsem.at[3])
    gain = jnp.concatenate([gain_ref[...], gb[0]], axis=1)
    bias = jnp.concatenate([bias_ref[...], gb[1]], axis=1)
    gain_high = gain.astype(BF16).astype(F32)
    bias_high = bias.astype(BF16).astype(F32)
    four = iota((16, 2 * L), 0)
    vectors = jnp.where(four == 0, gain_high, 0.0) + jnp.where(four == 1, gain - gain_high, 0.0)
    vectors = vectors + jnp.where(four == 2, bias_high, 0.0) + jnp.where(four == 3, bias - bias_high, 0.0)
    vectors = vectors.astype(BF16)
    for e in range(2):
        for g in range(2):
            line = jnp.dot(vectors, wgu[g, e], preferred_element_type=F32)
            for j in range(per_expert):
                piece = line[:, j * L : (j + 1) * L]
                ax1s[e * per_expert + j, 0:1, g * L : (g + 1) * L] = piece[0:1] + piece[1:2]
                ax1s[e * per_expert + j, 1:2, g * L : (g + 1) * L] = piece[2:3] + piece[3:4]
    ax1r[0] = ax1s[y]

    done(xt.at[pl.ds(1, 2 * nx - 1)], rsem.at[0])

    for k in range(2 * nx):
        tr[own_slot, k] = xt[k, 1]

    def z_copy(to):
        i = lax.rem(to - z + 1 + nz, nz)
        device = {"ep": to * nx + x, "tp": tp}
        at = slot(z, to)
        remote(xt.at[:, i], tr.at[at], ssem.at[2], tsem.at[at // part], device).start()

    def z_ready_copy(to):
        pl.semaphore_wait(zready.at[to], 1)
        z_copy(to)

    planes(first, z, z_copy)
    planes(z + 1, nz, z_ready_copy)

    def z_shares(d):
        i = lax.rem(d + 1, nz)
        at = slot(z, lax.rem(z + d, nz))
        return remote(zs.at[i], sr.at[at], ssem.at[3], rsem.at[3], dev(dz=d))

    done(xs.at[pl.ds(1, nx - 1)], rsem.at[1])
    blocks = [xs[dx].astype(F32) for dx in range(nx)]
    for d in range(nz):
        block = [b[d * CAP : (d + 1) * CAP, :] for b in blocks]
        zs[d] = jnp.concatenate(block, axis=0).astype(BF16)
    sr[own_slot] = zs[1]
    each(nz, lambda d: z_shares(d).start())

    @pl.when(rank < ny - 1)
    def _():
        pl.semaphore_wait(yready, ny - 1 - rank)

    def a1_copy(d):
        return remote(ax1s.at[(y + d) % ny], ax1r.at[d], ssem.at[4], rsem.at[4], dev(dy=d))

    each(ny, lambda d: a1_copy(d).start())

    batch_rows = all_rows // 2
    own_batch = 0

    def p_copy(b, d):
        return remote(ps.at[b, d - 1], pr.at[b, d - 1], ssem.at[6], psem.at[b, d - 1], dev(dy=d))

    def a2_copy(b, d):
        return remote(ax2s.at[b], ax2r.at[b, d], ssem.at[5], asem.at[b], dev(dy=d))

    gate_own, up_own = [], []
    for b in range(2):
        here = part - 1 if b == own_batch else part
        if here:
            done(tr.at[pl.ds(b * part, here)], tsem.at[b])

        slots = range(b * part, b * part + part)
        values = [
            jnp.concatenate([tr[i, 2 * dx + dc].astype(F32) for i in slots for dx in range(nx)], axis=0)
            for dc in range(2)
        ]
        values = jnp.concatenate(values, axis=1)
        middle = jnp.sum(values, axis=1, keepdims=True) * (1.0 / (2 * L))
        values = values - middle
        scaled = (values * gain).astype(BF16)
        for place, d in enumerate(far_first(ny) + [0]):
            q = (y + d) % ny
            e = q // per_expert
            cols = pl.ds(pl.multiple_of((q % per_expert) * L, L), L)
            gate_part = jnp.dot(scaled, wgu[0, e, :, cols], preferred_element_type=F32)
            up_part = jnp.dot(scaled, wgu[1, e, :, cols], preferred_element_type=F32)
            if d == 0:
                gate_own.append(gate_part)
                up_own.append(up_part)
            else:
                ps[b, d - 1, 0] = gate_part.astype(BF16)
                ps[b, d - 1, 1] = up_part.astype(BF16)
                p_copy(b, d).start()
            if place == 0:
                squares = jnp.sum(values * values, axis=1, keepdims=True)
                lanes = iota((batch_rows, L), 1)
                columns = jnp.where(lanes == 0, middle, 0.0) + jnp.where(lanes == 1, squares, 0.0)
                columns = jnp.transpose(columns)
                ax2s[b, :, 0:batch_rows] = columns[0:2, :]
                ax2r[b, 0, :, 0:batch_rows] = columns[0:2, :]
                each(ny, lambda d: a2_copy(b, d).start())

    def h_copy(b, d):
        return remote(hb.at[b, 0], hb.at[b, d], ssem.at[7], hsem.at[b, d - 1], dev(dy=d))

    done(sr.at[pl.ds(1, nz - 1)], rsem.at[3])
    done(ax1r.at[pl.ds(1, ny - 1)], rsem.at[4])
    expert = 2 * x + y // per_expert
    lanes = iota((batch_rows, L), 1)
    gate_bias = up_bias = jnp.zeros((1, L), F32)
    for d in range(ny):
        gate_bias = gate_bias + ax1r[d, 1:2, 0:L]
        up_bias = up_bias + ax1r[d, 1:2, L : 2 * L]
    for b in range(2):
        share = jnp.concatenate([sr[i].astype(F32) for i in range(b * part, b * part + part)], axis=0)
        share = jnp.sum(
            jnp.where((lanes == expert) | (lanes == expert + EPG), share, 0.0), axis=1, keepdims=True
        )
        done(ax2r.at[b, pl.ds(1, ny - 1)], asem.at[b])
        means = [ax2r[b, d, 0:1, 0:batch_rows] for d in range(ny)]
        center = sum(means) * (1.0 / ny)
        shifts = [m - center for m in means]
        spread = sum(ax2r[b, d, 1:2, 0:batch_rows] for d in range(ny))
        spread = spread + (features // ny) * sum(s * s for s in shifts)
        scale = lax.rsqrt(spread * (1.0 / features) + norm_epsilon)
        stack = iota((16, batch_rows), 0)
        table = jnp.where(stack == ny, scale, 0.0)
        for d in range(ny):
            table = table + jnp.where(stack == d, shifts[d], 0.0)
        table = jnp.transpose(table)
        scale = table[:, ny : ny + 1]
        gate, up = gate_own[b], up_own[b]
        for d in range(ny):
            shift = table[:, d : d + 1]
            gate = gate + shift * ax1r[d, 0:1, 0:L]
            up = up + shift * ax1r[d, 0:1, L : 2 * L]
        for d in far_first(ny):
            p_copy(b, d).wait_recv()
            gate = gate + pr[b, d - 1, 0].astype(F32)
            up = up + pr[b, d - 1, 1].astype(F32)
        gate = gate * scale + gate_bias
        up = up * scale + up_bias
        hb[b, 0] = (share * (gate / (1.0 + jnp.exp(-gate)) * up)).astype(BF16)
        for d in far_first(ny):
            h_copy(b, d).start()

    def down(b, d):
        q = (y - d + ny) % ny
        units = pl.ds(pl.multiple_of((q % per_expert) * L, L), L)
        return jnp.dot(hb[b, d], wd[q // per_expert, units, :], preferred_element_type=F32)

    done(wd.at[:, :, 0:L], lsem.at[1])
    done(wd.at[:, :, L : 2 * L], wsem.at[5])

    back_z, back_at = [], []
    last = lax.rem(z + 1, nz)
    for h in range(nz):
        source = lax.rem(z + 1 - h + (last - h + nz) // nz + nz, nz) * side if h else 0
        source = source + (1 - side) * h
        back_z.append(source * nx)
        back_at.append(lax.rem(z - source + 1 + nz, nz) * 2 * nx)
    back_x = [lax.rem(x - d + nx, nx) for d in range(nx)]
    back_tp = [tp, tp + 1 - 2 * c]
    order = sorted(range(2 * nx), key=lambda k: -min(k // 2, nx - k // 2))

    def send_back(h, k):
        to = {"ep": back_z[h] + back_x[k // 2], "tp": back_tp[k % 2]}
        remote(os.at[h * 2 * nx + k], rr.at[back_at[h] + k], ssem.at[8], rsem.at[6], to).start()

    for b in range(2):
        total = down(b, 0)
        for d in sorted(range(1, ny), key=lambda d: min(d, ny - d)):
            h_copy(b, d).wait_recv()
            total = total + down(b, d)
        slots = range(b * part, (b + 1) * part)
        for h in slots:
            for k in range(2 * nx):
                at = (h - b * part) * per_plane + k // 2 * CAP
                piece = total[at : at + CAP, (k % 2) * L : (k % 2 + 1) * L]
                os[h * 2 * nx + k] = piece.astype(BF16)
        for h in slots:
            for k in order:
                if k:
                    send_back(h, k)
                elif b == own_batch:
                    pl.when(own_slot != h)(functools.partial(send_back, h, k))
                else:
                    send_back(h, k)
    rr[2 * nx] = os[own_slot * 2 * nx]

    done(xt.at[pl.ds(1, 2 * nx - 1)], ssem.at[0])
    done(xs.at[pl.ds(1, nx - 1)], ssem.at[1])
    done(tr.at[pl.ds(1, nz - 1)], ssem.at[2])
    done(sr.at[pl.ds(1, nz - 1)], ssem.at[3])
    done(ax1r.at[pl.ds(1, ny - 1)], ssem.at[4])
    done(ax2r.at[:, pl.ds(1, ny - 1)], ssem.at[5])
    done(ps, ssem.at[6])
    done(hb.at[:, pl.ds(1, ny - 1)], ssem.at[7])
    done(gb, wsem.at[0])
    done(wgu.at[:, :, 0:L, :], wsem.at[2])
    done(wd.at[:, :, 0:L], wsem.at[4])
    done(rr.at[pl.ds(1, 2 * nx * nz - 1)], rsem.at[6])

    result = jnp.zeros((tokens, L), F32)
    for d in range(nz):
        back = rr[d * 2 * nx].astype(F32)
        for k in range(1, 2 * nx):
            back = back + rr[d * 2 * nx + k].astype(F32)
        for s in range(CAP):
            at = d * CAP + s
            result = result + chosen[:, at : at + 1] * back[s : s + 1, :]
    out_ref[...] = result.astype(BF16)
    done(os.at[pl.ds(1, 2 * nx * nz - 1)], ssem.at[8])


def solution(mesh):
    nx = EPG // 2
    nz = mesh.shape["ep"] // nx
    ny = mesh.shape["tp"] // 2

    def on_device(tokens, gain, bias, group_pick, member_pick, probs, gate, up, down):
        width = tokens.shape[1]
        half = gate.shape[2] // 2
        rows = nz * CAP
        all_rows = nx * rows
        vmem, dma = pltpu.VMEM, pltpu.SemaphoreType.DMA
        whole = pl.BlockSpec(memory_space=pltpu.VMEM)
        away = pl.BlockSpec(memory_space=pl.ANY)
        return pl.pallas_call(
            functools.partial(kernel, nz, nx, ny, width * 2 * ny),
            out_shape=pltpu.VMEM(tokens.shape, BF16),
            in_specs=[away] * 9,
            out_specs=whole,
            scratch_shapes=[
                vmem(tokens.shape, BF16),
                vmem((1, L), F32),
                vmem((1, L), F32),
                vmem((1, tokens.shape[0]), jnp.int32),
                vmem(member_pick.shape[::-1], jnp.int32),
                vmem(probs.shape[::-1], F32),
                vmem((2, 2, 2 * L, half), BF16),
                vmem((2, half, 2 * L), BF16),
                vmem((2, 1, L), F32),
                vmem((2 * nx, nz, CAP, L), BF16),
                vmem((nx, rows, L), BF16),
                vmem((nz, nx * CAP, L), BF16),
                vmem((nz, 2 * nx, CAP, L), BF16),
                vmem((nz, nx * CAP, L), BF16),
                vmem((ny, 2, 2 * L), F32),
                vmem((ny, 2, 2 * L), F32),
                vmem((2, 2, L), F32),
                vmem((2, ny, 2, L), F32),
                vmem((2, ny - 1, 2, all_rows // 2, L), BF16),
                vmem((2, ny - 1, 2, all_rows // 2, L), BF16),
                vmem((2, ny, all_rows // 2, L), BF16),
                vmem((2 * nx * nz, CAP, L), BF16),
                vmem((2 * nx * nz, CAP, L), BF16),
                pltpu.SemaphoreType.REGULAR((nz,)),
                pltpu.SemaphoreType.REGULAR,
                dma((6,)),
                dma((2,)),
                dma((6,)),
                dma((9,)),
                dma((7,)),
                dma((2,)),
                dma((2,)),
                dma((2, ny - 1)),
                dma((2, ny - 1)),
            ],
            compiler_params=pltpu.CompilerParams(collective_id=0, has_side_effects=True),
        )(tokens, gain.reshape(1, -1), bias.reshape(1, -1), group_pick.T, member_pick.T, probs.T, gate, up, down)

    return jax.shard_map(
        on_device,
        mesh=mesh,
        in_specs=(
            P("ep", "tp"),
            P("tp"),
            P("tp"),
            P("ep", None),
            P("ep", None),
            P("ep", None),
            P("ep", "tp", None),
            P("ep", "tp", None),
            P("ep", None, "tp"),
        ),
        out_specs=P("ep", "tp"),
        check_vma=False,
    )
```

```python
import functools

import jax
import jax.numpy as jnp
from jax import lax
from jax.experimental import pallas as pl
from jax.experimental.pallas import tpu as pltpu
from jax.sharding import PartitionSpec as P

EPG = 8
CAP = 2
EARLY = 2
norm_epsilon = 1e-05
MESH = pl.DeviceIdType.MESH
F32 = jnp.float32
BF16 = jnp.bfloat16
L = 128


def iota(shape, axis):
    return lax.broadcasted_iota(jnp.int32, shape, axis)


def far_first(n):
    return sorted(range(1, n), key=lambda d: -min(d, n - d))


def kernel(
    nz, nx, ny, features,
    tok_hbm, gain_hbm, bias_hbm, gp_hbm, mp_hbm, pp_hbm, gate_hbm, up_hbm, down_hbm,
    out_ref,
    tok_ref, gain_ref, bias_ref, gp_ref, mp_ref, pp_ref,
    wgu, wd, gb,
    xt, xs, zs, tr, sr, ax1s, ax1r, ax2s, ax2r, ps, pr, hb, os, rr,
    zready, yready, isem, lsem, wsem, ssem, rsem, tsem, asem, psem, hsem,
):
    tokens = tok_ref.shape[0]
    half = wgu.shape[3]
    rows = nz * CAP
    per_plane = nx * CAP
    all_rows = nz * per_plane
    per_expert = ny // 2
    ep, tp = lax.axis_index("ep"), lax.axis_index("tp")
    z, x, y, c = ep // nx, ep % nx, tp // 2, tp % 2

    def dev(dz=0, dx=0, dy=0, dc=0):
        return {
            "ep": lax.rem(z + dz + nz, nz) * nx + lax.rem(x + dx + nx, nx),
            "tp": lax.rem(y + dy + ny, ny) * 2 + lax.rem(c + dc, 2),
        }

    def remote(src, dst, ss, rs, device):
        return pltpu.make_async_remote_copy(
            src_ref=src, dst_ref=dst, send_sem=ss, recv_sem=rs, device_id=device, device_id_type=MESH
        )

    def each(n, body):
        lax.fori_loop(1, n, lambda d, carry: (body(d), carry)[1], 0)

    def done(ref, sem):
        pltpu.make_async_copy(ref, ref, sem).wait()

    def signal(sem, device):
        pl.semaphore_signal(sem, inc=1, device_id=device, device_id_type=MESH)

    inputs = [
        pltpu.make_async_copy(src, dst, isem.at[i])
        for i, (src, dst) in enumerate(
            (
                (gp_hbm, gp_ref),
                (mp_hbm, mp_ref),
                (pp_hbm, pp_ref),
                (tok_hbm, tok_ref),
                (gain_hbm, gain_ref),
                (bias_hbm, bias_ref),
            )
        )
    ]
    for copy in inputs:
        copy.start()

    def planes(low, high, body):
        lax.fori_loop(low, high, lambda to, carry: (body(to), carry)[1], 0)

    part = nz // 2
    side = z // part
    first = side * part

    def ranked(r):
        return r + r // per_expert * (3 * per_expert - 1 - 2 * r)

    rank = ranked(y)
    own_batch = (z + nz - EARLY) // nz
    barrier = pltpu.get_barrier_semaphore()

    def greet(to):
        signal(barrier, {"ep": to * nx + x, "tp": tp})

    planes(z + 1, first + part, greet)
    each(2 * nx, lambda k: signal(barrier, dev(dx=k // 2, dc=k % 2)))

    planes(rank + 1, ny, lambda r: signal(barrier, {"ep": ep, "tp": 2 * ranked(r) + c}))

    mine = pl.ds(pl.multiple_of(c * half, half), half)
    other = pl.ds(pl.multiple_of((1 - c) * half, half), half)
    pltpu.make_async_copy(gate_hbm.at[:, :, mine], wgu.at[0, :, 0:L, :], lsem.at[0]).start()
    pltpu.make_async_copy(up_hbm.at[:, :, mine], wgu.at[1, :, 0:L, :], lsem.at[0]).start()
    pltpu.make_async_copy(down_hbm.at[:, mine, :], wd.at[:, :, 0:L], lsem.at[1]).start()

    for copy in inputs:
        copy.wait()

    group = gp_ref[...]
    row = iota((rows, tokens), 0)
    lane = iota((rows, tokens), 1)
    member = (group == row // CAP).astype(F32)
    count = jnp.zeros((rows, tokens), F32)
    for t in range(tokens - 1):
        count = count + jnp.where(lane > t, member[:, t : t + 1], 0.0)
    rowwise = member * (count == (row % CAP).astype(F32)).astype(F32)
    def pack(source):
        packed = jnp.zeros((rows, L), F32)
        for t in range(tokens):
            packed = packed + rowwise[:, t : t + 1] * source[t : t + 1, :]
        return packed

    packed = pack(tok_ref[...].astype(F32))
    for d in range(nz):
        xt[0, d] = packed[d * CAP : (d + 1) * CAP, :].astype(BF16)

    pl.semaphore_wait(barrier, (2 * nx - 1) + z + rank)
    planes(0, z, lambda to: signal(zready.at[z], {"ep": to * nx + x, "tp": tp}))
    planes(0, rank, lambda r: signal(yready, {"ep": ep, "tp": 2 * ranked(r) + c}))

    @pl.when(side == 0)
    def _():
        planes(part, nz, greet)

    def x_copy(k):
        return remote(xt.at[0], xt.at[k], ssem.at[0], rsem.at[0], dev(dx=k // 2, dc=k % 2))

    def x_shares(dx):
        return remote(xs.at[0], xs.at[dx], ssem.at[1], rsem.at[1], dev(dx=dx))

    each(2 * nx, lambda k: x_copy(k).start())

    go_x = [lax.rem(x + d, nx) for d in range(nx)]
    go_tp = [tp, tp + 1 - 2 * c]

    def straight(to):
        for k in range(2 * nx):
            device = {"ep": to * nx + go_x[k // 2], "tp": go_tp[k % 2]}
            remote(xt.at[0, to], tr.at[z, k], ssem.at[2], tsem.at[own_batch], device).start()

    @pl.when(side == 1)
    def _():
        planes(0, part, straight)

    to = dev(dc=1)
    remote(gain_ref, gb.at[0], wsem.at[0], wsem.at[1], to).start()
    remote(bias_ref, gb.at[1], wsem.at[0], wsem.at[1], to).start()
    remote(gate_hbm.at[:, :, other], wgu.at[0, :, L : 2 * L, :], wsem.at[2], wsem.at[3], to).start()
    remote(up_hbm.at[:, :, other], wgu.at[1, :, L : 2 * L, :], wsem.at[2], wsem.at[3], to).start()
    remote(down_hbm.at[:, other, :], wd.at[:, :, L : 2 * L], wsem.at[4], wsem.at[5], to).start()

    probs = pp_ref[...]
    share = probs / jnp.sum(probs, axis=0, keepdims=True)
    top = probs.shape[0]
    table = [share[k : k + 1] for k in range(top)]
    table = table + [mp_ref[k : k + 1].astype(F32) for k in range(top)] + [rowwise]
    table = jnp.concatenate(table, axis=0)
    table = jnp.concatenate([table, jnp.zeros((2 * top + rows, L - tokens), F32)], axis=1)
    turned = jnp.transpose(table)[0:tokens, :]
    chosen = turned[:, 2 * top :]
    lane = iota((tokens, L), 1).astype(F32)
    shares = jnp.zeros((tokens, L), F32)
    for k in range(top):
        high = turned[:, k : k + 1].astype(BF16).astype(F32)
        low = turned[:, k : k + 1] - high
        pick = turned[:, top + k : top + k + 1]
        shares = shares + jnp.where(lane == pick, high, 0.0)
        shares = shares + jnp.where(lane == pick + EPG, low, 0.0)
    xs[0] = pack(shares).astype(BF16)
    each(nx, lambda k: x_shares(k).start())

    done(wgu.at[:, :, 0:L, :], lsem.at[0])
    done(gb, wsem.at[1])
    done(wgu.at[:, :, L : 2 * L, :], wsem.at[3])
    gain = jnp.concatenate([gain_ref[...], gb[0]], axis=1)
    bias = jnp.concatenate([bias_ref[...], gb[1]], axis=1)
    gain_high = gain.astype(BF16).astype(F32)
    bias_high = bias.astype(BF16).astype(F32)
    four = iota((16, 2 * L), 0)
    vectors = jnp.where(four == 0, gain_high, 0.0) + jnp.where(four == 1, gain - gain_high, 0.0)
    vectors = vectors + jnp.where(four == 2, bias_high, 0.0) + jnp.where(four == 3, bias - bias_high, 0.0)
    vectors = vectors.astype(BF16)
    for e in range(2):
        for g in range(2):
            line = jnp.dot(vectors, wgu[g, e], preferred_element_type=F32)
            for j in range(per_expert):
                piece = line[:, j * L : (j + 1) * L]
                ax1s[e * per_expert + j, 0:1, g * L : (g + 1) * L] = piece[0:1] + piece[1:2]
                ax1s[e * per_expert + j, 1:2, g * L : (g + 1) * L] = piece[2:3] + piece[3:4]
    ax1r[0] = ax1s[y]

    done(xt.at[pl.ds(1, 2 * nx - 1)], rsem.at[0])

    for k in range(2 * nx):
        tr[z, k] = xt[k, z]

    def z_copy(to):
        device = {"ep": to * nx + x, "tp": tp}
        remote(xt.at[:, to], tr.at[z], ssem.at[2], tsem.at[own_batch], device).start()

    def z_ready_copy(to):
        pl.semaphore_wait(zready.at[to], 1)
        z_copy(to)

    planes(first, z, z_copy)
    planes(z + 1, nz, z_ready_copy)

    def z_shares(d):
        return remote(zs.at[lax.rem(z + d, nz)], sr.at[z], ssem.at[3], rsem.at[3], dev(dz=d))

    done(xs.at[pl.ds(1, nx - 1)], rsem.at[1])
    blocks = [xs[dx].astype(F32) for dx in range(nx)]
    for d in range(nz):
        block = [b[d * CAP : (d + 1) * CAP, :] for b in blocks]
        zs[d] = jnp.concatenate(block, axis=0).astype(BF16)
    sr[z] = zs[z]
    each(nz, lambda d: z_shares(d).start())

    @pl.when(rank < ny - 1)
    def _():
        pl.semaphore_wait(yready, ny - 1 - rank)

    def a1_copy(d):
        return remote(ax1s.at[(y + d) % ny], ax1r.at[d], ssem.at[4], rsem.at[4], dev(dy=d))

    each(ny, lambda d: a1_copy(d).start())

    cuts = [0, EARLY, nz]

    def rows_of(b):
        return pl.ds(cuts[b] * per_plane, (cuts[b + 1] - cuts[b]) * per_plane)

    def p_copy(b, d):
        here = rows_of(b)
        return remote(
            ps.at[d - 1, :, here], pr.at[d - 1, :, here], ssem.at[6], psem.at[b, d - 1], dev(dy=d)
        )

    def a2_copy(b, d):
        return remote(ax2s.at[b], ax2r.at[b, d], ssem.at[5], asem.at[b], dev(dy=d))

    gate_own, up_own = [], []
    for b in range(2):
        slots = range(cuts[b], cuts[b + 1])
        here = rows_of(b)
        batch_rows = here.size

        @pl.when(own_batch == b)
        def _():
            done(tr.at[pl.ds(1, len(slots) - 1)], tsem.at[b])

        @pl.when(own_batch != b)
        def _():
            done(tr.at[pl.ds(0, len(slots))], tsem.at[b])

        values = [
            jnp.concatenate([tr[i, 2 * dx + dc].astype(F32) for i in slots for dx in range(nx)], axis=0)
            for dc in range(2)
        ]
        values = jnp.concatenate(values, axis=1)
        middle = jnp.sum(values, axis=1, keepdims=True) * (1.0 / (2 * L))
        values = values - middle
        scaled = (values * gain).astype(BF16)
        for place, d in enumerate(far_first(ny) + [0]):
            q = (y + d) % ny
            e = q // per_expert
            cols = pl.ds(pl.multiple_of((q % per_expert) * L, L), L)
            gate_part = jnp.dot(scaled, wgu[0, e, :, cols], preferred_element_type=F32)
            up_part = jnp.dot(scaled, wgu[1, e, :, cols], preferred_element_type=F32)
            if d == 0:
                gate_own.append(gate_part)
                up_own.append(up_part)
            else:
                ps[d - 1, 0, here] = gate_part.astype(BF16)
                ps[d - 1, 1, here] = up_part.astype(BF16)
                p_copy(b, d).start()
            if place == 0:
                squares = jnp.sum(values * values, axis=1, keepdims=True)
                lanes = iota((batch_rows, L), 1)
                columns = jnp.where(lanes == 0, middle, 0.0) + jnp.where(lanes == 1, squares, 0.0)
                columns = jnp.transpose(columns)
                ax2s[b, :, 0:batch_rows] = columns[0:2, :]
                ax2r[b, 0, :, 0:batch_rows] = columns[0:2, :]
                each(ny, lambda d: a2_copy(b, d).start())

    def h_copy(b, d):
        here = rows_of(b)
        return remote(hb.at[0, here], hb.at[d, here], ssem.at[7], hsem.at[b, d - 1], dev(dy=d))

    done(sr.at[pl.ds(1, nz - 1)], rsem.at[3])
    done(ax1r.at[pl.ds(1, ny - 1)], rsem.at[4])
    expert = 2 * x + y // per_expert
    gate_bias = up_bias = jnp.zeros((1, L), F32)
    for d in range(ny):
        gate_bias = gate_bias + ax1r[d, 1:2, 0:L]
        up_bias = up_bias + ax1r[d, 1:2, L : 2 * L]
    for b in range(2):
        here = rows_of(b)
        batch_rows = here.size
        lanes = iota((batch_rows, L), 1)
        share = jnp.concatenate([sr[i].astype(F32) for i in range(cuts[b], cuts[b + 1])], axis=0)
        share = jnp.sum(
            jnp.where((lanes == expert) | (lanes == expert + EPG), share, 0.0), axis=1, keepdims=True
        )
        done(ax2r.at[b, pl.ds(1, ny - 1)], asem.at[b])
        means = [ax2r[b, d, 0:1, 0:batch_rows] for d in range(ny)]
        center = sum(means) * (1.0 / ny)
        shifts = [m - center for m in means]
        spread = sum(ax2r[b, d, 1:2, 0:batch_rows] for d in range(ny))
        spread = spread + (features // ny) * sum(s * s for s in shifts)
        scale = lax.rsqrt(spread * (1.0 / features) + norm_epsilon)
        stack = iota((16, batch_rows), 0)
        table = jnp.where(stack == ny, scale, 0.0)
        for d in range(ny):
            table = table + jnp.where(stack == d, shifts[d], 0.0)
        table = jnp.transpose(table)
        scale = table[:, ny : ny + 1]
        gate, up = gate_own[b], up_own[b]
        for d in range(ny):
            shift = table[:, d : d + 1]
            gate = gate + shift * ax1r[d, 0:1, 0:L]
            up = up + shift * ax1r[d, 0:1, L : 2 * L]
        for d in far_first(ny):
            p_copy(b, d).wait_recv()
            gate = gate + pr[d - 1, 0, here].astype(F32)
            up = up + pr[d - 1, 1, here].astype(F32)
        gate = gate * scale + gate_bias
        up = up * scale + up_bias
        hb[0, here] = (share * (gate / (1.0 + jnp.exp(-gate)) * up)).astype(BF16)
        for d in far_first(ny):
            h_copy(b, d).start()

    def down(b, d):
        q = (y - d + ny) % ny
        units = pl.ds(pl.multiple_of((q % per_expert) * L, L), L)
        return jnp.dot(hb[d, rows_of(b)], wd[q // per_expert, units, :], preferred_element_type=F32)

    done(wd.at[:, :, 0:L], lsem.at[1])
    done(wd.at[:, :, L : 2 * L], wsem.at[5])

    back_x = [lax.rem(x - d + nx, nx) for d in range(nx)]
    back_tp = [tp, tp + 1 - 2 * c]
    order = sorted(range(2 * nx), key=lambda k: -min(k // 2, nx - k // 2))

    def send_back(h, k):
        to = {"ep": h * nx + back_x[k // 2], "tp": back_tp[k % 2]}
        remote(os.at[h * 2 * nx + k], rr.at[z * 2 * nx + k], ssem.at[8], rsem.at[6], to).start()

    for b in range(2):
        total = down(b, 0)
        for d in sorted(range(1, ny), key=lambda d: min(d, ny - d)):
            h_copy(b, d).wait_recv()
            total = total + down(b, d)
        slots = range(cuts[b], cuts[b + 1])
        for h in slots:
            for k in range(2 * nx):
                at = (h - cuts[b]) * per_plane + k // 2 * CAP
                piece = total[at : at + CAP, (k % 2) * L : (k % 2 + 1) * L]
                os[h * 2 * nx + k] = piece.astype(BF16)
        for h in slots:
            for k in order:
                if k:
                    send_back(h, k)
                else:
                    pl.when(z != h)(functools.partial(send_back, h, k))
    rr[z * 2 * nx] = os[z * 2 * nx]

    done(xt.at[pl.ds(1, 2 * nx - 1)], ssem.at[0])
    done(xs.at[pl.ds(1, nx - 1)], ssem.at[1])
    done(tr.at[pl.ds(1, nz - 1)], ssem.at[2])
    done(sr.at[pl.ds(1, nz - 1)], ssem.at[3])
    done(ax1r.at[pl.ds(1, ny - 1)], ssem.at[4])
    done(ax2r.at[:, pl.ds(1, ny - 1)], ssem.at[5])
    done(ps, ssem.at[6])
    done(hb.at[pl.ds(1, ny - 1)], ssem.at[7])
    done(gb, wsem.at[0])
    done(wgu.at[:, :, 0:L, :], wsem.at[2])
    done(wd.at[:, :, 0:L], wsem.at[4])
    done(rr.at[pl.ds(1, 2 * nx * nz - 1)], rsem.at[6])

    result = jnp.zeros((tokens, L), F32)
    for d in range(nz):
        back = rr[d * 2 * nx].astype(F32)
        for k in range(1, 2 * nx):
            back = back + rr[d * 2 * nx + k].astype(F32)
        for s in range(CAP):
            at = d * CAP + s
            result = result + chosen[:, at : at + 1] * back[s : s + 1, :]
    out_ref[...] = result.astype(BF16)
    done(os.at[pl.ds(1, 2 * nx * nz - 1)], ssem.at[8])


def solution(mesh):
    nx = EPG // 2
    nz = mesh.shape["ep"] // nx
    ny = mesh.shape["tp"] // 2

    def on_device(tokens, gain, bias, group_pick, member_pick, probs, gate, up, down):
        width = tokens.shape[1]
        half = gate.shape[2] // 2
        rows = nz * CAP
        all_rows = nx * rows
        vmem, dma = pltpu.VMEM, pltpu.SemaphoreType.DMA
        whole = pl.BlockSpec(memory_space=pltpu.VMEM)
        away = pl.BlockSpec(memory_space=pl.ANY)
        return pl.pallas_call(
            functools.partial(kernel, nz, nx, ny, width * 2 * ny),
            out_shape=pltpu.VMEM(tokens.shape, BF16),
            in_specs=[away] * 9,
            out_specs=whole,
            scratch_shapes=[
                vmem(tokens.shape, BF16),
                vmem((1, L), F32),
                vmem((1, L), F32),
                vmem((1, tokens.shape[0]), jnp.int32),
                vmem(member_pick.shape[::-1], jnp.int32),
                vmem(probs.shape[::-1], F32),
                vmem((2, 2, 2 * L, half), BF16),
                vmem((2, half, 2 * L), BF16),
                vmem((2, 1, L), F32),
                vmem((2 * nx, nz, CAP, L), BF16),
                vmem((nx, rows, L), BF16),
                vmem((nz, nx * CAP, L), BF16),
                vmem((nz, 2 * nx, CAP, L), BF16),
                vmem((nz, nx * CAP, L), BF16),
                vmem((ny, 2, 2 * L), F32),
                vmem((ny, 2, 2 * L), F32),
                vmem((2, 2, L), F32),
                vmem((2, ny, 2, L), F32),
                vmem((ny - 1, 2, all_rows, L), BF16),
                vmem((ny - 1, 2, all_rows, L), BF16),
                vmem((ny, all_rows, L), BF16),
                vmem((2 * nx * nz, CAP, L), BF16),
                vmem((2 * nx * nz, CAP, L), BF16),
                pltpu.SemaphoreType.REGULAR((nz,)),
                pltpu.SemaphoreType.REGULAR,
                dma((6,)),
                dma((2,)),
                dma((6,)),
                dma((9,)),
                dma((7,)),
                dma((2,)),
                dma((2,)),
                dma((2, ny - 1)),
                dma((2, ny - 1)),
            ],
            compiler_params=pltpu.CompilerParams(collective_id=0, has_side_effects=True),
        )(tokens, gain.reshape(1, -1), bias.reshape(1, -1), group_pick.T, member_pick.T, probs.T, gate, up, down)

    return jax.shard_map(
        on_device,
        mesh=mesh,
        in_specs=(
            P("ep", "tp"),
            P("tp"),
            P("tp"),
            P("ep", None),
            P("ep", None),
            P("ep", None),
            P("ep", "tp", None),
            P("ep", "tp", None),
            P("ep", None, "tp"),
        ),
        out_specs=P("ep", "tp"),
        check_vma=False,
    )
```

```python
import functools

import jax
import jax.numpy as jnp
from jax import lax
from jax.experimental import pallas as pl
from jax.experimental.pallas import tpu as pltpu
from jax.sharding import PartitionSpec as P

EPG = 8
CAP = 2
EARLY = 2
norm_epsilon = 1e-05
MESH = pl.DeviceIdType.MESH
F32 = jnp.float32
BF16 = jnp.bfloat16
L = 128


def iota(shape, axis):
    return lax.broadcasted_iota(jnp.int32, shape, axis)


def far_first(n):
    return sorted(range(1, n), key=lambda d: -min(d, n - d))


def kernel(
    nz, nx, ny, features,
    tok_hbm, gain_hbm, bias_hbm, gp_hbm, mp_hbm, pp_hbm, gate_hbm, up_hbm, down_hbm,
    out_ref,
    tok_ref, gain_ref, bias_ref, gp_ref, mp_ref, pp_ref,
    wgu, wd, gb,
    xt, xs, zs, tr, sr, ax1s, ax1r, ax2s, ax2r, ps, pr, hb, os, rr,
    zready, yready, isem, lsem, wsem, ssem, rsem, tsem, asem, psem, hsem,
):
    tokens = tok_ref.shape[0]
    half = wgu.shape[3]
    rows = nz * CAP
    per_plane = nx * CAP
    all_rows = nz * per_plane
    per_expert = ny // 2
    ep, tp = lax.axis_index("ep"), lax.axis_index("tp")
    z, x, y, c = ep // nx, ep % nx, tp // 2, tp % 2

    def dev(dz=0, dx=0, dy=0, dc=0):
        return {
            "ep": lax.rem(z + dz + nz, nz) * nx + lax.rem(x + dx + nx, nx),
            "tp": lax.rem(y + dy + ny, ny) * 2 + lax.rem(c + dc, 2),
        }

    def remote(src, dst, ss, rs, device):
        return pltpu.make_async_remote_copy(
            src_ref=src, dst_ref=dst, send_sem=ss, recv_sem=rs, device_id=device, device_id_type=MESH
        )

    def each(n, body):
        lax.fori_loop(1, n, lambda d, carry: (body(d), carry)[1], 0)

    def done(ref, sem):
        pltpu.make_async_copy(ref, ref, sem).wait()

    def signal(sem, device):
        pl.semaphore_signal(sem, inc=1, device_id=device, device_id_type=MESH)

    inputs = [
        pltpu.make_async_copy(src, dst, isem.at[i])
        for i, (src, dst) in enumerate(
            (
                (gp_hbm, gp_ref),
                (mp_hbm, mp_ref),
                (pp_hbm, pp_ref),
                (tok_hbm, tok_ref),
                (gain_hbm, gain_ref),
                (bias_hbm, bias_ref),
            )
        )
    ]
    for copy in inputs:
        copy.start()

    def planes(low, high, body):
        lax.fori_loop(low, high, lambda to, carry: (body(to), carry)[1], 0)

    part = nz // 2
    side = z // part
    first = side * part

    def ranked(r):
        return r + r // per_expert * (3 * per_expert - 1 - 2 * r)

    rank = ranked(y)
    own_batch = (z + nz - EARLY) // nz
    barrier = pltpu.get_barrier_semaphore()

    def greet(to):
        signal(barrier, {"ep": to * nx + x, "tp": tp})

    planes(z + 1, first + part, greet)
    each(2 * nx, lambda k: signal(barrier, dev(dx=k // 2, dc=k % 2)))

    planes(rank + 1, ny, lambda r: signal(barrier, {"ep": ep, "tp": 2 * ranked(r) + c}))

    mine = pl.ds(pl.multiple_of(c * half, half), half)
    other = pl.ds(pl.multiple_of((1 - c) * half, half), half)
    pltpu.make_async_copy(gate_hbm.at[:, :, mine], wgu.at[0, :, 0:L, :], lsem.at[0]).start()
    pltpu.make_async_copy(up_hbm.at[:, :, mine], wgu.at[1, :, 0:L, :], lsem.at[0]).start()
    pltpu.make_async_copy(down_hbm.at[:, mine, :], wd.at[:, :, 0:L], lsem.at[1]).start()

    for copy in inputs:
        copy.wait()

    group = gp_ref[...]
    row = iota((rows, tokens), 0)
    lane = iota((rows, tokens), 1)
    member = (group == row // CAP).astype(F32)
    count = jnp.zeros((rows, tokens), F32)
    for t in range(tokens - 1):
        count = count + jnp.where(lane > t, member[:, t : t + 1], 0.0)
    rowwise = member * (count == (row % CAP).astype(F32)).astype(F32)
    def pack(source):
        packed = jnp.zeros((rows, L), F32)
        for t in range(tokens):
            packed = packed + rowwise[:, t : t + 1] * source[t : t + 1, :]
        return packed

    packed = pack(tok_ref[...].astype(F32))
    for d in range(nz):
        xt[0, d] = packed[d * CAP : (d + 1) * CAP, :].astype(BF16)

    pl.semaphore_wait(barrier, (2 * nx - 1) + z + rank)
    planes(0, z, lambda to: signal(zready.at[z], {"ep": to * nx + x, "tp": tp}))
    planes(0, rank, lambda r: signal(yready, {"ep": ep, "tp": 2 * ranked(r) + c}))

    @pl.when(side == 0)
    def _():
        planes(part, nz, greet)

    def x_copy(k):
        return remote(xt.at[0], xt.at[k], ssem.at[0], rsem.at[0], dev(dx=k // 2, dc=k % 2))

    def x_shares(dx):
        return remote(xs.at[0], xs.at[dx], ssem.at[1], rsem.at[1], dev(dx=dx))

    each(2 * nx, lambda k: x_copy(k).start())

    go_x = [lax.rem(x + d, nx) for d in range(nx)]
    go_tp = [tp, tp + 1 - 2 * c]

    def straight(to):
        for k in range(2 * nx):
            device = {"ep": to * nx + go_x[k // 2], "tp": go_tp[k % 2]}
            remote(xt.at[0, to], tr.at[z, k], ssem.at[2], tsem.at[own_batch], device).start()

    @pl.when(side == 1)
    def _():
        planes(0, part, straight)

    to = dev(dc=1)
    remote(gain_ref, gb.at[0], wsem.at[0], wsem.at[1], to).start()
    remote(bias_ref, gb.at[1], wsem.at[0], wsem.at[1], to).start()
    remote(gate_hbm.at[:, :, other], wgu.at[0, :, L : 2 * L, :], wsem.at[2], wsem.at[3], to).start()
    remote(up_hbm.at[:, :, other], wgu.at[1, :, L : 2 * L, :], wsem.at[2], wsem.at[3], to).start()
    remote(down_hbm.at[:, other, :], wd.at[:, :, L : 2 * L], wsem.at[4], wsem.at[5], to).start()

    probs = pp_ref[...]
    share = probs / jnp.sum(probs, axis=0, keepdims=True)
    top = probs.shape[0]
    table = [share[k : k + 1] for k in range(top)]
    table = table + [mp_ref[k : k + 1].astype(F32) for k in range(top)] + [rowwise]
    table = jnp.concatenate(table, axis=0)
    table = jnp.concatenate([table, jnp.zeros((2 * top + rows, L - tokens), F32)], axis=1)
    turned = jnp.transpose(table)[0:tokens, :]
    chosen = turned[:, 2 * top :]
    lane = iota((tokens, L), 1).astype(F32)
    shares = jnp.zeros((tokens, L), F32)
    for k in range(top):
        high = turned[:, k : k + 1].astype(BF16).astype(F32)
        low = turned[:, k : k + 1] - high
        pick = turned[:, top + k : top + k + 1]
        shares = shares + jnp.where(lane == pick, high, 0.0)
        shares = shares + jnp.where(lane == pick + EPG, low, 0.0)
    xs[0] = pack(shares).astype(BF16)
    each(nx, lambda k: x_shares(k).start())

    done(wgu.at[:, :, 0:L, :], lsem.at[0])
    done(gb, wsem.at[1])
    done(wgu.at[:, :, L : 2 * L, :], wsem.at[3])
    gain = jnp.concatenate([gain_ref[...], gb[0]], axis=1)
    bias = jnp.concatenate([bias_ref[...], gb[1]], axis=1)
    gain_high = gain.astype(BF16).astype(F32)
    bias_high = bias.astype(BF16).astype(F32)
    four = iota((16, 2 * L), 0)
    vectors = jnp.where(four == 0, gain_high, 0.0) + jnp.where(four == 1, gain - gain_high, 0.0)
    vectors = vectors + jnp.where(four == 2, bias_high, 0.0) + jnp.where(four == 3, bias - bias_high, 0.0)
    vectors = vectors.astype(BF16)
    for e in range(2):
        for g in range(2):
            line = jnp.dot(vectors, wgu[g, e], preferred_element_type=F32)
            for j in range(per_expert):
                piece = line[:, j * L : (j + 1) * L]
                ax1s[e * per_expert + j, 0:1, g * L : (g + 1) * L] = piece[0:1] + piece[1:2]
                ax1s[e * per_expert + j, 1:2, g * L : (g + 1) * L] = piece[2:3] + piece[3:4]
    ax1r[0] = ax1s[y]

    done(xt.at[pl.ds(1, 2 * nx - 1)], rsem.at[0])

    for k in range(2 * nx):
        tr[z, k] = xt[k, z]

    def z_copy(to):
        device = {"ep": to * nx + x, "tp": tp}
        remote(xt.at[:, to], tr.at[z], ssem.at[2], tsem.at[own_batch], device).start()

    def z_ready_copy(to):
        pl.semaphore_wait(zready.at[to], 1)
        z_copy(to)

    planes(first, z, z_copy)
    planes(z + 1, nz, z_ready_copy)

    def z_shares(d):
        return remote(zs.at[lax.rem(z + d, nz)], sr.at[z], ssem.at[3], rsem.at[3], dev(dz=d))

    done(xs.at[pl.ds(1, nx - 1)], rsem.at[1])
    blocks = [xs[dx].astype(F32) for dx in range(nx)]
    for d in range(nz):
        block = [b[d * CAP : (d + 1) * CAP, :] for b in blocks]
        zs[d] = jnp.concatenate(block, axis=0).astype(BF16)
    sr[z] = zs[z]
    each(nz, lambda d: z_shares(d).start())

    @pl.when(rank < ny - 1)
    def _():
        pl.semaphore_wait(yready, ny - 1 - rank)

    def a1_copy(d):
        return remote(ax1s.at[(y + d) % ny], ax1r.at[d], ssem.at[4], rsem.at[4], dev(dy=d))

    each(ny, lambda d: a1_copy(d).start())

    cuts = [0, EARLY, nz]

    def rows_of(b):
        return pl.ds(cuts[b] * per_plane, (cuts[b + 1] - cuts[b]) * per_plane)

    def p_copy(b, d):
        here = rows_of(b)
        return remote(
            ps.at[d - 1, :, here], pr.at[d - 1, :, here], ssem.at[6], psem.at[b, d - 1], dev(dy=d)
        )

    def a2_copy(b, d):
        return remote(ax2s.at[b], ax2r.at[b, d], ssem.at[5], asem.at[b], dev(dy=d))

    gate_own, up_own = [], []
    for b in range(2):
        slots = range(cuts[b], cuts[b + 1])
        here = rows_of(b)
        batch_rows = here.size

        @pl.when(own_batch == b)
        def _():
            done(tr.at[pl.ds(1, len(slots) - 1)], tsem.at[b])

        @pl.when(own_batch != b)
        def _():
            done(tr.at[pl.ds(0, len(slots))], tsem.at[b])

        values = [
            jnp.concatenate([tr[i, 2 * dx + dc].astype(F32) for i in slots for dx in range(nx)], axis=0)
            for dc in range(2)
        ]
        values = jnp.concatenate(values, axis=1)
        middle = jnp.sum(values, axis=1, keepdims=True) * (1.0 / (2 * L))
        values = values - middle
        scaled = (values * gain).astype(BF16)
        waiting = []
        for place, d in enumerate(far_first(ny) + [0]):
            q = (y + d) % ny
            e = q // per_expert
            cols = pl.ds(pl.multiple_of((q % per_expert) * L, L), L)
            gate_part = jnp.dot(scaled, wgu[0, e, :, cols], preferred_element_type=F32)
            up_part = jnp.dot(scaled, wgu[1, e, :, cols], preferred_element_type=F32)
            if d == 0:
                gate_own.append(gate_part)
                up_own.append(up_part)
            else:
                ps[d - 1, 0, here] = gate_part.astype(BF16)
                ps[d - 1, 1, here] = up_part.astype(BF16)
                if place == 0:
                    p_copy(b, d).start()
                else:
                    waiting.append(d)
                if place in (2, ny - 2):

                    @pl.when(ep >= 0)
                    def _():
                        for w in waiting:
                            p_copy(b, w).start()

                    waiting = []
            if place == 0:
                squares = jnp.sum(values * values, axis=1, keepdims=True)
                lanes = iota((batch_rows, L), 1)
                columns = jnp.where(lanes == 0, middle, 0.0) + jnp.where(lanes == 1, squares, 0.0)
                columns = jnp.transpose(columns)
                ax2s[b, :, 0:batch_rows] = columns[0:2, :]
                ax2r[b, 0, :, 0:batch_rows] = columns[0:2, :]
                each(ny, lambda d: a2_copy(b, d).start())

    def h_copy(b, d):
        here = rows_of(b)
        return remote(hb.at[0, here], hb.at[d, here], ssem.at[7], hsem.at[b, d - 1], dev(dy=d))

    done(sr.at[pl.ds(1, nz - 1)], rsem.at[3])
    done(ax1r.at[pl.ds(1, ny - 1)], rsem.at[4])
    expert = 2 * x + y // per_expert
    gate_bias = up_bias = jnp.zeros((1, L), F32)
    for d in range(ny):
        gate_bias = gate_bias + ax1r[d, 1:2, 0:L]
        up_bias = up_bias + ax1r[d, 1:2, L : 2 * L]
    for b in range(2):
        here = rows_of(b)
        batch_rows = here.size
        lanes = iota((batch_rows, L), 1)
        share = jnp.concatenate([sr[i].astype(F32) for i in range(cuts[b], cuts[b + 1])], axis=0)
        share = jnp.sum(
            jnp.where((lanes == expert) | (lanes == expert + EPG), share, 0.0), axis=1, keepdims=True
        )
        done(ax2r.at[b, pl.ds(1, ny - 1)], asem.at[b])
        means = [ax2r[b, d, 0:1, 0:batch_rows] for d in range(ny)]
        center = sum(means) * (1.0 / ny)
        shifts = [m - center for m in means]
        spread = sum(ax2r[b, d, 1:2, 0:batch_rows] for d in range(ny))
        spread = spread + (features // ny) * sum(s * s for s in shifts)
        scale = lax.rsqrt(spread * (1.0 / features) + norm_epsilon)
        stack = iota((16, batch_rows), 0)
        table = jnp.where(stack == ny, scale, 0.0)
        for d in range(ny):
            table = table + jnp.where(stack == d, shifts[d], 0.0)
        table = jnp.transpose(table)
        scale = table[:, ny : ny + 1]
        gate, up = gate_own[b], up_own[b]
        for d in range(ny):
            shift = table[:, d : d + 1]
            gate = gate + shift * ax1r[d, 0:1, 0:L]
            up = up + shift * ax1r[d, 0:1, L : 2 * L]
        for d in far_first(ny):
            p_copy(b, d).wait_recv()
            gate = gate + pr[d - 1, 0, here].astype(F32)
            up = up + pr[d - 1, 1, here].astype(F32)
        gate = gate * scale + gate_bias
        up = up * scale + up_bias
        hb[0, here] = (share * (gate / (1.0 + jnp.exp(-gate)) * up)).astype(BF16)

        @pl.when(ep >= 0)
        def _():
            for d in far_first(ny):
                h_copy(b, d).start()


    def down(b, d):
        q = (y - d + ny) % ny
        units = pl.ds(pl.multiple_of((q % per_expert) * L, L), L)
        return jnp.dot(hb[d, rows_of(b)], wd[q // per_expert, units, :], preferred_element_type=F32)

    done(wd.at[:, :, 0:L], lsem.at[1])
    done(wd.at[:, :, L : 2 * L], wsem.at[5])

    back_x = [lax.rem(x - d + nx, nx) for d in range(nx)]
    back_tp = [tp, tp + 1 - 2 * c]
    order = sorted(range(2 * nx), key=lambda k: -min(k // 2, nx - k // 2))

    def send_back(h, k):
        to = {"ep": h * nx + back_x[k // 2], "tp": back_tp[k % 2]}
        remote(os.at[h * 2 * nx + k], rr.at[z * 2 * nx + k], ssem.at[8], rsem.at[6], to).start()

    for b in range(2):
        total = down(b, 0)
        for d in sorted(range(1, ny), key=lambda d: min(d, ny - d)):
            h_copy(b, d).wait_recv()
            total = total + down(b, d)
        slots = range(cuts[b], cuts[b + 1])
        for h in slots:
            for k in range(2 * nx):
                at = (h - cuts[b]) * per_plane + k // 2 * CAP
                piece = total[at : at + CAP, (k % 2) * L : (k % 2 + 1) * L]
                os[h * 2 * nx + k] = piece.astype(BF16)
        for h in slots:
            for k in order:
                if k:
                    send_back(h, k)
                else:
                    pl.when(z != h)(functools.partial(send_back, h, k))
    rr[z * 2 * nx] = os[z * 2 * nx]

    done(xt.at[pl.ds(1, 2 * nx - 1)], ssem.at[0])
    done(xs.at[pl.ds(1, nx - 1)], ssem.at[1])
    done(tr.at[pl.ds(1, nz - 1)], ssem.at[2])
    done(sr.at[pl.ds(1, nz - 1)], ssem.at[3])
    done(ax1r.at[pl.ds(1, ny - 1)], ssem.at[4])
    done(ax2r.at[:, pl.ds(1, ny - 1)], ssem.at[5])
    done(ps, ssem.at[6])
    done(hb.at[pl.ds(1, ny - 1)], ssem.at[7])
    done(gb, wsem.at[0])
    done(wgu.at[:, :, 0:L, :], wsem.at[2])
    done(wd.at[:, :, 0:L], wsem.at[4])
    done(rr.at[pl.ds(1, 2 * nx * nz - 1)], rsem.at[6])

    result = jnp.zeros((tokens, L), F32)
    for d in range(nz):
        back = rr[d * 2 * nx].astype(F32)
        for k in range(1, 2 * nx):
            back = back + rr[d * 2 * nx + k].astype(F32)
        for s in range(CAP):
            at = d * CAP + s
            result = result + chosen[:, at : at + 1] * back[s : s + 1, :]
    out_ref[...] = result.astype(BF16)
    done(os.at[pl.ds(1, 2 * nx * nz - 1)], ssem.at[8])


def solution(mesh):
    nx = EPG // 2
    nz = mesh.shape["ep"] // nx
    ny = mesh.shape["tp"] // 2

    def on_device(tokens, gain, bias, group_pick, member_pick, probs, gate, up, down):
        width = tokens.shape[1]
        half = gate.shape[2] // 2
        rows = nz * CAP
        all_rows = nx * rows
        vmem, dma = pltpu.VMEM, pltpu.SemaphoreType.DMA
        whole = pl.BlockSpec(memory_space=pltpu.VMEM)
        away = pl.BlockSpec(memory_space=pl.ANY)
        return pl.pallas_call(
            functools.partial(kernel, nz, nx, ny, width * 2 * ny),
            out_shape=pltpu.VMEM(tokens.shape, BF16),
            in_specs=[away] * 9,
            out_specs=whole,
            scratch_shapes=[
                vmem(tokens.shape, BF16),
                vmem((1, L), F32),
                vmem((1, L), F32),
                vmem((1, tokens.shape[0]), jnp.int32),
                vmem(member_pick.shape[::-1], jnp.int32),
                vmem(probs.shape[::-1], F32),
                vmem((2, 2, 2 * L, half), BF16),
                vmem((2, half, 2 * L), BF16),
                vmem((2, 1, L), F32),
                vmem((2 * nx, nz, CAP, L), BF16),
                vmem((nx, rows, L), BF16),
                vmem((nz, nx * CAP, L), BF16),
                vmem((nz, 2 * nx, CAP, L), BF16),
                vmem((nz, nx * CAP, L), BF16),
                vmem((ny, 2, 2 * L), F32),
                vmem((ny, 2, 2 * L), F32),
                vmem((2, 2, L), F32),
                vmem((2, ny, 2, L), F32),
                vmem((ny - 1, 2, all_rows, L), BF16),
                vmem((ny - 1, 2, all_rows, L), BF16),
                vmem((ny, all_rows, L), BF16),
                vmem((2 * nx * nz, CAP, L), BF16),
                vmem((2 * nx * nz, CAP, L), BF16),
                pltpu.SemaphoreType.REGULAR((nz,)),
                pltpu.SemaphoreType.REGULAR,
                dma((6,)),
                dma((2,)),
                dma((6,)),
                dma((9,)),
                dma((7,)),
                dma((2,)),
                dma((2,)),
                dma((2, ny - 1)),
                dma((2, ny - 1)),
            ],
            compiler_params=pltpu.CompilerParams(collective_id=0, has_side_effects=True),
        )(tokens, gain.reshape(1, -1), bias.reshape(1, -1), group_pick.T, member_pick.T, probs.T, gate, up, down)

    return jax.shard_map(
        on_device,
        mesh=mesh,
        in_specs=(
            P("ep", "tp"),
            P("tp"),
            P("tp"),
            P("ep", None),
            P("ep", None),
            P("ep", None),
            P("ep", "tp", None),
            P("ep", "tp", None),
            P("ep", None, "tp"),
        ),
        out_specs=P("ep", "tp"),
        check_vma=False,
    )
```

```python
import functools

import jax
import jax.numpy as jnp
from jax import lax
from jax.experimental import pallas as pl
from jax.experimental.pallas import tpu as pltpu
from jax.sharding import PartitionSpec as P

EPG = 8
CAP = 2
EARLY = 2
norm_epsilon = 1e-05
MESH = pl.DeviceIdType.MESH
F32 = jnp.float32
BF16 = jnp.bfloat16
L = 128


def iota(shape, axis):
    return lax.broadcasted_iota(jnp.int32, shape, axis)


def far_first(n):
    return sorted(range(1, n), key=lambda d: -min(d, n - d))


def kernel(
    nz, nx, ny, features,
    tok_hbm, gain_hbm, bias_hbm, gp_hbm, mp_hbm, pp_hbm, gate_hbm, up_hbm, down_hbm,
    out_ref,
    tok_ref, gain_ref, bias_ref, gp_ref, mp_ref, pp_ref,
    wgu, wd, gb,
    xt, xs, zs, tr, sr, ax1s, ax1r, ax2s, ax2r, ps, pr, hb, os, rr,
    zready, yready, isem, lsem, wsem, ssem, rsem, tsem, asem, psem, hsem,
):
    tokens = tok_ref.shape[0]
    half = wgu.shape[3]
    rows = nz * CAP
    per_plane = nx * CAP
    all_rows = nz * per_plane
    per_expert = ny // 2
    ep, tp = lax.axis_index("ep"), lax.axis_index("tp")
    z, x, y, c = ep // nx, ep % nx, tp // 2, tp % 2

    def dev(dz=0, dx=0, dy=0, dc=0):
        return {
            "ep": lax.rem(z + dz + nz, nz) * nx + lax.rem(x + dx + nx, nx),
            "tp": lax.rem(y + dy + ny, ny) * 2 + lax.rem(c + dc, 2),
        }

    def remote(src, dst, ss, rs, device):
        return pltpu.make_async_remote_copy(
            src_ref=src, dst_ref=dst, send_sem=ss, recv_sem=rs, device_id=device, device_id_type=MESH
        )

    def each(n, body):
        lax.fori_loop(1, n, lambda d, carry: (body(d), carry)[1], 0)

    def done(ref, sem):
        pltpu.make_async_copy(ref, ref, sem).wait()

    def signal(sem, device):
        pl.semaphore_signal(sem, inc=1, device_id=device, device_id_type=MESH)

    inputs = [
        pltpu.make_async_copy(src, dst, isem.at[i])
        for i, (src, dst) in enumerate(
            (
                (gp_hbm, gp_ref),
                (mp_hbm, mp_ref),
                (pp_hbm, pp_ref),
                (tok_hbm, tok_ref),
                (gain_hbm, gain_ref),
                (bias_hbm, bias_ref),
            )
        )
    ]
    for copy in inputs:
        copy.start()

    def planes(low, high, body):
        lax.fori_loop(low, high, lambda to, carry: (body(to), carry)[1], 0)

    part = nz // 2
    side = z // part
    first = side * part

    def ranked(r):
        return r + r // per_expert * (3 * per_expert - 1 - 2 * r)

    rank = ranked(y)
    own_batch = (z + nz - EARLY) // nz
    barrier = pltpu.get_barrier_semaphore()

    def greet(to):
        signal(barrier, {"ep": to * nx + x, "tp": tp})

    planes(z + 1, first + part, greet)
    go_x = [lax.rem(x + d, nx) for d in range(nx)]
    go_tp = [tp, tp + 1 - 2 * c]

    def mate(k):
        return {"ep": z * nx + go_x[k // 2], "tp": go_tp[k % 2]}

    for k in range(1, 2 * nx):
        signal(barrier, mate(k))

    planes(rank + 1, ny, lambda r: signal(barrier, {"ep": ep, "tp": 2 * ranked(r) + c}))

    mine = pl.ds(pl.multiple_of(c * half, half), half)
    other = pl.ds(pl.multiple_of((1 - c) * half, half), half)
    pltpu.make_async_copy(gate_hbm.at[:, :, mine], wgu.at[0, :, 0:L, :], lsem.at[0]).start()
    pltpu.make_async_copy(up_hbm.at[:, :, mine], wgu.at[1, :, 0:L, :], lsem.at[0]).start()
    pltpu.make_async_copy(down_hbm.at[:, mine, :], wd.at[:, :, 0:L], lsem.at[1]).start()

    for copy in inputs:
        copy.wait()

    group = gp_ref[...]
    row = iota((rows, tokens), 0)
    lane = iota((rows, tokens), 1)
    member = (group == row // CAP).astype(F32)
    count = jnp.zeros((rows, tokens), F32)
    for t in range(tokens - 1):
        count = count + jnp.where(lane > t, member[:, t : t + 1], 0.0)
    rowwise = member * (count == (row % CAP).astype(F32)).astype(F32)
    def pack(source):
        packed = jnp.zeros((rows, L), F32)
        for t in range(tokens):
            packed = packed + rowwise[:, t : t + 1] * source[t : t + 1, :]
        return packed

    packed = pack(tok_ref[...].astype(F32))
    for d in range(nz):
        xt[0, d] = packed[d * CAP : (d + 1) * CAP, :].astype(BF16)

    pl.semaphore_wait(barrier, (2 * nx - 1) + z + rank)
    planes(0, z, lambda to: signal(zready.at[z], {"ep": to * nx + x, "tp": tp}))
    planes(0, rank, lambda r: signal(yready, {"ep": ep, "tp": 2 * ranked(r) + c}))

    @pl.when(side == 0)
    def _():
        planes(part, nz, greet)

    def x_copy(k):
        return remote(xt.at[0], xt.at[k], ssem.at[0], rsem.at[0], mate(k))

    def x_shares(dx):
        return remote(xs.at[0], xs.at[dx], ssem.at[1], rsem.at[1], mate(2 * dx))

    for k in range(1, 2 * nx):
        x_copy(k).start()


    def straight(to):
        for k in range(2 * nx):
            device = {"ep": to * nx + go_x[k // 2], "tp": go_tp[k % 2]}
            remote(xt.at[0, to], tr.at[z, k], ssem.at[2], tsem.at[own_batch], device).start()

    @pl.when(side == 1)
    def _():
        planes(0, part, straight)

    to = dev(dc=1)
    remote(gain_ref, gb.at[0], wsem.at[0], wsem.at[1], to).start()
    remote(bias_ref, gb.at[1], wsem.at[0], wsem.at[1], to).start()
    remote(gate_hbm.at[:, :, other], wgu.at[0, :, L : 2 * L, :], wsem.at[2], wsem.at[3], to).start()
    remote(up_hbm.at[:, :, other], wgu.at[1, :, L : 2 * L, :], wsem.at[2], wsem.at[3], to).start()
    remote(down_hbm.at[:, other, :], wd.at[:, :, L : 2 * L], wsem.at[4], wsem.at[5], to).start()

    probs = pp_ref[...]
    share = probs / jnp.sum(probs, axis=0, keepdims=True)
    top = probs.shape[0]
    table = [share[k : k + 1] for k in range(top)]
    table = table + [mp_ref[k : k + 1].astype(F32) for k in range(top)] + [rowwise]
    table = jnp.concatenate(table, axis=0)
    table = jnp.concatenate([table, jnp.zeros((2 * top + rows, L - tokens), F32)], axis=1)
    turned = jnp.transpose(table)[0:tokens, :]
    chosen = turned[:, 2 * top :]
    lane = iota((tokens, L), 1).astype(F32)
    shares = jnp.zeros((tokens, L), F32)
    for k in range(top):
        high = turned[:, k : k + 1].astype(BF16).astype(F32)
        low = turned[:, k : k + 1] - high
        pick = turned[:, top + k : top + k + 1]
        shares = shares + jnp.where(lane == pick, high, 0.0)
        shares = shares + jnp.where(lane == pick + EPG, low, 0.0)
    xs[0] = pack(shares).astype(BF16)
    for dx in range(1, nx):
        x_shares(dx).start()

    done(wgu.at[:, :, 0:L, :], lsem.at[0])
    done(gb, wsem.at[1])
    done(wgu.at[:, :, L : 2 * L, :], wsem.at[3])
    gain = jnp.concatenate([gain_ref[...], gb[0]], axis=1)
    bias = jnp.concatenate([bias_ref[...], gb[1]], axis=1)
    gain_high = gain.astype(BF16).astype(F32)
    bias_high = bias.astype(BF16).astype(F32)
    four = iota((16, 2 * L), 0)
    vectors = jnp.where(four == 0, gain_high, 0.0) + jnp.where(four == 1, gain - gain_high, 0.0)
    vectors = vectors + jnp.where(four == 2, bias_high, 0.0) + jnp.where(four == 3, bias - bias_high, 0.0)
    vectors = vectors.astype(BF16)
    for e in range(2):
        for g in range(2):
            line = jnp.dot(vectors, wgu[g, e], preferred_element_type=F32)
            for j in range(per_expert):
                piece = line[:, j * L : (j + 1) * L]
                ax1s[e * per_expert + j, 0:1, g * L : (g + 1) * L] = piece[0:1] + piece[1:2]
                ax1s[e * per_expert + j, 1:2, g * L : (g + 1) * L] = piece[2:3] + piece[3:4]
    ax1r[0] = ax1s[y]

    done(xt.at[pl.ds(1, 2 * nx - 1)], rsem.at[0])

    for k in range(2 * nx):
        tr[z, k] = xt[k, z]

    def z_copy(to):
        device = {"ep": to * nx + x, "tp": tp}
        remote(xt.at[:, to], tr.at[z], ssem.at[2], tsem.at[own_batch], device).start()

    def z_ready_copy(to):
        pl.semaphore_wait(zready.at[to], 1)
        z_copy(to)

    planes(first, z, z_copy)
    planes(z + 1, nz, z_ready_copy)

    def z_shares(d):
        return remote(zs.at[lax.rem(z + d, nz)], sr.at[z], ssem.at[3], rsem.at[3], dev(dz=d))

    done(xs.at[pl.ds(1, nx - 1)], rsem.at[1])
    blocks = [xs[dx].astype(F32) for dx in range(nx)]
    for d in range(nz):
        block = [b[d * CAP : (d + 1) * CAP, :] for b in blocks]
        zs[d] = jnp.concatenate(block, axis=0).astype(BF16)
    sr[z] = zs[z]
    each(nz, lambda d: z_shares(d).start())

    @pl.when(rank < ny - 1)
    def _():
        pl.semaphore_wait(yready, ny - 1 - rank)

    def a1_copy(d):
        return remote(ax1s.at[(y + d) % ny], ax1r.at[d], ssem.at[4], rsem.at[4], dev(dy=d))

    each(ny, lambda d: a1_copy(d).start())

    cuts = [0, EARLY, nz]

    def rows_of(b):
        return pl.ds(cuts[b] * per_plane, (cuts[b + 1] - cuts[b]) * per_plane)

    def p_copy(b, d):
        here = rows_of(b)
        return remote(
            ps.at[d - 1, :, here], pr.at[d - 1, :, here], ssem.at[6], psem.at[b, d - 1], dev(dy=d)
        )

    def a2_copy(b, d):
        return remote(ax2s.at[b], ax2r.at[b, d], ssem.at[5], asem.at[b], dev(dy=d))

    gate_own, up_own = [], []
    for b in range(2):
        slots = range(cuts[b], cuts[b + 1])
        here = rows_of(b)
        batch_rows = here.size

        @pl.when(own_batch == b)
        def _():
            done(tr.at[pl.ds(1, len(slots) - 1)], tsem.at[b])

        @pl.when(own_batch != b)
        def _():
            done(tr.at[pl.ds(0, len(slots))], tsem.at[b])

        values = [
            jnp.concatenate([tr[i, 2 * dx + dc].astype(F32) for i in slots for dx in range(nx)], axis=0)
            for dc in range(2)
        ]
        values = jnp.concatenate(values, axis=1)
        middle = jnp.sum(values, axis=1, keepdims=True) * (1.0 / (2 * L))
        values = values - middle
        scaled = (values * gain).astype(BF16)
        waiting = []
        for place, d in enumerate(far_first(ny) + [0]):
            q = (y + d) % ny
            e = q // per_expert
            cols = pl.ds(pl.multiple_of((q % per_expert) * L, L), L)
            gate_part = jnp.dot(scaled, wgu[0, e, :, cols], preferred_element_type=F32)
            up_part = jnp.dot(scaled, wgu[1, e, :, cols], preferred_element_type=F32)
            if d == 0:
                gate_own.append(gate_part)
                up_own.append(up_part)
            else:
                ps[d - 1, 0, here] = gate_part.astype(BF16)
                ps[d - 1, 1, here] = up_part.astype(BF16)
                if place:
                    waiting.append(d)
                if place in (2, ny - 2):

                    @pl.when(ep >= 0)
                    def _():
                        for w in waiting:
                            p_copy(b, w).start()

                    waiting = []
            if place == 0:
                squares = jnp.sum(values * values, axis=1, keepdims=True)
                lanes = iota((batch_rows, L), 1)
                columns = jnp.where(lanes == 0, middle, 0.0) + jnp.where(lanes == 1, squares, 0.0)
                columns = jnp.transpose(columns)
                ax2s[b, :, 0:batch_rows] = columns[0:2, :]
                ax2r[b, 0, :, 0:batch_rows] = columns[0:2, :]

                @pl.when(ep >= 0)
                def _():
                    for w in far_first(ny):
                        a2_copy(b, w).start()
                    p_copy(b, far_first(ny)[0]).start()


    def h_copy(b, d):
        here = rows_of(b)
        return remote(hb.at[0, here], hb.at[d, here], ssem.at[7], hsem.at[b, d - 1], dev(dy=d))

    done(sr.at[pl.ds(1, nz - 1)], rsem.at[3])
    done(ax1r.at[pl.ds(1, ny - 1)], rsem.at[4])
    expert = 2 * x + y // per_expert
    gate_bias = up_bias = jnp.zeros((1, L), F32)
    for d in range(ny):
        gate_bias = gate_bias + ax1r[d, 1:2, 0:L]
        up_bias = up_bias + ax1r[d, 1:2, L : 2 * L]
    for b in range(2):
        here = rows_of(b)
        batch_rows = here.size
        lanes = iota((batch_rows, L), 1)
        share = jnp.concatenate([sr[i].astype(F32) for i in range(cuts[b], cuts[b + 1])], axis=0)
        share = jnp.sum(
            jnp.where((lanes == expert) | (lanes == expert + EPG), share, 0.0), axis=1, keepdims=True
        )
        done(ax2r.at[b, pl.ds(1, ny - 1)], asem.at[b])
        means = [ax2r[b, d, 0:1, 0:batch_rows] for d in range(ny)]
        center = sum(means) * (1.0 / ny)
        shifts = [m - center for m in means]
        spread = sum(ax2r[b, d, 1:2, 0:batch_rows] for d in range(ny))
        spread = spread + (features // ny) * sum(s * s for s in shifts)
        scale = lax.rsqrt(spread * (1.0 / features) + norm_epsilon)
        stack = iota((16, batch_rows), 0)
        table = jnp.where(stack == ny, scale, 0.0)
        for d in range(ny):
            table = table + jnp.where(stack == d, shifts[d], 0.0)
        table = jnp.transpose(table)
        scale = table[:, ny : ny + 1]
        gate, up = gate_own[b], up_own[b]
        for d in range(ny):
            shift = table[:, d : d + 1]
            gate = gate + shift * ax1r[d, 0:1, 0:L]
            up = up + shift * ax1r[d, 0:1, L : 2 * L]
        for d in far_first(ny):
            p_copy(b, d).wait_recv()
            gate = gate + pr[d - 1, 0, here].astype(F32)
            up = up + pr[d - 1, 1, here].astype(F32)
        gate = gate * scale + gate_bias
        up = up * scale + up_bias
        hb[0, here] = (share * (gate / (1.0 + jnp.exp(-gate)) * up)).astype(BF16)

        @pl.when(ep >= 0)
        def _():
            for d in far_first(ny):
                h_copy(b, d).start()


    def down(b, d):
        q = (y - d + ny) % ny
        units = pl.ds(pl.multiple_of((q % per_expert) * L, L), L)
        return jnp.dot(hb[d, rows_of(b)], wd[q // per_expert, units, :], preferred_element_type=F32)

    done(wd.at[:, :, 0:L], lsem.at[1])
    done(wd.at[:, :, L : 2 * L], wsem.at[5])

    back_x = [lax.rem(x - d + nx, nx) for d in range(nx)]
    back_tp = [tp, tp + 1 - 2 * c]
    order = sorted(range(2 * nx), key=lambda k: -min(k // 2, nx - k // 2))

    def send_back(h, k):
        to = {"ep": h * nx + back_x[k // 2], "tp": back_tp[k % 2]}
        remote(os.at[h * 2 * nx + k], rr.at[z * 2 * nx + k], ssem.at[8], rsem.at[6], to).start()

    for b in range(2):
        total = down(b, 0)
        for d in sorted(range(1, ny), key=lambda d: min(d, ny - d)):
            h_copy(b, d).wait_recv()
            total = total + down(b, d)
        slots = range(cuts[b], cuts[b + 1])
        for h in slots:
            for k in range(2 * nx):
                at = (h - cuts[b]) * per_plane + k // 2 * CAP
                piece = total[at : at + CAP, (k % 2) * L : (k % 2 + 1) * L]
                os[h * 2 * nx + k] = piece.astype(BF16)
        for h in slots:
            for k in order:
                if k:
                    send_back(h, k)
                else:
                    pl.when(z != h)(functools.partial(send_back, h, k))
    rr[z * 2 * nx] = os[z * 2 * nx]

    done(xt.at[pl.ds(1, 2 * nx - 1)], ssem.at[0])
    done(xs.at[pl.ds(1, nx - 1)], ssem.at[1])
    done(tr.at[pl.ds(1, nz - 1)], ssem.at[2])
    done(sr.at[pl.ds(1, nz - 1)], ssem.at[3])
    done(ax1r.at[pl.ds(1, ny - 1)], ssem.at[4])
    done(ax2r.at[:, pl.ds(1, ny - 1)], ssem.at[5])
    done(ps, ssem.at[6])
    done(hb.at[pl.ds(1, ny - 1)], ssem.at[7])
    done(gb, wsem.at[0])
    done(wgu.at[:, :, 0:L, :], wsem.at[2])
    done(wd.at[:, :, 0:L], wsem.at[4])
    done(rr.at[pl.ds(1, 2 * nx * nz - 1)], rsem.at[6])

    result = jnp.zeros((tokens, L), F32)
    for d in range(nz):
        back = rr[d * 2 * nx].astype(F32)
        for k in range(1, 2 * nx):
            back = back + rr[d * 2 * nx + k].astype(F32)
        for s in range(CAP):
            at = d * CAP + s
            result = result + chosen[:, at : at + 1] * back[s : s + 1, :]
    out_ref[...] = result.astype(BF16)
    done(os.at[pl.ds(1, 2 * nx * nz - 1)], ssem.at[8])


def solution(mesh):
    nx = EPG // 2
    nz = mesh.shape["ep"] // nx
    ny = mesh.shape["tp"] // 2

    def on_device(tokens, gain, bias, group_pick, member_pick, probs, gate, up, down):
        width = tokens.shape[1]
        half = gate.shape[2] // 2
        rows = nz * CAP
        all_rows = nx * rows
        vmem, dma = pltpu.VMEM, pltpu.SemaphoreType.DMA
        whole = pl.BlockSpec(memory_space=pltpu.VMEM)
        away = pl.BlockSpec(memory_space=pl.ANY)
        return pl.pallas_call(
            functools.partial(kernel, nz, nx, ny, width * 2 * ny),
            out_shape=pltpu.VMEM(tokens.shape, BF16),
            in_specs=[away] * 9,
            out_specs=whole,
            scratch_shapes=[
                vmem(tokens.shape, BF16),
                vmem((1, L), F32),
                vmem((1, L), F32),
                vmem((1, tokens.shape[0]), jnp.int32),
                vmem(member_pick.shape[::-1], jnp.int32),
                vmem(probs.shape[::-1], F32),
                vmem((2, 2, 2 * L, half), BF16),
                vmem((2, half, 2 * L), BF16),
                vmem((2, 1, L), F32),
                vmem((2 * nx, nz, CAP, L), BF16),
                vmem((nx, rows, L), BF16),
                vmem((nz, nx * CAP, L), BF16),
                vmem((nz, 2 * nx, CAP, L), BF16),
                vmem((nz, nx * CAP, L), BF16),
                vmem((ny, 2, 2 * L), F32),
                vmem((ny, 2, 2 * L), F32),
                vmem((2, 2, L), F32),
                vmem((2, ny, 2, L), F32),
                vmem((ny - 1, 2, all_rows, L), BF16),
                vmem((ny - 1, 2, all_rows, L), BF16),
                vmem((ny, all_rows, L), BF16),
                vmem((2 * nx * nz, CAP, L), BF16),
                vmem((2 * nx * nz, CAP, L), BF16),
                pltpu.SemaphoreType.REGULAR((nz,)),
                pltpu.SemaphoreType.REGULAR,
                dma((6,)),
                dma((2,)),
                dma((6,)),
                dma((9,)),
                dma((7,)),
                dma((2,)),
                dma((2,)),
                dma((2, ny - 1)),
                dma((2, ny - 1)),
            ],
            compiler_params=pltpu.CompilerParams(collective_id=0, has_side_effects=True),
        )(tokens, gain.reshape(1, -1), bias.reshape(1, -1), group_pick.T, member_pick.T, probs.T, gate, up, down)

    return jax.shard_map(
        on_device,
        mesh=mesh,
        in_specs=(
            P("ep", "tp"),
            P("tp"),
            P("tp"),
            P("ep", None),
            P("ep", None),
            P("ep", None),
            P("ep", "tp", None),
            P("ep", "tp", None),
            P("ep", None, "tp"),
        ),
        out_specs=P("ep", "tp"),
        check_vma=False,
    )
```

```python
import functools

import jax
import jax.numpy as jnp
from jax import lax
from jax.experimental import pallas as pl
from jax.experimental.pallas import tpu as pltpu
from jax.sharding import PartitionSpec as P

EPG = 8
CAP = 2
EARLY = 2
norm_epsilon = 1e-05
MESH = pl.DeviceIdType.MESH
F32 = jnp.float32
BF16 = jnp.bfloat16
L = 128


def iota(shape, axis):
    return lax.broadcasted_iota(jnp.int32, shape, axis)


def far_first(n):
    return sorted(range(1, n), key=lambda d: -min(d, n - d))


def kernel(
    nz, nx, ny, features,
    tok_hbm, gain_hbm, bias_hbm, gp_hbm, mp_hbm, pp_hbm, gate_hbm, up_hbm, down_hbm,
    out_ref,
    tok_ref, gain_ref, bias_ref, gp_ref, mp_ref, pp_ref,
    wgu, wd, gb,
    xt, xs, zs, tr, sr, halfway, ax1s, ax1r, ax2s, ax2r, ps, pr, hb, os, rr,
    zready, yready, fsem, isem, lsem, wsem, ssem, rsem, tsem, asem, psem, hsem,
):
    tokens = tok_ref.shape[0]
    half = wgu.shape[3]
    rows = nz * CAP
    per_plane = nx * CAP
    all_rows = nz * per_plane
    per_expert = ny // 2
    ep, tp = lax.axis_index("ep"), lax.axis_index("tp")
    z, x, y, c = ep // nx, ep % nx, tp // 2, tp % 2

    def dev(dz=0, dx=0, dy=0, dc=0):
        return {
            "ep": lax.rem(z + dz + nz, nz) * nx + lax.rem(x + dx + nx, nx),
            "tp": lax.rem(y + dy + ny, ny) * 2 + lax.rem(c + dc, 2),
        }

    def remote(src, dst, ss, rs, device):
        return pltpu.make_async_remote_copy(
            src_ref=src, dst_ref=dst, send_sem=ss, recv_sem=rs, device_id=device, device_id_type=MESH
        )

    def each(n, body):
        lax.fori_loop(1, n, lambda d, carry: (body(d), carry)[1], 0)

    def done(ref, sem):
        pltpu.make_async_copy(ref, ref, sem).wait()

    def signal(sem, device):
        pl.semaphore_signal(sem, inc=1, device_id=device, device_id_type=MESH)

    inputs = [
        pltpu.make_async_copy(src, dst, isem.at[i])
        for i, (src, dst) in enumerate(
            (
                (gp_hbm, gp_ref),
                (mp_hbm, mp_ref),
                (pp_hbm, pp_ref),
                (tok_hbm, tok_ref),
                (gain_hbm, gain_ref),
                (bias_hbm, bias_ref),
            )
        )
    ]
    for copy in inputs:
        copy.start()

    def planes(low, high, body):
        lax.fori_loop(low, high, lambda to, carry: (body(to), carry)[1], 0)

    part = nz // 2
    side = z // part
    first = side * part

    def ranked(r):
        return r + r // per_expert * (3 * per_expert - 1 - 2 * r)

    rank = ranked(y)
    own_batch = (z + nz - EARLY) // nz
    barrier = pltpu.get_barrier_semaphore()

    def greet(to):
        signal(barrier, {"ep": to * nx + x, "tp": tp})

    planes(z + 1, first + part, greet)
    go_x = [lax.rem(x + d, nx) for d in range(nx)]
    go_tp = [tp, tp + 1 - 2 * c]

    def mate(k):
        return {"ep": z * nx + go_x[k // 2], "tp": go_tp[k % 2]}

    for k in range(1, 2 * nx):
        signal(barrier, mate(k))

    planes(rank + 1, ny, lambda r: signal(barrier, {"ep": ep, "tp": 2 * ranked(r) + c}))

    mine = pl.ds(pl.multiple_of(c * half, half), half)
    other = pl.ds(pl.multiple_of((1 - c) * half, half), half)
    pltpu.make_async_copy(gate_hbm.at[:, :, mine], wgu.at[0, :, 0:L, :], lsem.at[0]).start()
    pltpu.make_async_copy(up_hbm.at[:, :, mine], wgu.at[1, :, 0:L, :], lsem.at[0]).start()
    pltpu.make_async_copy(down_hbm.at[:, mine, :], wd.at[:, :, 0:L], lsem.at[1]).start()

    for copy in inputs:
        copy.wait()

    group = gp_ref[...]
    row = iota((rows, tokens), 0)
    lane = iota((rows, tokens), 1)
    member = (group == row // CAP).astype(F32)
    count = jnp.zeros((rows, tokens), F32)
    for t in range(tokens - 1):
        count = count + jnp.where(lane > t, member[:, t : t + 1], 0.0)
    rowwise = member * (count == (row % CAP).astype(F32)).astype(F32)
    def pack(source):
        packed = jnp.zeros((rows, L), F32)
        for t in range(tokens):
            packed = packed + rowwise[:, t : t + 1] * source[t : t + 1, :]
        return packed

    packed = pack(tok_ref[...].astype(F32))
    for d in range(nz):
        xt[0, d] = packed[d * CAP : (d + 1) * CAP, :].astype(BF16)

    pl.semaphore_wait(barrier, (2 * nx - 1) + z + rank)
    planes(0, z, lambda to: signal(zready.at[z], {"ep": to * nx + x, "tp": tp}))
    planes(0, rank, lambda r: signal(yready, {"ep": ep, "tp": 2 * ranked(r) + c}))

    @pl.when(side == 0)
    def _():
        planes(part, nz, greet)

    def x_copy(k):
        return remote(xt.at[0], xt.at[k], ssem.at[0], rsem.at[0], mate(k))

    def x_shares(dx):
        return remote(xs.at[0], xs.at[dx], ssem.at[1], rsem.at[1], mate(2 * dx))

    for k in range(1, 2 * nx):
        x_copy(k).start()


    def straight(to):
        for k in range(2 * nx):
            device = {"ep": to * nx + go_x[k // 2], "tp": go_tp[k % 2]}
            remote(xt.at[0, to], tr.at[z, k], ssem.at[2], tsem.at[own_batch], device).start()

    @pl.when(side == 1)
    def _():
        planes(0, part, straight)

    to = dev(dc=1)
    remote(gain_ref, gb.at[0], wsem.at[0], wsem.at[1], to).start()
    remote(bias_ref, gb.at[1], wsem.at[0], wsem.at[1], to).start()
    remote(gate_hbm.at[:, :, other], wgu.at[0, :, L : 2 * L, :], wsem.at[2], wsem.at[3], to).start()
    remote(up_hbm.at[:, :, other], wgu.at[1, :, L : 2 * L, :], wsem.at[2], wsem.at[3], to).start()
    remote(down_hbm.at[:, other, :], wd.at[:, :, L : 2 * L], wsem.at[4], wsem.at[5], to).start()

    probs = pp_ref[...]
    share = probs / jnp.sum(probs, axis=0, keepdims=True)
    top = probs.shape[0]
    table = [share[k : k + 1] for k in range(top)]
    table = table + [mp_ref[k : k + 1].astype(F32) for k in range(top)] + [rowwise]
    table = jnp.concatenate(table, axis=0)
    table = jnp.concatenate([table, jnp.zeros((2 * top + rows, L - tokens), F32)], axis=1)
    turned = jnp.transpose(table)[0:tokens, :]
    chosen = turned[:, 2 * top :]
    lane = iota((tokens, L), 1).astype(F32)
    shares = jnp.zeros((tokens, L), F32)
    for k in range(top):
        high = turned[:, k : k + 1].astype(BF16).astype(F32)
        low = turned[:, k : k + 1] - high
        pick = turned[:, top + k : top + k + 1]
        shares = shares + jnp.where(lane == pick, high, 0.0)
        shares = shares + jnp.where(lane == pick + EPG, low, 0.0)
    xs[0] = pack(shares).astype(BF16)
    for dx in range(1, nx):
        x_shares(dx).start()

    done(wgu.at[:, :, 0:L, :], lsem.at[0])
    done(gb, wsem.at[1])
    done(wgu.at[:, :, L : 2 * L, :], wsem.at[3])
    gain = jnp.concatenate([gain_ref[...], gb[0]], axis=1)
    bias = jnp.concatenate([bias_ref[...], gb[1]], axis=1)
    gain_high = gain.astype(BF16).astype(F32)
    bias_high = bias.astype(BF16).astype(F32)
    four = iota((16, 2 * L), 0)
    vectors = jnp.where(four == 0, gain_high, 0.0) + jnp.where(four == 1, gain - gain_high, 0.0)
    vectors = vectors + jnp.where(four == 2, bias_high, 0.0) + jnp.where(four == 3, bias - bias_high, 0.0)
    vectors = vectors.astype(BF16)
    for e in range(2):
        for g in range(2):
            line = jnp.dot(vectors, wgu[g, e], preferred_element_type=F32)
            for j in range(per_expert):
                piece = line[:, j * L : (j + 1) * L]
                ax1s[e * per_expert + j, 0:1, g * L : (g + 1) * L] = piece[0:1] + piece[1:2]
                ax1s[e * per_expert + j, 1:2, g * L : (g + 1) * L] = piece[2:3] + piece[3:4]
    ax1r[0] = ax1s[y]

    done(xt.at[pl.ds(1, 2 * nx - 1)], rsem.at[0])

    for k in range(2 * nx):
        tr[z, k] = xt[k, z]

    def z_copy(to):
        device = {"ep": to * nx + x, "tp": tp}
        remote(xt.at[:, to], tr.at[z], ssem.at[2], tsem.at[own_batch], device).start()

    def z_ready_copy(to):
        pl.semaphore_wait(zready.at[to], 1)
        z_copy(to)

    planes(first, z, z_copy)
    planes(z + 1, first + part, z_ready_copy)
    step = part // 2

    @pl.when(z < step)
    def _():
        device = {"ep": (z + step) * nx + x, "tp": tp}
        remote(xt.at[:, z + part], halfway, ssem.at[2], fsem.at[0], device).start()
        planes(part, z + part, z_ready_copy)
        planes(z + part + 1, nz, z_ready_copy)
        pl.semaphore_wait(zready.at[z + part], 1)

    @pl.when((z >= step) & (z < part))
    def _():
        pl.semaphore_wait(zready.at[z + step], 1)
        done(halfway, fsem.at[0])
        device = {"ep": (z + step) * nx + x, "tp": tp}
        remote(halfway, tr.at[z - step], fsem.at[1], tsem.at[0], device).start()
        z_copy(z + step)
        planes(part, z + step, z_ready_copy)
        planes(z + step + 1, nz, z_ready_copy)

    def z_shares(d):
        return remote(zs.at[lax.rem(z + d, nz)], sr.at[z], ssem.at[3], rsem.at[3], dev(dz=d))

    done(xs.at[pl.ds(1, nx - 1)], rsem.at[1])
    blocks = [xs[dx].astype(F32) for dx in range(nx)]
    for d in range(nz):
        block = [b[d * CAP : (d + 1) * CAP, :] for b in blocks]
        zs[d] = jnp.concatenate(block, axis=0).astype(BF16)
    sr[z] = zs[z]
    each(nz, lambda d: z_shares(d).start())

    @pl.when(rank < ny - 1)
    def _():
        pl.semaphore_wait(yready, ny - 1 - rank)

    def a1_copy(d):
        return remote(ax1s.at[(y + d) % ny], ax1r.at[d], ssem.at[4], rsem.at[4], dev(dy=d))

    each(ny, lambda d: a1_copy(d).start())

    cuts = [0, EARLY, nz]

    def rows_of(b):
        return pl.ds(cuts[b] * per_plane, (cuts[b + 1] - cuts[b]) * per_plane)

    def p_copy(b, d):
        here = rows_of(b)
        return remote(
            ps.at[d - 1, :, here], pr.at[d - 1, :, here], ssem.at[6], psem.at[b, d - 1], dev(dy=d)
        )

    def a2_copy(b, d):
        return remote(ax2s.at[b], ax2r.at[b, d], ssem.at[5], asem.at[b], dev(dy=d))

    gate_own, up_own = [], []
    for b in range(2):
        slots = range(cuts[b], cuts[b + 1])
        here = rows_of(b)
        batch_rows = here.size

        @pl.when(own_batch == b)
        def _():
            done(tr.at[pl.ds(1, len(slots) - 1)], tsem.at[b])

        @pl.when(own_batch != b)
        def _():
            done(tr.at[pl.ds(0, len(slots))], tsem.at[b])

        values = [
            jnp.concatenate([tr[i, 2 * dx + dc].astype(F32) for i in slots for dx in range(nx)], axis=0)
            for dc in range(2)
        ]
        values = jnp.concatenate(values, axis=1)
        middle = jnp.sum(values, axis=1, keepdims=True) * (1.0 / (2 * L))
        values = values - middle
        scaled = (values * gain).astype(BF16)
        waiting = []
        for place, d in enumerate(far_first(ny) + [0]):
            q = (y + d) % ny
            e = q // per_expert
            cols = pl.ds(pl.multiple_of((q % per_expert) * L, L), L)
            gate_part = jnp.dot(scaled, wgu[0, e, :, cols], preferred_element_type=F32)
            up_part = jnp.dot(scaled, wgu[1, e, :, cols], preferred_element_type=F32)
            if d == 0:
                gate_own.append(gate_part)
                up_own.append(up_part)
            else:
                ps[d - 1, 0, here] = gate_part.astype(BF16)
                ps[d - 1, 1, here] = up_part.astype(BF16)
                if place:
                    waiting.append(d)
                if place in (2, ny - 2):

                    @pl.when(ep >= 0)
                    def _():
                        for w in waiting:
                            p_copy(b, w).start()

                    waiting = []
            if place == 0:
                squares = jnp.sum(values * values, axis=1, keepdims=True)
                lanes = iota((batch_rows, L), 1)
                columns = jnp.where(lanes == 0, middle, 0.0) + jnp.where(lanes == 1, squares, 0.0)
                columns = jnp.transpose(columns)
                ax2s[b, :, 0:batch_rows] = columns[0:2, :]
                ax2r[b, 0, :, 0:batch_rows] = columns[0:2, :]

                @pl.when(ep >= 0)
                def _():
                    for w in far_first(ny):
                        a2_copy(b, w).start()
                    p_copy(b, far_first(ny)[0]).start()


    def h_copy(b, d):
        here = rows_of(b)
        return remote(hb.at[0, here], hb.at[d, here], ssem.at[7], hsem.at[b, d - 1], dev(dy=d))

    done(sr.at[pl.ds(1, nz - 1)], rsem.at[3])
    done(ax1r.at[pl.ds(1, ny - 1)], rsem.at[4])
    expert = 2 * x + y // per_expert
    gate_bias = up_bias = jnp.zeros((1, L), F32)
    for d in range(ny):
        gate_bias = gate_bias + ax1r[d, 1:2, 0:L]
        up_bias = up_bias + ax1r[d, 1:2, L : 2 * L]
    for b in range(2):
        here = rows_of(b)
        batch_rows = here.size
        lanes = iota((batch_rows, L), 1)
        share = jnp.concatenate([sr[i].astype(F32) for i in range(cuts[b], cuts[b + 1])], axis=0)
        share = jnp.sum(
            jnp.where((lanes == expert) | (lanes == expert + EPG), share, 0.0), axis=1, keepdims=True
        )
        done(ax2r.at[b, pl.ds(1, ny - 1)], asem.at[b])
        means = [ax2r[b, d, 0:1, 0:batch_rows] for d in range(ny)]
        center = sum(means) * (1.0 / ny)
        shifts = [m - center for m in means]
        spread = sum(ax2r[b, d, 1:2, 0:batch_rows] for d in range(ny))
        spread = spread + (features // ny) * sum(s * s for s in shifts)
        scale = lax.rsqrt(spread * (1.0 / features) + norm_epsilon)
        stack = iota((16, batch_rows), 0)
        table = jnp.where(stack == ny, scale, 0.0)
        for d in range(ny):
            table = table + jnp.where(stack == d, shifts[d], 0.0)
        table = jnp.transpose(table)
        scale = table[:, ny : ny + 1]
        gate, up = gate_own[b], up_own[b]
        for d in range(ny):
            shift = table[:, d : d + 1]
            gate = gate + shift * ax1r[d, 0:1, 0:L]
            up = up + shift * ax1r[d, 0:1, L : 2 * L]
        for d in far_first(ny):
            p_copy(b, d).wait_recv()
            gate = gate + pr[d - 1, 0, here].astype(F32)
            up = up + pr[d - 1, 1, here].astype(F32)
        gate = gate * scale + gate_bias
        up = up * scale + up_bias
        hb[0, here] = (share * (gate / (1.0 + jnp.exp(-gate)) * up)).astype(BF16)

        @pl.when(ep >= 0)
        def _():
            for d in far_first(ny):
                h_copy(b, d).start()


    def down(b, d):
        q = (y - d + ny) % ny
        units = pl.ds(pl.multiple_of((q % per_expert) * L, L), L)
        return jnp.dot(hb[d, rows_of(b)], wd[q // per_expert, units, :], preferred_element_type=F32)

    done(wd.at[:, :, 0:L], lsem.at[1])
    done(wd.at[:, :, L : 2 * L], wsem.at[5])

    back_x = [lax.rem(x - d + nx, nx) for d in range(nx)]
    back_tp = [tp, tp + 1 - 2 * c]
    order = sorted(range(2 * nx), key=lambda k: -min(k // 2, nx - k // 2))

    def send_back(h, k):
        to = {"ep": h * nx + back_x[k // 2], "tp": back_tp[k % 2]}
        remote(os.at[h * 2 * nx + k], rr.at[z * 2 * nx + k], ssem.at[8], rsem.at[6], to).start()

    for b in range(2):
        total = down(b, 0)
        for d in sorted(range(1, ny), key=lambda d: min(d, ny - d)):
            h_copy(b, d).wait_recv()
            total = total + down(b, d)
        slots = range(cuts[b], cuts[b + 1])
        for h in slots:
            for k in range(2 * nx):
                at = (h - cuts[b]) * per_plane + k // 2 * CAP
                piece = total[at : at + CAP, (k % 2) * L : (k % 2 + 1) * L]
                os[h * 2 * nx + k] = piece.astype(BF16)
        for h in slots:
            for k in order:
                if k:
                    send_back(h, k)
                else:
                    pl.when(z != h)(functools.partial(send_back, h, k))
    rr[z * 2 * nx] = os[z * 2 * nx]

    done(xt.at[pl.ds(1, 2 * nx - 1)], ssem.at[0])

    @pl.when((z >= step) & (z < part))
    def _():
        done(halfway, fsem.at[1])

    done(xs.at[pl.ds(1, nx - 1)], ssem.at[1])
    done(tr.at[pl.ds(1, nz - 1)], ssem.at[2])
    done(sr.at[pl.ds(1, nz - 1)], ssem.at[3])
    done(ax1r.at[pl.ds(1, ny - 1)], ssem.at[4])
    done(ax2r.at[:, pl.ds(1, ny - 1)], ssem.at[5])
    done(ps, ssem.at[6])
    done(hb.at[pl.ds(1, ny - 1)], ssem.at[7])
    done(gb, wsem.at[0])
    done(wgu.at[:, :, 0:L, :], wsem.at[2])
    done(wd.at[:, :, 0:L], wsem.at[4])
    done(rr.at[pl.ds(1, 2 * nx * nz - 1)], rsem.at[6])

    result = jnp.zeros((tokens, L), F32)
    for d in range(nz):
        back = rr[d * 2 * nx].astype(F32)
        for k in range(1, 2 * nx):
            back = back + rr[d * 2 * nx + k].astype(F32)
        for s in range(CAP):
            at = d * CAP + s
            result = result + chosen[:, at : at + 1] * back[s : s + 1, :]
    out_ref[...] = result.astype(BF16)
    done(os.at[pl.ds(1, 2 * nx * nz - 1)], ssem.at[8])


def solution(mesh):
    nx = EPG // 2
    nz = mesh.shape["ep"] // nx
    ny = mesh.shape["tp"] // 2

    def on_device(tokens, gain, bias, group_pick, member_pick, probs, gate, up, down):
        width = tokens.shape[1]
        half = gate.shape[2] // 2
        rows = nz * CAP
        all_rows = nx * rows
        vmem, dma = pltpu.VMEM, pltpu.SemaphoreType.DMA
        whole = pl.BlockSpec(memory_space=pltpu.VMEM)
        away = pl.BlockSpec(memory_space=pl.ANY)
        return pl.pallas_call(
            functools.partial(kernel, nz, nx, ny, width * 2 * ny),
            out_shape=pltpu.VMEM(tokens.shape, BF16),
            in_specs=[away] * 9,
            out_specs=whole,
            scratch_shapes=[
                vmem(tokens.shape, BF16),
                vmem((1, L), F32),
                vmem((1, L), F32),
                vmem((1, tokens.shape[0]), jnp.int32),
                vmem(member_pick.shape[::-1], jnp.int32),
                vmem(probs.shape[::-1], F32),
                vmem((2, 2, 2 * L, half), BF16),
                vmem((2, half, 2 * L), BF16),
                vmem((2, 1, L), F32),
                vmem((2 * nx, nz, CAP, L), BF16),
                vmem((nx, rows, L), BF16),
                vmem((nz, nx * CAP, L), BF16),
                vmem((nz, 2 * nx, CAP, L), BF16),
                vmem((nz, nx * CAP, L), BF16),
                vmem((2 * nx, CAP, L), BF16),
                vmem((ny, 2, 2 * L), F32),
                vmem((ny, 2, 2 * L), F32),
                vmem((2, 2, L), F32),
                vmem((2, ny, 2, L), F32),
                vmem((ny - 1, 2, all_rows, L), BF16),
                vmem((ny - 1, 2, all_rows, L), BF16),
                vmem((ny, all_rows, L), BF16),
                vmem((2 * nx * nz, CAP, L), BF16),
                vmem((2 * nx * nz, CAP, L), BF16),
                pltpu.SemaphoreType.REGULAR((nz,)),
                pltpu.SemaphoreType.REGULAR,
                dma((2,)),
                dma((6,)),
                dma((2,)),
                dma((6,)),
                dma((9,)),
                dma((7,)),
                dma((2,)),
                dma((2,)),
                dma((2, ny - 1)),
                dma((2, ny - 1)),
            ],
            compiler_params=pltpu.CompilerParams(collective_id=0, has_side_effects=True),
        )(tokens, gain.reshape(1, -1), bias.reshape(1, -1), group_pick.T, member_pick.T, probs.T, gate, up, down)

    return jax.shard_map(
        on_device,
        mesh=mesh,
        in_specs=(
            P("ep", "tp"),
            P("tp"),
            P("tp"),
            P("ep", None),
            P("ep", None),
            P("ep", None),
            P("ep", "tp", None),
            P("ep", "tp", None),
            P("ep", None, "tp"),
        ),
        out_specs=P("ep", "tp"),
        check_vma=False,
    )
```

```python
import functools

import jax
import jax.numpy as jnp
from jax import lax
from jax.experimental import pallas as pl
from jax.experimental.pallas import tpu as pltpu
from jax.sharding import PartitionSpec as P

EPG = 8
CAP = 2
EARLY = 2
norm_epsilon = 1e-05
MESH = pl.DeviceIdType.MESH
F32 = jnp.float32
BF16 = jnp.bfloat16
L = 128


def iota(shape, axis):
    return lax.broadcasted_iota(jnp.int32, shape, axis)


def far_first(n):
    return sorted(range(1, n), key=lambda d: -min(d, n - d))


def kernel(
    nz, nx, ny, features,
    tok_hbm, gain_hbm, bias_hbm, gp_hbm, mp_hbm, pp_hbm, gate_hbm, up_hbm, down_hbm,
    out_ref,
    tok_ref, gain_ref, bias_ref, gp_ref, mp_ref, pp_ref,
    wgu, wd, gb,
    xt, xs, zs, tr, sr, halfway, ax1s, ax1r, ax2s, ax2r, ps, pr, hb, os, rr,
    zready, yready, fsem, isem, lsem, wsem, ssem, rsem, tsem, asem, psem, hsem,
):
    tokens = tok_ref.shape[0]
    half = wgu.shape[3]
    rows = nz * CAP
    per_plane = nx * CAP
    all_rows = nz * per_plane
    per_expert = ny // 2
    ep, tp = lax.axis_index("ep"), lax.axis_index("tp")
    z, x, y, c = ep // nx, ep % nx, tp // 2, tp % 2

    def dev(dz=0, dx=0, dy=0, dc=0):
        return {
            "ep": lax.rem(z + dz + nz, nz) * nx + lax.rem(x + dx + nx, nx),
            "tp": lax.rem(y + dy + ny, ny) * 2 + lax.rem(c + dc, 2),
        }

    def remote(src, dst, ss, rs, device):
        return pltpu.make_async_remote_copy(
            src_ref=src, dst_ref=dst, send_sem=ss, recv_sem=rs, device_id=device, device_id_type=MESH
        )

    def each(n, body):
        lax.fori_loop(1, n, lambda d, carry: (body(d), carry)[1], 0)

    def done(ref, sem):
        pltpu.make_async_copy(ref, ref, sem).wait()

    def signal(sem, device):
        pl.semaphore_signal(sem, inc=1, device_id=device, device_id_type=MESH)

    inputs = [
        pltpu.make_async_copy(src, dst, isem.at[i])
        for i, (src, dst) in enumerate(
            (
                (gp_hbm, gp_ref),
                (mp_hbm, mp_ref),
                (pp_hbm, pp_ref),
                (tok_hbm, tok_ref),
                (gain_hbm, gain_ref),
                (bias_hbm, bias_ref),
            )
        )
    ]
    for copy in inputs:
        copy.start()

    def planes(low, high, body):
        lax.fori_loop(low, high, lambda to, carry: (body(to), carry)[1], 0)

    part = nz // 2
    side = z // part
    first = side * part

    def ranked(r):
        return r + r // per_expert * (3 * per_expert - 1 - 2 * r)

    rank = ranked(y)
    own_batch = (z + nz - EARLY) // nz
    barrier = pltpu.get_barrier_semaphore()

    def greet(to):
        signal(barrier, {"ep": to * nx + x, "tp": tp})

    planes(z + 1, first + part, greet)
    go_x = [lax.rem(x + d, nx) for d in range(nx)]
    go_tp = [tp, tp + 1 - 2 * c]

    def mate(k):
        return {"ep": z * nx + go_x[k // 2], "tp": go_tp[k % 2]}

    for k in range(1, 2 * nx):
        signal(barrier, mate(k))

    planes(rank + 1, ny, lambda r: signal(barrier, {"ep": ep, "tp": 2 * ranked(r) + c}))

    mine = pl.ds(pl.multiple_of(c * half, half), half)
    other = pl.ds(pl.multiple_of((1 - c) * half, half), half)
    pltpu.make_async_copy(gate_hbm.at[:, :, mine], wgu.at[0, :, 0:L, :], lsem.at[0]).start()
    pltpu.make_async_copy(up_hbm.at[:, :, mine], wgu.at[1, :, 0:L, :], lsem.at[0]).start()
    pltpu.make_async_copy(down_hbm.at[:, mine, :], wd.at[:, :, 0:L], lsem.at[1]).start()

    for copy in inputs:
        copy.wait()

    group = gp_ref[...]
    row = iota((rows, tokens), 0)
    lane = iota((rows, tokens), 1)
    member = (group == row // CAP).astype(F32)
    count = jnp.zeros((rows, tokens), F32)
    for t in range(tokens - 1):
        count = count + jnp.where(lane > t, member[:, t : t + 1], 0.0)
    rowwise = member * (count == (row % CAP).astype(F32)).astype(F32)
    def pack(source):
        packed = jnp.zeros((rows, L), F32)
        for t in range(tokens):
            packed = packed + rowwise[:, t : t + 1] * source[t : t + 1, :]
        return packed

    packed = pack(tok_ref[...].astype(F32))
    for d in range(nz):
        xt[0, d] = packed[d * CAP : (d + 1) * CAP, :].astype(BF16)

    pl.semaphore_wait(barrier, (2 * nx - 1) + z + rank)
    planes(0, z, lambda to: signal(zready.at[z], {"ep": to * nx + x, "tp": tp}))

    @pl.when(side == 0)
    def _():
        planes(part, nz, greet)

    def x_copy(k):
        return remote(xt.at[0], xt.at[k], ssem.at[0], rsem.at[0], mate(k))

    def x_shares(dx):
        return remote(xs.at[0], xs.at[dx], ssem.at[1], rsem.at[1], mate(2 * dx))

    for k in range(1, 2 * nx):
        x_copy(k).start()
    planes(0, rank, lambda r: signal(yready, {"ep": ep, "tp": 2 * ranked(r) + c}))


    def straight(to):
        for k in range(2 * nx):
            device = {"ep": to * nx + go_x[k // 2], "tp": go_tp[k % 2]}
            remote(xt.at[0, to], tr.at[z, k], ssem.at[2], tsem.at[own_batch], device).start()

    @pl.when(side == 1)
    def _():
        planes(0, part, straight)

    to = dev(dc=1)
    remote(gain_ref, gb.at[0], wsem.at[0], wsem.at[1], to).start()
    remote(bias_ref, gb.at[1], wsem.at[0], wsem.at[1], to).start()
    remote(gate_hbm.at[:, :, other], wgu.at[0, :, L : 2 * L, :], wsem.at[2], wsem.at[3], to).start()
    remote(up_hbm.at[:, :, other], wgu.at[1, :, L : 2 * L, :], wsem.at[2], wsem.at[3], to).start()
    remote(down_hbm.at[:, other, :], wd.at[:, :, L : 2 * L], wsem.at[4], wsem.at[5], to).start()

    probs = pp_ref[...]
    share = probs / jnp.sum(probs, axis=0, keepdims=True)
    top = probs.shape[0]
    table = [share[k : k + 1] for k in range(top)]
    table = table + [mp_ref[k : k + 1].astype(F32) for k in range(top)] + [rowwise]
    table = jnp.concatenate(table, axis=0)
    table = jnp.concatenate([table, jnp.zeros((2 * top + rows, L - tokens), F32)], axis=1)
    turned = jnp.transpose(table)[0:tokens, :]
    chosen = turned[:, 2 * top :]
    lane = iota((tokens, L), 1).astype(F32)
    shares = jnp.zeros((tokens, L), F32)
    for k in range(top):
        high = turned[:, k : k + 1].astype(BF16).astype(F32)
        low = turned[:, k : k + 1] - high
        pick = turned[:, top + k : top + k + 1]
        shares = shares + jnp.where(lane == pick, high, 0.0)
        shares = shares + jnp.where(lane == pick + EPG, low, 0.0)
    xs[0] = pack(shares).astype(BF16)
    for dx in range(1, nx):
        x_shares(dx).start()

    done(wgu.at[:, :, 0:L, :], lsem.at[0])
    done(gb, wsem.at[1])
    done(wgu.at[:, :, L : 2 * L, :], wsem.at[3])
    gain = jnp.concatenate([gain_ref[...], gb[0]], axis=1)
    bias = jnp.concatenate([bias_ref[...], gb[1]], axis=1)
    gain_high = gain.astype(BF16).astype(F32)
    bias_high = bias.astype(BF16).astype(F32)
    four = iota((16, 2 * L), 0)
    vectors = jnp.where(four == 0, gain_high, 0.0) + jnp.where(four == 1, gain - gain_high, 0.0)
    vectors = vectors + jnp.where(four == 2, bias_high, 0.0) + jnp.where(four == 3, bias - bias_high, 0.0)
    vectors = vectors.astype(BF16)
    for e in range(2):
        for g in range(2):
            line = jnp.dot(vectors, wgu[g, e], preferred_element_type=F32)
            for j in range(per_expert):
                piece = line[:, j * L : (j + 1) * L]
                ax1s[e * per_expert + j, 0:1, g * L : (g + 1) * L] = piece[0:1] + piece[1:2]
                ax1s[e * per_expert + j, 1:2, g * L : (g + 1) * L] = piece[2:3] + piece[3:4]
    ax1r[0] = ax1s[y]

    done(xt.at[pl.ds(1, 2 * nx - 1)], rsem.at[0])

    for k in range(2 * nx):
        tr[z, k] = xt[k, z]

    def z_copy(to):
        device = {"ep": to * nx + x, "tp": tp}
        remote(xt.at[:, to], tr.at[z], ssem.at[2], tsem.at[own_batch], device).start()

    def z_ready_copy(to):
        pl.semaphore_wait(zready.at[to], 1)
        z_copy(to)

    planes(first, z, z_copy)
    planes(z + 1, first + part, z_ready_copy)
    step = part // 2

    @pl.when(z < step)
    def _():
        device = {"ep": (z + step) * nx + x, "tp": tp}
        remote(xt.at[:, z + part], halfway, ssem.at[2], fsem.at[0], device).start()
        planes(part, z + part, z_ready_copy)
        planes(z + part + 1, nz, z_ready_copy)
        pl.semaphore_wait(zready.at[z + part], 1)

    @pl.when((z >= step) & (z < part))
    def _():
        pl.semaphore_wait(zready.at[z + step], 1)
        done(halfway, fsem.at[0])
        device = {"ep": (z + step) * nx + x, "tp": tp}
        remote(halfway, tr.at[z - step], fsem.at[1], tsem.at[0], device).start()
        z_copy(z + step)
        planes(part, z + step, z_ready_copy)
        planes(z + step + 1, nz, z_ready_copy)

    def z_shares(d):
        return remote(zs.at[lax.rem(z + d, nz)], sr.at[z], ssem.at[3], rsem.at[3], dev(dz=d))

    done(xs.at[pl.ds(1, nx - 1)], rsem.at[1])
    blocks = [xs[dx].astype(F32) for dx in range(nx)]
    for d in range(nz):
        block = [b[d * CAP : (d + 1) * CAP, :] for b in blocks]
        zs[d] = jnp.concatenate(block, axis=0).astype(BF16)
    sr[z] = zs[z]
    each(nz, lambda d: z_shares(d).start())

    @pl.when(rank < ny - 1)
    def _():
        pl.semaphore_wait(yready, ny - 1 - rank)

    def a1_copy(d):
        return remote(ax1s.at[(y + d) % ny], ax1r.at[d], ssem.at[4], rsem.at[4], dev(dy=d))

    each(ny, lambda d: a1_copy(d).start())

    cuts = [0, EARLY, nz]

    def rows_of(b):
        return pl.ds(cuts[b] * per_plane, (cuts[b + 1] - cuts[b]) * per_plane)

    def p_copy(b, d):
        here = rows_of(b)
        return remote(
            ps.at[d - 1, :, here], pr.at[d - 1, :, here], ssem.at[6], psem.at[b, d - 1], dev(dy=d)
        )

    def a2_copy(b, d):
        return remote(ax2s.at[b], ax2r.at[b, d], ssem.at[5], asem.at[b], dev(dy=d))

    gate_own, up_own = [], []
    for b in range(2):
        slots = range(cuts[b], cuts[b + 1])
        here = rows_of(b)
        batch_rows = here.size

        @pl.when(own_batch == b)
        def _():
            done(tr.at[pl.ds(1, len(slots) - 1)], tsem.at[b])

        @pl.when(own_batch != b)
        def _():
            done(tr.at[pl.ds(0, len(slots))], tsem.at[b])

        values = [
            jnp.concatenate([tr[i, 2 * dx + dc].astype(F32) for i in slots for dx in range(nx)], axis=0)
            for dc in range(2)
        ]
        values = jnp.concatenate(values, axis=1)
        middle = jnp.sum(values, axis=1, keepdims=True) * (1.0 / (2 * L))
        values = values - middle
        scaled = (values * gain).astype(BF16)
        waiting = []
        for place, d in enumerate(far_first(ny) + [0]):
            q = (y + d) % ny
            e = q // per_expert
            cols = pl.ds(pl.multiple_of((q % per_expert) * L, L), L)
            gate_part = jnp.dot(scaled, wgu[0, e, :, cols], preferred_element_type=F32)
            up_part = jnp.dot(scaled, wgu[1, e, :, cols], preferred_element_type=F32)
            if d == 0:
                gate_own.append(gate_part)
                up_own.append(up_part)
            else:
                ps[d - 1, 0, here] = gate_part.astype(BF16)
                ps[d - 1, 1, here] = up_part.astype(BF16)
                if place:
                    waiting.append(d)
                if place in (2, ny - 2):

                    @pl.when(ep >= 0)
                    def _():
                        for w in waiting:
                            p_copy(b, w).start()

                    waiting = []
            if place == 0:
                squares = jnp.sum(values * values, axis=1, keepdims=True)
                lanes = iota((batch_rows, L), 1)
                columns = jnp.where(lanes == 0, middle, 0.0) + jnp.where(lanes == 1, squares, 0.0)
                columns = jnp.transpose(columns)
                ax2s[b, :, 0:batch_rows] = columns[0:2, :]
                ax2r[b, 0, :, 0:batch_rows] = columns[0:2, :]

                @pl.when(ep >= 0)
                def _():
                    for w in far_first(ny):
                        a2_copy(b, w).start()
                    p_copy(b, far_first(ny)[0]).start()


    def h_copy(b, d):
        here = rows_of(b)
        return remote(hb.at[0, here], hb.at[d, here], ssem.at[7], hsem.at[b, d - 1], dev(dy=d))

    done(sr.at[pl.ds(1, nz - 1)], rsem.at[3])
    done(ax1r.at[pl.ds(1, ny - 1)], rsem.at[4])
    expert = 2 * x + y // per_expert
    gate_bias = up_bias = jnp.zeros((1, L), F32)
    for d in range(ny):
        gate_bias = gate_bias + ax1r[d, 1:2, 0:L]
        up_bias = up_bias + ax1r[d, 1:2, L : 2 * L]
    for b in range(2):
        here = rows_of(b)
        batch_rows = here.size
        lanes = iota((batch_rows, L), 1)
        share = jnp.concatenate([sr[i].astype(F32) for i in range(cuts[b], cuts[b + 1])], axis=0)
        share = jnp.sum(
            jnp.where((lanes == expert) | (lanes == expert + EPG), share, 0.0), axis=1, keepdims=True
        )
        done(ax2r.at[b, pl.ds(1, ny - 1)], asem.at[b])
        means = [ax2r[b, d, 0:1, 0:batch_rows] for d in range(ny)]
        center = sum(means) * (1.0 / ny)
        shifts = [m - center for m in means]
        spread = sum(ax2r[b, d, 1:2, 0:batch_rows] for d in range(ny))
        spread = spread + (features // ny) * sum(s * s for s in shifts)
        scale = lax.rsqrt(spread * (1.0 / features) + norm_epsilon)
        stack = iota((16, batch_rows), 0)
        table = jnp.where(stack == ny, scale, 0.0)
        for d in range(ny):
            table = table + jnp.where(stack == d, shifts[d], 0.0)
        table = jnp.transpose(table)
        scale = table[:, ny : ny + 1]
        gate, up = gate_own[b], up_own[b]
        for d in range(ny):
            shift = table[:, d : d + 1]
            gate = gate + shift * ax1r[d, 0:1, 0:L]
            up = up + shift * ax1r[d, 0:1, L : 2 * L]
        for d in far_first(ny):
            p_copy(b, d).wait_recv()
            gate = gate + pr[d - 1, 0, here].astype(F32)
            up = up + pr[d - 1, 1, here].astype(F32)
        gate = gate * scale + gate_bias
        up = up * scale + up_bias
        hb[0, here] = (share * (gate / (1.0 + jnp.exp(-gate)) * up)).astype(BF16)

        @pl.when(ep >= 0)
        def _():
            for d in far_first(ny):
                h_copy(b, d).start()


    def down(b, d):
        q = (y - d + ny) % ny
        units = pl.ds(pl.multiple_of((q % per_expert) * L, L), L)
        return jnp.dot(hb[d, rows_of(b)], wd[q // per_expert, units, :], preferred_element_type=F32)

    done(wd.at[:, :, 0:L], lsem.at[1])
    done(wd.at[:, :, L : 2 * L], wsem.at[5])

    back_x = [lax.rem(x - d + nx, nx) for d in range(nx)]
    back_tp = [tp, tp + 1 - 2 * c]
    order = sorted(range(2 * nx), key=lambda k: -min(k // 2, nx - k // 2))

    def send_back(h, k):
        to = {"ep": h * nx + back_x[k // 2], "tp": back_tp[k % 2]}
        remote(os.at[h * 2 * nx + k], rr.at[z * 2 * nx + k], ssem.at[8], rsem.at[6], to).start()

    for b in range(2):
        total = down(b, 0)
        for d in sorted(range(1, ny), key=lambda d: min(d, ny - d)):
            h_copy(b, d).wait_recv()
            total = total + down(b, d)
        slots = range(cuts[b], cuts[b + 1])
        for h in slots:
            for k in range(2 * nx):
                at = (h - cuts[b]) * per_plane + k // 2 * CAP
                piece = total[at : at + CAP, (k % 2) * L : (k % 2 + 1) * L]
                os[h * 2 * nx + k] = piece.astype(BF16)
        for h in slots:
            for k in order:
                if k:
                    send_back(h, k)
                else:
                    pl.when(z != h)(functools.partial(send_back, h, k))
    rr[z * 2 * nx] = os[z * 2 * nx]

    done(xt.at[pl.ds(1, 2 * nx - 1)], ssem.at[0])

    @pl.when((z >= step) & (z < part))
    def _():
        done(halfway, fsem.at[1])

    done(xs.at[pl.ds(1, nx - 1)], ssem.at[1])
    done(tr.at[pl.ds(1, nz - 1)], ssem.at[2])
    done(sr.at[pl.ds(1, nz - 1)], ssem.at[3])
    done(ax1r.at[pl.ds(1, ny - 1)], ssem.at[4])
    done(ax2r.at[:, pl.ds(1, ny - 1)], ssem.at[5])
    done(ps, ssem.at[6])
    done(hb.at[pl.ds(1, ny - 1)], ssem.at[7])
    done(gb, wsem.at[0])
    done(wgu.at[:, :, 0:L, :], wsem.at[2])
    done(wd.at[:, :, 0:L], wsem.at[4])
    done(rr.at[pl.ds(1, 2 * nx * nz - 1)], rsem.at[6])

    result = jnp.zeros((tokens, L), F32)
    for d in range(nz):
        back = rr[d * 2 * nx].astype(F32)
        for k in range(1, 2 * nx):
            back = back + rr[d * 2 * nx + k].astype(F32)
        for s in range(CAP):
            at = d * CAP + s
            result = result + chosen[:, at : at + 1] * back[s : s + 1, :]
    out_ref[...] = result.astype(BF16)
    done(os.at[pl.ds(1, 2 * nx * nz - 1)], ssem.at[8])


def solution(mesh):
    nx = EPG // 2
    nz = mesh.shape["ep"] // nx
    ny = mesh.shape["tp"] // 2

    def on_device(tokens, gain, bias, group_pick, member_pick, probs, gate, up, down):
        width = tokens.shape[1]
        half = gate.shape[2] // 2
        rows = nz * CAP
        all_rows = nx * rows
        vmem, dma = pltpu.VMEM, pltpu.SemaphoreType.DMA
        whole = pl.BlockSpec(memory_space=pltpu.VMEM)
        away = pl.BlockSpec(memory_space=pl.ANY)
        return pl.pallas_call(
            functools.partial(kernel, nz, nx, ny, width * 2 * ny),
            out_shape=pltpu.VMEM(tokens.shape, BF16),
            in_specs=[away] * 9,
            out_specs=whole,
            scratch_shapes=[
                vmem(tokens.shape, BF16),
                vmem((1, L), F32),
                vmem((1, L), F32),
                vmem((1, tokens.shape[0]), jnp.int32),
                vmem(member_pick.shape[::-1], jnp.int32),
                vmem(probs.shape[::-1], F32),
                vmem((2, 2, 2 * L, half), BF16),
                vmem((2, half, 2 * L), BF16),
                vmem((2, 1, L), F32),
                vmem((2 * nx, nz, CAP, L), BF16),
                vmem((nx, rows, L), BF16),
                vmem((nz, nx * CAP, L), BF16),
                vmem((nz, 2 * nx, CAP, L), BF16),
                vmem((nz, nx * CAP, L), BF16),
                vmem((2 * nx, CAP, L), BF16),
                vmem((ny, 2, 2 * L), F32),
                vmem((ny, 2, 2 * L), F32),
                vmem((2, 2, L), F32),
                vmem((2, ny, 2, L), F32),
                vmem((ny - 1, 2, all_rows, L), BF16),
                vmem((ny - 1, 2, all_rows, L), BF16),
                vmem((ny, all_rows, L), BF16),
                vmem((2 * nx * nz, CAP, L), BF16),
                vmem((2 * nx * nz, CAP, L), BF16),
                pltpu.SemaphoreType.REGULAR((nz,)),
                pltpu.SemaphoreType.REGULAR,
                dma((2,)),
                dma((6,)),
                dma((2,)),
                dma((6,)),
                dma((9,)),
                dma((7,)),
                dma((2,)),
                dma((2,)),
                dma((2, ny - 1)),
                dma((2, ny - 1)),
            ],
            compiler_params=pltpu.CompilerParams(collective_id=0, has_side_effects=True),
        )(tokens, gain.reshape(1, -1), bias.reshape(1, -1), group_pick.T, member_pick.T, probs.T, gate, up, down)

    return jax.shard_map(
        on_device,
        mesh=mesh,
        in_specs=(
            P("ep", "tp"),
            P("tp"),
            P("tp"),
            P("ep", None),
            P("ep", None),
            P("ep", None),
            P("ep", "tp", None),
            P("ep", "tp", None),
            P("ep", None, "tp"),
        ),
        out_specs=P("ep", "tp"),
        check_vma=False,
    )
```

```python
import functools

import jax
import jax.numpy as jnp
from jax import lax
from jax.experimental import pallas as pl
from jax.experimental.pallas import tpu as pltpu
from jax.sharding import PartitionSpec as P

EPG = 8
CAP = 2
EARLY = 2
norm_epsilon = 1e-05
MESH = pl.DeviceIdType.MESH
F32 = jnp.float32
BF16 = jnp.bfloat16
L = 128


def iota(shape, axis):
    return lax.broadcasted_iota(jnp.int32, shape, axis)


def far_first(n):
    return sorted(range(1, n), key=lambda d: -min(d, n - d))


def kernel(
    nz, nx, ny, features,
    tok_hbm, gain_hbm, bias_hbm, gp_hbm, mp_hbm, pp_hbm, gate_hbm, up_hbm, down_hbm,
    out_ref,
    tok_ref, gain_ref, bias_ref, gp_ref, mp_ref, pp_ref,
    wgu, wd, gb,
    xt, xs, zs, tr, sr, halfway, ax1s, ax1r, ax2s, ax2r, ps, pr, hb, os, rr,
    zready, yready, fsem, isem, lsem, wsem, ssem, rsem, tsem, asem, psem, hsem,
):
    tokens = tok_ref.shape[0]
    half = wgu.shape[3]
    rows = nz * CAP
    per_plane = nx * CAP
    all_rows = nz * per_plane
    per_expert = ny // 2
    ep, tp = lax.axis_index("ep"), lax.axis_index("tp")
    z, x, y, c = ep // nx, ep % nx, tp // 2, tp % 2

    def dev(dz=0, dx=0, dy=0, dc=0):
        return {
            "ep": lax.rem(z + dz + nz, nz) * nx + lax.rem(x + dx + nx, nx),
            "tp": lax.rem(y + dy + ny, ny) * 2 + lax.rem(c + dc, 2),
        }

    def remote(src, dst, ss, rs, device):
        return pltpu.make_async_remote_copy(
            src_ref=src, dst_ref=dst, send_sem=ss, recv_sem=rs, device_id=device, device_id_type=MESH
        )

    def each(n, body):
        lax.fori_loop(1, n, lambda d, carry: (body(d), carry)[1], 0)

    def done(ref, sem):
        pltpu.make_async_copy(ref, ref, sem).wait()

    def signal(sem, device):
        pl.semaphore_signal(sem, inc=1, device_id=device, device_id_type=MESH)

    def planes(low, high, body):
        lax.fori_loop(low, high, lambda to, carry: (body(to), carry)[1], 0)

    part = nz // 2
    side = z // part
    first = side * part

    def ranked(r):
        return r + r // per_expert * (3 * per_expert - 1 - 2 * r)

    rank = ranked(y)
    own_batch = (z + nz - EARLY) // nz
    barrier = pltpu.get_barrier_semaphore()

    def greet(to):
        signal(barrier, {"ep": to * nx + x, "tp": tp})

    go_x = [lax.rem(x + d, nx) for d in range(nx)]
    go_tp = [tp, tp + 1 - 2 * c]

    def mate(k):
        return {"ep": z * nx + go_x[k // 2], "tp": go_tp[k % 2]}

    for k in range(1, 2 * nx):
        signal(barrier, mate(k))

    planes(z + 1, first + part, greet)
    inputs = [
        pltpu.make_async_copy(src, dst, isem.at[i])
        for i, (src, dst) in enumerate(
            (
                (gp_hbm, gp_ref),
                (mp_hbm, mp_ref),
                (pp_hbm, pp_ref),
                (tok_hbm, tok_ref),
                (gain_hbm, gain_ref),
                (bias_hbm, bias_ref),
            )
        )
    ]
    for copy in inputs:
        copy.start()

    planes(rank + 1, ny, lambda r: signal(barrier, {"ep": ep, "tp": 2 * ranked(r) + c}))

    mine = pl.ds(pl.multiple_of(c * half, half), half)
    other = pl.ds(pl.multiple_of((1 - c) * half, half), half)
    pltpu.make_async_copy(gate_hbm.at[:, :, mine], wgu.at[0, :, 0:L, :], lsem.at[0]).start()
    pltpu.make_async_copy(up_hbm.at[:, :, mine], wgu.at[1, :, 0:L, :], lsem.at[0]).start()
    pltpu.make_async_copy(down_hbm.at[:, mine, :], wd.at[:, :, 0:L], lsem.at[1]).start()

    for copy in inputs:
        copy.wait()

    group = gp_ref[...]
    row = iota((rows, tokens), 0)
    lane = iota((rows, tokens), 1)
    member = (group == row // CAP).astype(F32)
    count = jnp.zeros((rows, tokens), F32)
    for t in range(tokens - 1):
        count = count + jnp.where(lane > t, member[:, t : t + 1], 0.0)
    rowwise = member * (count == (row % CAP).astype(F32)).astype(F32)
    def pack(source):
        packed = jnp.zeros((rows, L), F32)
        for t in range(tokens):
            packed = packed + rowwise[:, t : t + 1] * source[t : t + 1, :]
        return packed

    packed = pack(tok_ref[...].astype(F32))
    for d in range(nz):
        xt[0, d] = packed[d * CAP : (d + 1) * CAP, :].astype(BF16)

    pl.semaphore_wait(barrier, (2 * nx - 1) + z + rank)
    planes(0, z, lambda to: signal(zready.at[z], {"ep": to * nx + x, "tp": tp}))

    @pl.when(side == 0)
    def _():
        planes(part, nz, greet)

    def x_copy(k):
        return remote(xt.at[0], xt.at[k], ssem.at[0], rsem.at[0], mate(k))

    def x_shares(dx):
        return remote(xs.at[0], xs.at[dx], ssem.at[1], rsem.at[1], mate(2 * dx))

    for k in range(1, 2 * nx):
        x_copy(k).start()
    planes(0, rank, lambda r: signal(yready, {"ep": ep, "tp": 2 * ranked(r) + c}))


    def straight(to):
        for k in range(2 * nx):
            device = {"ep": to * nx + go_x[k // 2], "tp": go_tp[k % 2]}
            remote(xt.at[0, to], tr.at[z, k], ssem.at[2], tsem.at[own_batch], device).start()

    @pl.when(side == 1)
    def _():
        planes(0, part, straight)

    to = dev(dc=1)
    remote(gain_ref, gb.at[0], wsem.at[0], wsem.at[1], to).start()
    remote(bias_ref, gb.at[1], wsem.at[0], wsem.at[1], to).start()
    remote(gate_hbm.at[:, :, other], wgu.at[0, :, L : 2 * L, :], wsem.at[2], wsem.at[3], to).start()
    remote(up_hbm.at[:, :, other], wgu.at[1, :, L : 2 * L, :], wsem.at[2], wsem.at[3], to).start()
    remote(down_hbm.at[:, other, :], wd.at[:, :, L : 2 * L], wsem.at[4], wsem.at[5], to).start()

    probs = pp_ref[...]
    share = probs / jnp.sum(probs, axis=0, keepdims=True)
    top = probs.shape[0]
    table = [share[k : k + 1] for k in range(top)]
    table = table + [mp_ref[k : k + 1].astype(F32) for k in range(top)] + [rowwise]
    table = jnp.concatenate(table, axis=0)
    table = jnp.concatenate([table, jnp.zeros((2 * top + rows, L - tokens), F32)], axis=1)
    turned = jnp.transpose(table)[0:tokens, :]
    chosen = turned[:, 2 * top :]
    lane = iota((tokens, L), 1).astype(F32)
    shares = jnp.zeros((tokens, L), F32)
    for k in range(top):
        high = turned[:, k : k + 1].astype(BF16).astype(F32)
        low = turned[:, k : k + 1] - high
        pick = turned[:, top + k : top + k + 1]
        shares = shares + jnp.where(lane == pick, high, 0.0)
        shares = shares + jnp.where(lane == pick + EPG, low, 0.0)
    xs[0] = pack(shares).astype(BF16)
    for dx in range(1, nx):
        x_shares(dx).start()

    done(wgu.at[:, :, 0:L, :], lsem.at[0])
    done(gb, wsem.at[1])
    done(wgu.at[:, :, L : 2 * L, :], wsem.at[3])
    gain = jnp.concatenate([gain_ref[...], gb[0]], axis=1)
    bias = jnp.concatenate([bias_ref[...], gb[1]], axis=1)
    gain_high = gain.astype(BF16).astype(F32)
    bias_high = bias.astype(BF16).astype(F32)
    four = iota((16, 2 * L), 0)
    vectors = jnp.where(four == 0, gain_high, 0.0) + jnp.where(four == 1, gain - gain_high, 0.0)
    vectors = vectors + jnp.where(four == 2, bias_high, 0.0) + jnp.where(four == 3, bias - bias_high, 0.0)
    vectors = vectors.astype(BF16)
    for e in range(2):
        for g in range(2):
            line = jnp.dot(vectors, wgu[g, e], preferred_element_type=F32)
            for j in range(per_expert):
                piece = line[:, j * L : (j + 1) * L]
                ax1s[e * per_expert + j, 0:1, g * L : (g + 1) * L] = piece[0:1] + piece[1:2]
                ax1s[e * per_expert + j, 1:2, g * L : (g + 1) * L] = piece[2:3] + piece[3:4]
    ax1r[0] = ax1s[y]

    done(xt.at[pl.ds(1, 2 * nx - 1)], rsem.at[0])

    for k in range(2 * nx):
        tr[z, k] = xt[k, z]

    def z_copy(to):
        device = {"ep": to * nx + x, "tp": tp}
        remote(xt.at[:, to], tr.at[z], ssem.at[2], tsem.at[own_batch], device).start()

    def z_ready_copy(to):
        pl.semaphore_wait(zready.at[to], 1)
        z_copy(to)

    planes(first, z, z_copy)
    planes(z + 1, first + part, z_ready_copy)
    step = part // 2

    @pl.when(z < step)
    def _():
        device = {"ep": (z + step) * nx + x, "tp": tp}
        remote(xt.at[:, z + part], halfway, ssem.at[2], fsem.at[0], device).start()
        planes(part, z + part, z_ready_copy)
        planes(z + part + 1, nz, z_ready_copy)
        pl.semaphore_wait(zready.at[z + part], 1)

    @pl.when((z >= step) & (z < part))
    def _():
        pl.semaphore_wait(zready.at[z + step], 1)
        done(halfway, fsem.at[0])
        device = {"ep": (z + step) * nx + x, "tp": tp}
        remote(halfway, tr.at[z - step], fsem.at[1], tsem.at[0], device).start()
        z_copy(z + step)
        planes(part, z + step, z_ready_copy)
        planes(z + step + 1, nz, z_ready_copy)

    def z_shares(d):
        return remote(zs.at[lax.rem(z + d, nz)], sr.at[z], ssem.at[3], rsem.at[3], dev(dz=d))

    done(xs.at[pl.ds(1, nx - 1)], rsem.at[1])
    blocks = [xs[dx].astype(F32) for dx in range(nx)]
    for d in range(nz):
        block = [b[d * CAP : (d + 1) * CAP, :] for b in blocks]
        zs[d] = jnp.concatenate(block, axis=0).astype(BF16)
    sr[z] = zs[z]
    each(nz, lambda d: z_shares(d).start())

    @pl.when(rank < ny - 1)
    def _():
        pl.semaphore_wait(yready, ny - 1 - rank)

    def a1_copy(d):
        return remote(ax1s.at[(y + d) % ny], ax1r.at[d], ssem.at[4], rsem.at[4], dev(dy=d))

    each(ny, lambda d: a1_copy(d).start())

    cuts = [0, EARLY, nz]

    def rows_of(b):
        return pl.ds(cuts[b] * per_plane, (cuts[b + 1] - cuts[b]) * per_plane)

    def p_copy(b, d):
        here = rows_of(b)
        return remote(
            ps.at[d - 1, :, here], pr.at[d - 1, :, here], ssem.at[6], psem.at[b, d - 1], dev(dy=d)
        )

    def a2_copy(b, d):
        return remote(ax2s.at[b], ax2r.at[b, d], ssem.at[5], asem.at[b], dev(dy=d))

    gate_own, up_own = [], []
    for b in range(2):
        slots = range(cuts[b], cuts[b + 1])
        here = rows_of(b)
        batch_rows = here.size

        @pl.when(own_batch == b)
        def _():
            done(tr.at[pl.ds(1, len(slots) - 1)], tsem.at[b])

        @pl.when(own_batch != b)
        def _():
            done(tr.at[pl.ds(0, len(slots))], tsem.at[b])

        values = [
            jnp.concatenate([tr[i, 2 * dx + dc].astype(F32) for i in slots for dx in range(nx)], axis=0)
            for dc in range(2)
        ]
        values = jnp.concatenate(values, axis=1)
        middle = jnp.sum(values, axis=1, keepdims=True) * (1.0 / (2 * L))
        values = values - middle
        scaled = (values * gain).astype(BF16)
        waiting = []
        for place, d in enumerate(far_first(ny) + [0]):
            q = (y + d) % ny
            e = q // per_expert
            cols = pl.ds(pl.multiple_of((q % per_expert) * L, L), L)
            gate_part = jnp.dot(scaled, wgu[0, e, :, cols], preferred_element_type=F32)
            up_part = jnp.dot(scaled, wgu[1, e, :, cols], preferred_element_type=F32)
            if d == 0:
                gate_own.append(gate_part)
                up_own.append(up_part)
            else:
                ps[d - 1, 0, here] = gate_part.astype(BF16)
                ps[d - 1, 1, here] = up_part.astype(BF16)
                if place:
                    waiting.append(d)
                if place in (2, ny - 2):

                    @pl.when(ep >= 0)
                    def _():
                        for w in waiting:
                            p_copy(b, w).start()

                    waiting = []
            if place == 0:
                squares = jnp.sum(values * values, axis=1, keepdims=True)
                lanes = iota((batch_rows, L), 1)
                columns = jnp.where(lanes == 0, middle, 0.0) + jnp.where(lanes == 1, squares, 0.0)
                columns = jnp.transpose(columns)
                ax2s[b, :, 0:batch_rows] = columns[0:2, :]
                ax2r[b, 0, :, 0:batch_rows] = columns[0:2, :]

                @pl.when(ep >= 0)
                def _():
                    for w in far_first(ny):
                        a2_copy(b, w).start()
                    p_copy(b, far_first(ny)[0]).start()


    def h_copy(b, d):
        here = rows_of(b)
        return remote(hb.at[0, here], hb.at[d, here], ssem.at[7], hsem.at[b, d - 1], dev(dy=d))

    done(sr.at[pl.ds(1, nz - 1)], rsem.at[3])
    done(ax1r.at[pl.ds(1, ny - 1)], rsem.at[4])
    expert = 2 * x + y // per_expert
    gate_bias = up_bias = jnp.zeros((1, L), F32)
    for d in range(ny):
        gate_bias = gate_bias + ax1r[d, 1:2, 0:L]
        up_bias = up_bias + ax1r[d, 1:2, L : 2 * L]
    for b in range(2):
        here = rows_of(b)
        batch_rows = here.size
        lanes = iota((batch_rows, L), 1)
        share = jnp.concatenate([sr[i].astype(F32) for i in range(cuts[b], cuts[b + 1])], axis=0)
        share = jnp.sum(
            jnp.where((lanes == expert) | (lanes == expert + EPG), share, 0.0), axis=1, keepdims=True
        )
        done(ax2r.at[b, pl.ds(1, ny - 1)], asem.at[b])
        means = [ax2r[b, d, 0:1, 0:batch_rows] for d in range(ny)]
        center = sum(means) * (1.0 / ny)
        shifts = [m - center for m in means]
        spread = sum(ax2r[b, d, 1:2, 0:batch_rows] for d in range(ny))
        spread = spread + (features // ny) * sum(s * s for s in shifts)
        scale = lax.rsqrt(spread * (1.0 / features) + norm_epsilon)
        stack = iota((16, batch_rows), 0)
        table = jnp.where(stack == ny, scale, 0.0)
        for d in range(ny):
            table = table + jnp.where(stack == d, shifts[d], 0.0)
        table = jnp.transpose(table)
        scale = table[:, ny : ny + 1]
        gate, up = gate_own[b], up_own[b]
        for d in range(ny):
            shift = table[:, d : d + 1]
            gate = gate + shift * ax1r[d, 0:1, 0:L]
            up = up + shift * ax1r[d, 0:1, L : 2 * L]
        for d in far_first(ny):
            p_copy(b, d).wait_recv()
            gate = gate + pr[d - 1, 0, here].astype(F32)
            up = up + pr[d - 1, 1, here].astype(F32)
        gate = gate * scale + gate_bias
        up = up * scale + up_bias
        hb[0, here] = (share * (gate / (1.0 + jnp.exp(-gate)) * up)).astype(BF16)

        @pl.when(ep >= 0)
        def _():
            for d in far_first(ny):
                h_copy(b, d).start()


    def down(b, d):
        q = (y - d + ny) % ny
        units = pl.ds(pl.multiple_of((q % per_expert) * L, L), L)
        return jnp.dot(hb[d, rows_of(b)], wd[q // per_expert, units, :], preferred_element_type=F32)

    done(wd.at[:, :, 0:L], lsem.at[1])
    done(wd.at[:, :, L : 2 * L], wsem.at[5])

    back_x = [lax.rem(x - d + nx, nx) for d in range(nx)]
    back_tp = [tp, tp + 1 - 2 * c]
    order = sorted(range(2 * nx), key=lambda k: -min(k // 2, nx - k // 2))

    def send_back(h, k):
        to = {"ep": h * nx + back_x[k // 2], "tp": back_tp[k % 2]}
        remote(os.at[h * 2 * nx + k], rr.at[z * 2 * nx + k], ssem.at[8], rsem.at[6], to).start()

    for b in range(2):
        total = down(b, 0)
        for d in sorted(range(1, ny), key=lambda d: min(d, ny - d)):
            h_copy(b, d).wait_recv()
            total = total + down(b, d)
        slots = range(cuts[b], cuts[b + 1])
        for h in slots:
            for k in range(2 * nx):
                at = (h - cuts[b]) * per_plane + k // 2 * CAP
                piece = total[at : at + CAP, (k % 2) * L : (k % 2 + 1) * L]
                os[h * 2 * nx + k] = piece.astype(BF16)
        for h in slots:
            for k in order:
                if k:
                    send_back(h, k)
                else:
                    pl.when(z != h)(functools.partial(send_back, h, k))
    rr[z * 2 * nx] = os[z * 2 * nx]

    done(xt.at[pl.ds(1, 2 * nx - 1)], ssem.at[0])

    @pl.when((z >= step) & (z < part))
    def _():
        done(halfway, fsem.at[1])

    done(xs.at[pl.ds(1, nx - 1)], ssem.at[1])
    done(tr.at[pl.ds(1, nz - 1)], ssem.at[2])
    done(sr.at[pl.ds(1, nz - 1)], ssem.at[3])
    done(ax1r.at[pl.ds(1, ny - 1)], ssem.at[4])
    done(ax2r.at[:, pl.ds(1, ny - 1)], ssem.at[5])
    done(ps, ssem.at[6])
    done(hb.at[pl.ds(1, ny - 1)], ssem.at[7])
    done(gb, wsem.at[0])
    done(wgu.at[:, :, 0:L, :], wsem.at[2])
    done(wd.at[:, :, 0:L], wsem.at[4])
    done(rr.at[pl.ds(1, 2 * nx * nz - 1)], rsem.at[6])

    result = jnp.zeros((tokens, L), F32)
    for d in range(nz):
        back = rr[d * 2 * nx].astype(F32)
        for k in range(1, 2 * nx):
            back = back + rr[d * 2 * nx + k].astype(F32)
        for s in range(CAP):
            at = d * CAP + s
            result = result + chosen[:, at : at + 1] * back[s : s + 1, :]
    out_ref[...] = result.astype(BF16)
    done(os.at[pl.ds(1, 2 * nx * nz - 1)], ssem.at[8])


def solution(mesh):
    nx = EPG // 2
    nz = mesh.shape["ep"] // nx
    ny = mesh.shape["tp"] // 2

    def on_device(tokens, gain, bias, group_pick, member_pick, probs, gate, up, down):
        width = tokens.shape[1]
        half = gate.shape[2] // 2
        rows = nz * CAP
        all_rows = nx * rows
        vmem, dma = pltpu.VMEM, pltpu.SemaphoreType.DMA
        whole = pl.BlockSpec(memory_space=pltpu.VMEM)
        away = pl.BlockSpec(memory_space=pl.ANY)
        return pl.pallas_call(
            functools.partial(kernel, nz, nx, ny, width * 2 * ny),
            out_shape=pltpu.VMEM(tokens.shape, BF16),
            in_specs=[away] * 9,
            out_specs=whole,
            scratch_shapes=[
                vmem(tokens.shape, BF16),
                vmem((1, L), F32),
                vmem((1, L), F32),
                vmem((1, tokens.shape[0]), jnp.int32),
                vmem(member_pick.shape[::-1], jnp.int32),
                vmem(probs.shape[::-1], F32),
                vmem((2, 2, 2 * L, half), BF16),
                vmem((2, half, 2 * L), BF16),
                vmem((2, 1, L), F32),
                vmem((2 * nx, nz, CAP, L), BF16),
                vmem((nx, rows, L), BF16),
                vmem((nz, nx * CAP, L), BF16),
                vmem((nz, 2 * nx, CAP, L), BF16),
                vmem((nz, nx * CAP, L), BF16),
                vmem((2 * nx, CAP, L), BF16),
                vmem((ny, 2, 2 * L), F32),
                vmem((ny, 2, 2 * L), F32),
                vmem((2, 2, L), F32),
                vmem((2, ny, 2, L), F32),
                vmem((ny - 1, 2, all_rows, L), BF16),
                vmem((ny - 1, 2, all_rows, L), BF16),
                vmem((ny, all_rows, L), BF16),
                vmem((2 * nx * nz, CAP, L), BF16),
                vmem((2 * nx * nz, CAP, L), BF16),
                pltpu.SemaphoreType.REGULAR((nz,)),
                pltpu.SemaphoreType.REGULAR,
                dma((2,)),
                dma((6,)),
                dma((2,)),
                dma((6,)),
                dma((9,)),
                dma((7,)),
                dma((2,)),
                dma((2,)),
                dma((2, ny - 1)),
                dma((2, ny - 1)),
            ],
            compiler_params=pltpu.CompilerParams(collective_id=0, has_side_effects=True),
        )(tokens, gain.reshape(1, -1), bias.reshape(1, -1), group_pick.T, member_pick.T, probs.T, gate, up, down)

    return jax.shard_map(
        on_device,
        mesh=mesh,
        in_specs=(
            P("ep", "tp"),
            P("tp"),
            P("tp"),
            P("ep", None),
            P("ep", None),
            P("ep", None),
            P("ep", "tp", None),
            P("ep", "tp", None),
            P("ep", None, "tp"),
        ),
        out_specs=P("ep", "tp"),
        check_vma=False,
    )
```

```python
import functools

import jax
import jax.numpy as jnp
from jax import lax
from jax.experimental import pallas as pl
from jax.experimental.pallas import tpu as pltpu
from jax.sharding import PartitionSpec as P

EPG = 8
CAP = 2
EARLY = 2
norm_epsilon = 1e-05
MESH = pl.DeviceIdType.MESH
F32 = jnp.float32
BF16 = jnp.bfloat16
L = 128


def iota(shape, axis):
    return lax.broadcasted_iota(jnp.int32, shape, axis)


def far_first(n):
    return sorted(range(1, n), key=lambda d: -min(d, n - d))


def kernel(
    nz, nx, ny, features,
    tok_hbm, gain_hbm, bias_hbm, gp_hbm, mp_hbm, pp_hbm, gate_hbm, up_hbm, down_hbm,
    out_ref,
    tok_ref, gain_ref, bias_ref, gp_ref, mp_ref, pp_ref,
    wgu, wd, gb,
    xt, xs, zs, tr, sr, halfway, ax1s, ax1r, ax2s, ax2r, ps, pr, hb, os, rr,
    zready, yready, fsem, isem, lsem, wsem, ssem, rsem, tsem, asem, psem, hsem,
):
    tokens = tok_ref.shape[0]
    half = wgu.shape[3]
    rows = nz * CAP
    per_plane = nx * CAP
    all_rows = nz * per_plane
    per_expert = ny // 2
    ep, tp = lax.axis_index("ep"), lax.axis_index("tp")
    z, x, y, c = ep // nx, ep % nx, tp // 2, tp % 2

    def dev(dz=0, dx=0, dy=0, dc=0):
        return {
            "ep": lax.rem(z + dz + nz, nz) * nx + lax.rem(x + dx + nx, nx),
            "tp": lax.rem(y + dy + ny, ny) * 2 + lax.rem(c + dc, 2),
        }

    def remote(src, dst, ss, rs, device):
        return pltpu.make_async_remote_copy(
            src_ref=src, dst_ref=dst, send_sem=ss, recv_sem=rs, device_id=device, device_id_type=MESH
        )

    def each(n, body):
        lax.fori_loop(1, n, lambda d, carry: (body(d), carry)[1], 0)

    def done(ref, sem):
        pltpu.make_async_copy(ref, ref, sem).wait()

    def signal(sem, device):
        pl.semaphore_signal(sem, inc=1, device_id=device, device_id_type=MESH)

    def planes(low, high, body):
        lax.fori_loop(low, high, lambda to, carry: (body(to), carry)[1], 0)

    part = nz // 2
    side = z // part
    first = side * part

    def ranked(r):
        return r + r // per_expert * (3 * per_expert - 1 - 2 * r)

    rank = ranked(y)
    own_batch = (z + nz - EARLY) // nz
    barrier = pltpu.get_barrier_semaphore()

    def greet(to):
        signal(barrier, {"ep": to * nx + x, "tp": tp})

    go_x = [lax.rem(x + d, nx) for d in range(nx)]
    go_tp = [tp, tp + 1 - 2 * c]

    def mate(k):
        return {"ep": z * nx + go_x[k // 2], "tp": go_tp[k % 2]}

    for k in range(1, 2 * nx):
        signal(barrier, mate(k))

    planes(z + 1, first + part, greet)
    inputs = [
        pltpu.make_async_copy(src, dst, isem.at[i])
        for i, (src, dst) in enumerate(
            (
                (gp_hbm, gp_ref),
                (mp_hbm, mp_ref),
                (pp_hbm, pp_ref),
                (tok_hbm, tok_ref),
                (gain_hbm, gain_ref),
                (bias_hbm, bias_ref),
            )
        )
    ]
    for copy in inputs:
        copy.start()

    planes(rank + 1, ny, lambda r: signal(barrier, {"ep": ep, "tp": 2 * ranked(r) + c}))

    mine = pl.ds(pl.multiple_of(c * half, half), half)
    other = pl.ds(pl.multiple_of((1 - c) * half, half), half)
    pltpu.make_async_copy(gate_hbm.at[:, :, mine], wgu.at[0, :, 0:L, :], lsem.at[0]).start()
    pltpu.make_async_copy(up_hbm.at[:, :, mine], wgu.at[1, :, 0:L, :], lsem.at[0]).start()
    pltpu.make_async_copy(down_hbm.at[:, mine, :], wd.at[:, :, 0:L], lsem.at[1]).start()

    for copy in inputs:
        copy.wait()

    group = gp_ref[...]
    row = iota((rows, tokens), 0)
    lane = iota((rows, tokens), 1)
    member = (group == row // CAP).astype(F32)
    count = jnp.zeros((rows, tokens), F32)
    for t in range(tokens - 1):
        count = count + jnp.where(lane > t, member[:, t : t + 1], 0.0)
    rowwise = member * (count == (row % CAP).astype(F32)).astype(F32)
    def pack(source):
        packed = jnp.zeros((rows, L), F32)
        for t in range(tokens):
            packed = packed + rowwise[:, t : t + 1] * source[t : t + 1, :]
        return packed

    packed = pack(tok_ref[...].astype(F32))
    for d in range(nz):
        xt[0, d] = packed[d * CAP : (d + 1) * CAP, :].astype(BF16)

    pl.semaphore_wait(barrier, (2 * nx - 1) + z + rank)
    planes(0, z, lambda to: signal(zready.at[z], {"ep": to * nx + x, "tp": tp}))

    @pl.when(side == 0)
    def _():
        planes(part, nz, greet)

    def x_copy(k):
        return remote(xt.at[0], xt.at[k], ssem.at[0], rsem.at[0], mate(k))

    def x_shares(dx):
        return remote(xs.at[0], xs.at[dx], ssem.at[1], rsem.at[1], mate(2 * dx))

    for k in range(1, 2 * nx):
        x_copy(k).start()
    planes(0, rank, lambda r: signal(yready, {"ep": ep, "tp": 2 * ranked(r) + c}))


    def straight(to):
        for k in range(2 * nx):
            device = {"ep": to * nx + go_x[k // 2], "tp": go_tp[k % 2]}
            remote(xt.at[0, to], tr.at[z, k], ssem.at[2], tsem.at[own_batch], device).start()

    @pl.when(side == 1)
    def _():
        planes(0, part, straight)

    to = dev(dc=1)
    remote(gain_ref, gb.at[0], wsem.at[0], wsem.at[1], to).start()
    remote(bias_ref, gb.at[1], wsem.at[0], wsem.at[1], to).start()
    remote(gate_hbm.at[:, :, other], wgu.at[0, :, L : 2 * L, :], wsem.at[2], wsem.at[3], to).start()
    remote(up_hbm.at[:, :, other], wgu.at[1, :, L : 2 * L, :], wsem.at[2], wsem.at[3], to).start()
    remote(down_hbm.at[:, other, :], wd.at[:, :, L : 2 * L], wsem.at[4], wsem.at[5], to).start()

    probs = pp_ref[...]
    share = probs / jnp.sum(probs, axis=0, keepdims=True)
    top = probs.shape[0]
    table = [share[k : k + 1] for k in range(top)]
    table = table + [mp_ref[k : k + 1].astype(F32) for k in range(top)] + [rowwise]
    table = jnp.concatenate(table, axis=0)
    table = jnp.concatenate([table, jnp.zeros((2 * top + rows, L - tokens), F32)], axis=1)
    turned = jnp.transpose(table)[0:tokens, :]
    chosen = turned[:, 2 * top :]
    lane = iota((tokens, L), 1).astype(F32)
    shares = jnp.zeros((tokens, L), F32)
    for k in range(top):
        high = turned[:, k : k + 1].astype(BF16).astype(F32)
        low = turned[:, k : k + 1] - high
        pick = turned[:, top + k : top + k + 1]
        shares = shares + jnp.where(lane == pick, high, 0.0)
        shares = shares + jnp.where(lane == pick + EPG, low, 0.0)
    xs[0] = pack(shares).astype(BF16)
    for dx in range(1, nx):
        x_shares(dx).start()

    done(wgu.at[:, :, 0:L, :], lsem.at[0])
    done(gb, wsem.at[1])
    done(wgu.at[:, :, L : 2 * L, :], wsem.at[3])
    gain = jnp.concatenate([gain_ref[...], gb[0]], axis=1)
    bias = jnp.concatenate([bias_ref[...], gb[1]], axis=1)
    gain_high = gain.astype(BF16).astype(F32)
    bias_high = bias.astype(BF16).astype(F32)
    four = iota((16, 2 * L), 0)
    vectors = jnp.where(four == 0, gain_high, 0.0) + jnp.where(four == 1, gain - gain_high, 0.0)
    vectors = vectors + jnp.where(four == 2, bias_high, 0.0) + jnp.where(four == 3, bias - bias_high, 0.0)
    vectors = vectors.astype(BF16)
    for e in range(2):
        for g in range(2):
            line = jnp.dot(vectors, wgu[g, e], preferred_element_type=F32)
            for j in range(per_expert):
                piece = line[:, j * L : (j + 1) * L]
                ax1s[e * per_expert + j, 0:1, g * L : (g + 1) * L] = piece[0:1] + piece[1:2]
                ax1s[e * per_expert + j, 1:2, g * L : (g + 1) * L] = piece[2:3] + piece[3:4]
    ax1r[0] = ax1s[y]

    done(xt.at[pl.ds(1, 2 * nx - 1)], rsem.at[0])

    for k in range(2 * nx):
        tr[z, k] = xt[k, z]

    def z_copy(to):
        device = {"ep": to * nx + x, "tp": tp}
        remote(xt.at[:, to], tr.at[z], ssem.at[2], tsem.at[own_batch], device).start()

    def z_ready_copy(to):
        pl.semaphore_wait(zready.at[to], 1)
        z_copy(to)

    planes(first, z, z_copy)
    planes(z + 1, first + part, z_ready_copy)
    step = part // 2

    @pl.when(z < step)
    def _():
        device = {"ep": (z + step) * nx + x, "tp": tp}
        remote(xt.at[:, z + part], halfway, ssem.at[2], fsem.at[0], device).start()
        planes(part, z + part, z_ready_copy)
        planes(z + part + 1, nz, z_ready_copy)
        pl.semaphore_wait(zready.at[z + part], 1)

    @pl.when((z >= step) & (z < part))
    def _():
        pl.semaphore_wait(zready.at[z + step], 1)
        done(halfway, fsem.at[0])
        device = {"ep": (z + step) * nx + x, "tp": tp}
        remote(halfway, tr.at[z - step], fsem.at[1], tsem.at[0], device).start()
        z_copy(z + step)
        planes(part, z + step, z_ready_copy)
        planes(z + step + 1, nz, z_ready_copy)

    def z_shares(d):
        return remote(zs.at[lax.rem(z + d, nz)], sr.at[z], ssem.at[3], rsem.at[3], dev(dz=d))

    done(xs.at[pl.ds(1, nx - 1)], rsem.at[1])
    blocks = [xs[dx].astype(F32) for dx in range(nx)]
    for d in range(nz):
        block = [b[d * CAP : (d + 1) * CAP, :] for b in blocks]
        zs[d] = jnp.concatenate(block, axis=0).astype(BF16)
    sr[z] = zs[z]
    each(nz, lambda d: z_shares(d).start())

    @pl.when(rank < ny - 1)
    def _():
        pl.semaphore_wait(yready, ny - 1 - rank)

    def a1_copy(d):
        return remote(ax1s.at[(y + d) % ny], ax1r.at[d], ssem.at[4], rsem.at[4], dev(dy=d))

    each(ny, lambda d: a1_copy(d).start())

    cuts = [0, EARLY, nz]

    def rows_of(b):
        return pl.ds(cuts[b] * per_plane, (cuts[b + 1] - cuts[b]) * per_plane)

    def p_copy(b, d):
        here = rows_of(b)
        return remote(
            ps.at[d - 1, :, here], pr.at[d - 1, :, here], ssem.at[6], psem.at[b, d - 1], dev(dy=d)
        )

    def a2_copy(b, d):
        return remote(ax2s.at[b], ax2r.at[b, d], ssem.at[5], asem.at[b], dev(dy=d))

    gate_own, up_own = [], []
    for b in range(2):
        slots = range(cuts[b], cuts[b + 1])
        here = rows_of(b)
        batch_rows = here.size

        @pl.when(own_batch == b)
        def _():
            done(tr.at[pl.ds(1, len(slots) - 1)], tsem.at[b])

        @pl.when(own_batch != b)
        def _():
            done(tr.at[pl.ds(0, len(slots))], tsem.at[b])

        values = [
            jnp.concatenate([tr[i, 2 * dx + dc].astype(F32) for i in slots for dx in range(nx)], axis=0)
            for dc in range(2)
        ]
        values = jnp.concatenate(values, axis=1)
        middle = jnp.sum(values, axis=1, keepdims=True) * (1.0 / (2 * L))
        values = values - middle
        scaled = (values * gain).astype(BF16)
        waiting = []
        for place, d in enumerate(far_first(ny) + [0]):
            q = (y + d) % ny
            e = q // per_expert
            cols = pl.ds(pl.multiple_of((q % per_expert) * L, L), L)
            gate_part = jnp.dot(scaled, wgu[0, e, :, cols], preferred_element_type=F32)
            up_part = jnp.dot(scaled, wgu[1, e, :, cols], preferred_element_type=F32)
            if d == 0:
                gate_own.append(gate_part)
                up_own.append(up_part)
            else:
                ps[d - 1, 0, here] = gate_part.astype(BF16)
                ps[d - 1, 1, here] = up_part.astype(BF16)
                if place:
                    waiting.append(d)
                if place in (2, 4, ny - 2):

                    @pl.when(ep >= 0)
                    def _():
                        for w in waiting:
                            p_copy(b, w).start()

                    waiting = []
            if place == 0:
                squares = jnp.sum(values * values, axis=1, keepdims=True)
                lanes = iota((batch_rows, L), 1)
                columns = jnp.where(lanes == 0, middle, 0.0) + jnp.where(lanes == 1, squares, 0.0)
                columns = jnp.transpose(columns)
                ax2s[b, :, 0:batch_rows] = columns[0:2, :]
                ax2r[b, 0, :, 0:batch_rows] = columns[0:2, :]

                @pl.when(ep >= 0)
                def _():
                    for w in far_first(ny):
                        a2_copy(b, w).start()
                    p_copy(b, far_first(ny)[0]).start()


    def h_copy(b, d):
        here = rows_of(b)
        return remote(hb.at[0, here], hb.at[d, here], ssem.at[7], hsem.at[b, d - 1], dev(dy=d))

    done(sr.at[pl.ds(1, nz - 1)], rsem.at[3])
    done(ax1r.at[pl.ds(1, ny - 1)], rsem.at[4])
    expert = 2 * x + y // per_expert
    gate_bias = up_bias = jnp.zeros((1, L), F32)
    for d in range(ny):
        gate_bias = gate_bias + ax1r[d, 1:2, 0:L]
        up_bias = up_bias + ax1r[d, 1:2, L : 2 * L]
    for b in range(2):
        here = rows_of(b)
        batch_rows = here.size
        lanes = iota((batch_rows, L), 1)
        share = jnp.concatenate([sr[i].astype(F32) for i in range(cuts[b], cuts[b + 1])], axis=0)
        share = jnp.sum(
            jnp.where((lanes == expert) | (lanes == expert + EPG), share, 0.0), axis=1, keepdims=True
        )
        done(ax2r.at[b, pl.ds(1, ny - 1)], asem.at[b])
        means = [ax2r[b, d, 0:1, 0:batch_rows] for d in range(ny)]
        center = sum(means) * (1.0 / ny)
        shifts = [m - center for m in means]
        spread = sum(ax2r[b, d, 1:2, 0:batch_rows] for d in range(ny))
        spread = spread + (features // ny) * sum(s * s for s in shifts)
        scale = lax.rsqrt(spread * (1.0 / features) + norm_epsilon)
        stack = iota((16, batch_rows), 0)
        table = jnp.where(stack == ny, scale, 0.0)
        for d in range(ny):
            table = table + jnp.where(stack == d, shifts[d], 0.0)
        table = jnp.transpose(table)
        scale = table[:, ny : ny + 1]
        gate, up = gate_own[b], up_own[b]
        for d in range(ny):
            shift = table[:, d : d + 1]
            gate = gate + shift * ax1r[d, 0:1, 0:L]
            up = up + shift * ax1r[d, 0:1, L : 2 * L]
        for d in far_first(ny):
            p_copy(b, d).wait_recv()
            gate = gate + pr[d - 1, 0, here].astype(F32)
            up = up + pr[d - 1, 1, here].astype(F32)
        gate = gate * scale + gate_bias
        up = up * scale + up_bias
        hb[0, here] = (share * (gate / (1.0 + jnp.exp(-gate)) * up)).astype(BF16)

        @pl.when(ep >= 0)
        def _():
            for d in far_first(ny):
                h_copy(b, d).start()


    def down(b, d):
        q = (y - d + ny) % ny
        units = pl.ds(pl.multiple_of((q % per_expert) * L, L), L)
        return jnp.dot(hb[d, rows_of(b)], wd[q // per_expert, units, :], preferred_element_type=F32)

    done(wd.at[:, :, 0:L], lsem.at[1])
    done(wd.at[:, :, L : 2 * L], wsem.at[5])

    back_x = [lax.rem(x - d + nx, nx) for d in range(nx)]
    back_tp = [tp, tp + 1 - 2 * c]
    order = sorted(range(2 * nx), key=lambda k: -min(k // 2, nx - k // 2))

    def send_back(h, k):
        to = {"ep": h * nx + back_x[k // 2], "tp": back_tp[k % 2]}
        remote(os.at[h * 2 * nx + k], rr.at[z * 2 * nx + k], ssem.at[8], rsem.at[6], to).start()

    for b in range(2):
        total = down(b, 0)
        for d in sorted(range(1, ny), key=lambda d: min(d, ny - d)):
            h_copy(b, d).wait_recv()
            total = total + down(b, d)
        slots = range(cuts[b], cuts[b + 1])
        for h in slots:
            for k in range(2 * nx):
                at = (h - cuts[b]) * per_plane + k // 2 * CAP
                piece = total[at : at + CAP, (k % 2) * L : (k % 2 + 1) * L]
                os[h * 2 * nx + k] = piece.astype(BF16)
        for h in slots:
            for k in order:
                if k:
                    send_back(h, k)
                else:
                    pl.when(z != h)(functools.partial(send_back, h, k))
    rr[z * 2 * nx] = os[z * 2 * nx]

    done(xt.at[pl.ds(1, 2 * nx - 1)], ssem.at[0])

    @pl.when((z >= step) & (z < part))
    def _():
        done(halfway, fsem.at[1])

    done(xs.at[pl.ds(1, nx - 1)], ssem.at[1])
    done(tr.at[pl.ds(1, nz - 1)], ssem.at[2])
    done(sr.at[pl.ds(1, nz - 1)], ssem.at[3])
    done(ax1r.at[pl.ds(1, ny - 1)], ssem.at[4])
    done(ax2r.at[:, pl.ds(1, ny - 1)], ssem.at[5])
    done(ps, ssem.at[6])
    done(hb.at[pl.ds(1, ny - 1)], ssem.at[7])
    done(gb, wsem.at[0])
    done(wgu.at[:, :, 0:L, :], wsem.at[2])
    done(wd.at[:, :, 0:L], wsem.at[4])
    done(rr.at[pl.ds(1, 2 * nx * nz - 1)], rsem.at[6])

    result = jnp.zeros((tokens, L), F32)
    for d in range(nz):
        back = rr[d * 2 * nx].astype(F32)
        for k in range(1, 2 * nx):
            back = back + rr[d * 2 * nx + k].astype(F32)
        for s in range(CAP):
            at = d * CAP + s
            result = result + chosen[:, at : at + 1] * back[s : s + 1, :]
    out_ref[...] = result.astype(BF16)
    done(os.at[pl.ds(1, 2 * nx * nz - 1)], ssem.at[8])


def solution(mesh):
    nx = EPG // 2
    nz = mesh.shape["ep"] // nx
    ny = mesh.shape["tp"] // 2

    def on_device(tokens, gain, bias, group_pick, member_pick, probs, gate, up, down):
        width = tokens.shape[1]
        half = gate.shape[2] // 2
        rows = nz * CAP
        all_rows = nx * rows
        vmem, dma = pltpu.VMEM, pltpu.SemaphoreType.DMA
        whole = pl.BlockSpec(memory_space=pltpu.VMEM)
        away = pl.BlockSpec(memory_space=pl.ANY)
        return pl.pallas_call(
            functools.partial(kernel, nz, nx, ny, width * 2 * ny),
            out_shape=pltpu.VMEM(tokens.shape, BF16),
            in_specs=[away] * 9,
            out_specs=whole,
            scratch_shapes=[
                vmem(tokens.shape, BF16),
                vmem((1, L), F32),
                vmem((1, L), F32),
                vmem((1, tokens.shape[0]), jnp.int32),
                vmem(member_pick.shape[::-1], jnp.int32),
                vmem(probs.shape[::-1], F32),
                vmem((2, 2, 2 * L, half), BF16),
                vmem((2, half, 2 * L), BF16),
                vmem((2, 1, L), F32),
                vmem((2 * nx, nz, CAP, L), BF16),
                vmem((nx, rows, L), BF16),
                vmem((nz, nx * CAP, L), BF16),
                vmem((nz, 2 * nx, CAP, L), BF16),
                vmem((nz, nx * CAP, L), BF16),
                vmem((2 * nx, CAP, L), BF16),
                vmem((ny, 2, 2 * L), F32),
                vmem((ny, 2, 2 * L), F32),
                vmem((2, 2, L), F32),
                vmem((2, ny, 2, L), F32),
                vmem((ny - 1, 2, all_rows, L), BF16),
                vmem((ny - 1, 2, all_rows, L), BF16),
                vmem((ny, all_rows, L), BF16),
                vmem((2 * nx * nz, CAP, L), BF16),
                vmem((2 * nx * nz, CAP, L), BF16),
                pltpu.SemaphoreType.REGULAR((nz,)),
                pltpu.SemaphoreType.REGULAR,
                dma((2,)),
                dma((6,)),
                dma((2,)),
                dma((6,)),
                dma((9,)),
                dma((7,)),
                dma((2,)),
                dma((2,)),
                dma((2, ny - 1)),
                dma((2, ny - 1)),
            ],
            compiler_params=pltpu.CompilerParams(collective_id=0, has_side_effects=True),
        )(tokens, gain.reshape(1, -1), bias.reshape(1, -1), group_pick.T, member_pick.T, probs.T, gate, up, down)

    return jax.shard_map(
        on_device,
        mesh=mesh,
        in_specs=(
            P("ep", "tp"),
            P("tp"),
            P("tp"),
            P("ep", None),
            P("ep", None),
            P("ep", None),
            P("ep", "tp", None),
            P("ep", "tp", None),
            P("ep", None, "tp"),
        ),
        out_specs=P("ep", "tp"),
        check_vma=False,
    )
```
